32 devices in a mesh: ep: 8 (over z, core), tp: 4 (over y, x).
Axes of the slice: x: 2, y: 2, z: 4, core: 2. Of those that a mesh axis runs over, the one named last changes fastest.
Arguments:
- tokens: bfloat16 [128, 2048], P('ep'), may hold values from -6 to 6
- old_state: float32 [128, 16, 128, 128], P('ep', 'tp'), may hold values from -2 to 2
- lower_bound: float32 [2048], P('tp'), may hold values from 0.05 to 0.95
- head_gain: float32 [2048], P('tp'), may hold values from 0.1 to 1.9
- norm_gains: float32 [4, 2048], replicated, may hold values from 0.1 to 1.9
- w_query: bfloat16 [2048, 2048], P('ep', 'tp'), may hold values from -0.125 to 0.125
- w_forget: bfloat16 [2048, 2048], P('ep', 'tp'), may hold values from -0.125 to 0.125
- w_value: bfloat16 [2048, 2048], P('ep', 'tp'), may hold values from -0.125 to 0.125
- w_outgate: bfloat16 [2048, 2048], P('ep', 'tp'), may hold values from -0.125 to 0.125
- w_mix_out: bfloat16 [2048, 2048], P('tp', 'ep'), may hold values from -0.125 to 0.125
- routes: int32 [128, 2], P('ep'), may hold values from 0 to 7, all different within a row; in each aligned block of 16 rows (0 to 15, 16 to 31, ...) at most 8 rows name the same one
- route_scores: float32 [128, 2], P('ep'), may hold values from -6 to 6
- w_exp_gate: bfloat16 [8, 2048, 3584], P('ep', None, 'tp'), may hold values from -0.125 to 0.125
- w_exp_up: bfloat16 [8, 2048, 3584], P('ep', None, 'tp'), may hold values from -0.125 to 0.125
- w_exp_down: bfloat16 [8, 3584, 2048], P('ep', 'tp'), may hold values from -0.75 to 0.75
- w_dense_gate: bfloat16 [2048, 6144], P('ep', 'tp'), may hold values from -0.125 to 0.125
- w_dense_up: bfloat16 [2048, 6144], P('ep', 'tp'), may hold values from -0.125 to 0.125
- w_dense_down: bfloat16 [6144, 2048], P('tp', 'ep'), may hold values from -0.75 to 0.75
- dense_mix: bfloat16 [2048], replicated, may hold values from -0.125 to 0.125
Outputs:
- layer_out: bfloat16 [128, 2048], P('ep', 'tp')
- new_state: float32 [128, 16, 128, 128], P('ep', 'tp')
The draws below stay inside these ranges and needn't reach their ends.
Inputs may be any that keep to these rules, and one draw needn't show every extreme that they name: `routes`: each row names 2 different experts. In each aligned block of 16 rows no expert is named by more than 8 rows, and in every draw some expert is named by exactly 8 rows of some block.
All inputs are finite; a program needn't handle non-finite values.
Results may differ from the reference program's by a relative error of at most 0.025.
Values may be sent and summed in bfloat16 or wider, within the bound.
A program may use at most 64 MiB of HBM per device.

```python
import math
import jax
import jax.numpy as jnp
import numpy as np
from jax import lax

D = 2048
HEADS = 16
HEAD = 128
EXP_FF = 3584
DENSE_FF = 6144
TOPK = 2
SEQ_DEV = 16
HW = 2048
EXPERTS = 8
CAP = 8
TOKENS = 128
N_EP = 8
N_TP = 4


def column_scaled(key, leading, fan_in):
    noise_key = jax.random.fold_in(key, 11)
    spread_key = jax.random.fold_in(key, 23)
    position = jnp.arange(D, dtype=jnp.float32) / D
    base = jnp.clip(jax.random.normal(noise_key, leading + (D,), jnp.float32), -6.0, 6.0)
    profile = 10.0 ** position
    rough = jnp.exp(jax.random.uniform(spread_key, (D,), jnp.float32, -0.7, 0.7))
    return jnp.clip(base * profile * rough * fan_in ** (-0.5) / 3.0, -0.75, 0.75)


def draw_w_exp_down(key, part):
    return column_scaled(key, (EXPERTS, EXP_FF), EXP_FF).astype(jnp.bfloat16)


def draw_w_dense_down(key, part):
    return column_scaled(key, (DENSE_FF,), DENSE_FF).astype(jnp.bfloat16)


def level_of(key, shape, split, low, largest):
    gain, own = 1.0, jax.random.fold_in(key, 6)
    for axis_at, shards_of in split:
        steps = jnp.exp(jax.random.uniform(jax.random.fold_in(own, axis_at), (shards_of,), jnp.float32, low / len(split), largest / len(split)))
        gain = gain * jnp.repeat(steps, shape[axis_at] // shards_of).reshape([-1 if axis == axis_at else 1 for axis in range(len(shape))])
    return gain


def assign_block(own_key, own, number, rows, amount, top, reach, skew):
    sequence = jax.random.permutation(own_key, amount)
    crowded, ordinary = shares(amount, rows * top, reach, skew, True), shares(amount, rows * top, reach, skew, False)
    places = jnp.arange(amount)

    def named(tallies, rotation):
        used = int((tallies > 0).sum())
        fixed = max(1, used // 4)
        passed = fixed + (places - fixed + rotation * (used - fixed)) % max(1, amount - fixed)
        return jnp.zeros((amount,), jnp.int32).at[sequence[jnp.where(places < fixed, places, passed)]].set(jnp.asarray(tallies, jnp.int32))

    tallies = jnp.where(number % 4 == 0, named(crowded, number // 4), named(ordinary, number - number // 4 - 1))
    mixed = jax.random.permutation(jax.random.fold_in(own, 3), amount)
    donor, sink = mixed[0:amount // 2 * 2:2], mixed[1:amount // 2 * 2:2]
    margin = jnp.minimum(tallies[donor] - 1, reach - tallies[sink]) // 2
    margin = jnp.where((donor == sequence[0]) | (sink == sequence[0]) | (tallies[sink] == 0), 0, jnp.maximum(margin, 0))
    passed = jax.random.randint(jax.random.fold_in(own, 4), (amount // 2,), 0, 1 << 20) % (margin + 1)
    tallies = tallies.at[donor].add(-passed).at[sink].add(passed)
    items = jnp.searchsorted(jnp.cumsum(tallies), jnp.arange(rows * top), side="right").astype(jnp.int32)
    table = items.reshape(top, rows).T
    table = table[jax.random.permutation(jax.random.fold_in(own, 1), rows)]
    rotation = jax.random.randint(jax.random.fold_in(own, 2), (rows, 1), 0, top)
    return jnp.take_along_axis(table, (jnp.arange(top)[None, :] + rotation) % top, axis=1)


def shares(number_of, total, bound, skew, full):
    weights = [(1 << 20) // math.isqrt(grade ** skew) + 1 for grade in range(1, number_of + 1)]
    largest = bound if full else min(bound, max(-(-total // number_of), total * weights[0] // sum(weights)))
    least = 1 if total - largest >= number_of - 1 else 0
    holding, rest = [largest] + [least] * (number_of - 1), total - largest - least * (number_of - 1)
    while rest > 0:
        candidates = [i for i in range(1, number_of) if holding[i] < largest] or [i for i in range(1, number_of) if holding[i] < bound]
        mass, budget = sum([weights[i] for i in candidates]), rest
        for i in candidates:
            addition = min(bound - holding[i], max(1, budget * weights[i] // mass), rest)
            holding[i] = holding[i] + addition
            rest = rest - addition
    return np.array(holding)


def noise(key, shape, width, most, cuts=(), held_as=jnp.bfloat16):
    level = level_of(key, shape, cuts, -0.22, 0.18) if cuts else 1.0
    drawn = jax.random.normal(key, shape, jnp.float32) * width * level
    return jnp.minimum(jnp.maximum(drawn, -most), most).astype(held_as)


def setup_inputs(seed: int = 0) -> dict:
    keys = jax.random.split(jax.random.key(seed), 20)
    tokens = noise(keys[0], (TOKENS, D), 1.0, 6.0, ((0, 8),))
    old_state = noise(keys[1], (TOKENS, HEADS, HEAD, HEAD), 0.3, 2.0, ((0, 8), (1, 4)), jnp.float32)
    lower_bound = jnp.clip(0.05 + 0.9 * jax.random.uniform(keys[2], (HW,), jnp.float32) ** level_of(keys[2], (HW,), ((0, 4),), -0.2, 0.2), 0.05, 0.95)
    head_gain = jnp.clip(1.0 + 0.18 * jax.random.normal(keys[3], (HW,), jnp.float32), 0.1, 1.9)
    norm_gains = jnp.clip(1.0 + 0.18 * jax.random.normal(keys[4], (4, D), jnp.float32), 0.1, 1.9)
    w_query = noise(keys[5], (D, HW), D ** -0.5, 0.125, ((0, 8), (1, 4)))
    w_forget = noise(keys[6], (D, HW), D ** -0.5, 0.125, ((0, 8), (1, 4)))
    w_value = noise(keys[7], (D, HW), D ** -0.5, 0.125, ((0, 8), (1, 4)))
    w_outgate = noise(keys[8], (D, HW), D ** -0.5, 0.125, ((0, 8), (1, 4)))
    w_mix_out = noise(keys[9], (HW, D), HW ** -0.5, 0.125, ((0, 4), (1, 8)))
    routes_keys = jax.random.split(jax.random.fold_in(keys[10], 1), TOKENS // SEQ_DEV)
    routes_turns = jax.random.permutation(jax.random.fold_in(keys[10], 3), TOKENS // SEQ_DEV)
    routes = jax.vmap(lambda own, number: assign_block(jax.random.fold_in(keys[10], 2), own, number, SEQ_DEV, EXPERTS, TOPK, CAP, 1))(routes_keys, routes_turns).reshape((TOKENS, TOPK))
    route_scores = noise(keys[11], (TOKENS, TOPK), 1.5, 6.0, ((0, 8),), jnp.float32)
    w_exp_gate = noise(keys[12], (EXPERTS, D, EXP_FF), D ** -0.5, 0.125, ((0, 8), (2, 4)))
    w_exp_up = noise(keys[13], (EXPERTS, D, EXP_FF), D ** -0.5, 0.125, ((0, 8), (2, 4)))
    w_exp_down = draw_w_exp_down(jax.random.fold_in(keys[19], 71), 0)
    w_dense_gate = noise(keys[15], (D, DENSE_FF), D ** -0.5, 0.125, ((0, 8), (1, 4)))
    w_dense_up = noise(keys[16], (D, DENSE_FF), D ** -0.5, 0.125, ((0, 8), (1, 4)))
    w_dense_down = draw_w_dense_down(jax.random.fold_in(keys[19], 71), 0)
    dense_mix = noise(keys[18], (D,), D ** -0.5, 0.125)
    return dict(tokens=tokens, old_state=old_state, lower_bound=lower_bound, head_gain=head_gain, norm_gains=norm_gains, w_query=w_query, w_forget=w_forget, w_value=w_value, w_outgate=w_outgate, w_mix_out=w_mix_out, routes=routes, route_scores=route_scores, w_exp_gate=w_exp_gate, w_exp_up=w_exp_up, w_exp_down=w_exp_down, w_dense_gate=w_dense_gate, w_dense_up=w_dense_up, w_dense_down=w_dense_down, dense_mix=dense_mix)


EPS = 1e-06

def rms_scale(values):
    return lax.rsqrt(lax.optimization_barrier(jnp.mean(values * values, axis=-1, keepdims=True)) + EPS)

def reference(tokens, old_state, lower_bound, head_gain, norm_gains, w_query, w_forget, w_value, w_outgate, w_mix_out, routes, route_scores, w_exp_gate, w_exp_up, w_exp_down, w_dense_gate, w_dense_up, w_dense_down, dense_mix):
    highest = lax.Precision.HIGHEST
    resid = tokens.astype(jnp.float32)
    normed = (resid * rms_scale(resid) * norm_gains[0]).astype(jnp.bfloat16)
    query_raw = jnp.dot(normed, w_query, preferred_element_type=jnp.float32)
    forget_raw = jnp.dot(normed, w_forget, preferred_element_type=jnp.float32)
    value = jnp.dot(normed, w_value, preferred_element_type=jnp.float32)
    out_gate = jnp.dot(normed, w_outgate, preferred_element_type=jnp.float32)
    forget = lower_bound + (1.0 - lower_bound) * jax.nn.sigmoid(forget_raw)
    key_in = (1.0 - lower_bound) * jax.nn.sigmoid(-forget_raw)
    shape_heads = (TOKENS, HEADS, HEAD)
    new_state = forget.reshape(shape_heads)[..., None] * old_state + key_in.reshape(shape_heads)[..., None] * value.reshape(TOKENS, HEADS, 1, HEAD)
    query = jax.nn.silu(query_raw).reshape(shape_heads)
    read = jnp.einsum('thk,thkv->thv', query, new_state, precision=highest)
    gated = read * rms_scale(read) * head_gain.reshape(HEADS, HEAD) * jax.nn.silu(out_gate).reshape(shape_heads)
    mixed_heads = gated.reshape(TOKENS, HW).astype(jnp.bfloat16)
    groups = mixed_heads.reshape(TOKENS, N_TP, HW // N_TP).astype(jnp.float32)
    out_rows = w_mix_out.reshape(N_TP, HW // N_TP, D).astype(jnp.float32)
    mix_parts = jnp.einsum('tgk,gkd->gtd', groups, out_rows, precision=highest).astype(jnp.bfloat16)
    mix_out = lax.optimization_barrier(jnp.sum(mix_parts.astype(jnp.float32), axis=0)).astype(jnp.bfloat16)
    mix_wide = lax.optimization_barrier(mix_out).astype(jnp.float32)
    after_mix = resid + mix_wide * rms_scale(mix_wide) * norm_gains[1]
    ffn_in = (after_mix * rms_scale(after_mix) * norm_gains[2]).astype(jnp.bfloat16)
    blocks = routes.reshape(N_EP, SEQ_DEV * TOPK)
    expert_ids = jnp.arange(EXPERTS).astype(jnp.int32)
    onehot = (blocks[:, :, None] == expert_ids[None, None, :]).astype(jnp.int32)
    before = jnp.cumsum(onehot, axis=1).astype(jnp.int32) - onehot
    slots = lax.optimization_barrier(jnp.sum(onehot * before, axis=2)).astype(jnp.int32)
    route_rows = jnp.repeat(ffn_in.reshape(N_EP, SEQ_DEV, D), TOPK, axis=1).astype(jnp.float32)
    slot_ids = jnp.arange(CAP).astype(jnp.int32)

    def one_expert(index):
        chosen = ((blocks == index)[:, None, :] & (slots[:, None, :] == slot_ids[None, :, None])).astype(jnp.float32)
        expert_in = jnp.einsum('bcr,brd->bcd', chosen, route_rows, precision=highest).astype(jnp.bfloat16)
        expert_in = expert_in.reshape(N_EP * CAP, D)
        gate_pre = jnp.dot(expert_in, w_exp_gate[index], preferred_element_type=jnp.float32)
        up_pre = jnp.dot(expert_in, w_exp_up[index], preferred_element_type=jnp.float32)
        hidden = (jax.nn.silu(gate_pre) * up_pre).astype(jnp.bfloat16)
        hidden_groups = hidden.reshape(N_EP * CAP, N_TP, EXP_FF // N_TP).astype(jnp.float32)
        down_groups = w_exp_down[index].reshape(N_TP, EXP_FF // N_TP, D).astype(jnp.float32)
        parts = jnp.einsum('rgk,gkd->grd', hidden_groups, down_groups, precision=highest).astype(jnp.bfloat16)
        result = lax.optimization_barrier(jnp.sum(parts.astype(jnp.float32), axis=0)).astype(jnp.bfloat16)
        return result.reshape(N_EP, CAP, D)
    expert_out = lax.map(one_expert, expert_ids)
    block_ids = jnp.broadcast_to(jnp.arange(N_EP).astype(jnp.int32)[:, None], blocks.shape)
    picked = expert_out[blocks, block_ids, slots].astype(jnp.float32)
    first = jax.nn.sigmoid(route_scores[:, 0] - route_scores[:, 1])
    second = jax.nn.sigmoid(route_scores[:, 1] - route_scores[:, 0])
    route_weight = jnp.stack([first, second], axis=1).reshape(N_EP, SEQ_DEV * TOPK)
    weighted = (picked * route_weight[..., None]).reshape(N_EP, SEQ_DEV, TOPK, D)
    expert_sum = lax.optimization_barrier(jnp.sum(weighted, axis=2)).reshape(TOKENS, D)
    dense_gate_pre = jnp.dot(ffn_in, w_dense_gate, preferred_element_type=jnp.float32)
    dense_up_pre = jnp.dot(ffn_in, w_dense_up, preferred_element_type=jnp.float32)
    dense_hidden = (jax.nn.silu(dense_gate_pre) * dense_up_pre).astype(jnp.bfloat16)
    dense_out = jnp.dot(dense_hidden, w_dense_down, preferred_element_type=jnp.float32)
    mix_weight = jax.nn.sigmoid(jnp.dot(ffn_in, dense_mix, preferred_element_type=jnp.float32))
    ffn_out = expert_sum + mix_weight[:, None] * dense_out
    layer_out = (after_mix + ffn_out * rms_scale(ffn_out) * norm_gains[3]).astype(jnp.bfloat16)
    return (layer_out, new_state)
```

```python
import jax
import jax.numpy as jnp
from jax import lax
from jax.experimental import pallas as pl
from jax.experimental.pallas import tpu as pltpu
from jax.sharding import PartitionSpec as P

EPS = 1e-06


def rms_scale(values):
    return lax.rsqrt(jnp.mean(values * values, axis=-1, keepdims=True) + EPS)


def body(
    tokens,
    old_state,
    lower_bound,
    head_gain,
    norm_gains,
    w_query,
    w_forget,
    w_value,
    w_outgate,
    w_mix_out,
    routes,
    route_scores,
    w_exp_gate,
    w_exp_up,
    w_exp_down,
    w_dense_gate,
    w_dense_up,
    w_dense_down,
    dense_mix,
):
    highest = lax.Precision.HIGHEST
    seqs, width = tokens.shape
    column_index = lax.axis_index("tp")
    part_width = width // lax.axis_size("tp")
    resid = tokens.astype(jnp.float32)
    normed = (resid * rms_scale(resid) * norm_gains[0]).astype(jnp.bfloat16)
    in_weights = jnp.concatenate([w_query, w_forget, w_value, w_outgate], axis=1)
    mix_rows = lax.all_to_all(normed, "ep", split_axis=1, concat_axis=0, tiled=True)
    projected = lax.psum_scatter(
        jnp.dot(mix_rows, in_weights, preferred_element_type=jnp.float32).astype(jnp.bfloat16),
        "ep",
        scatter_dimension=0,
        tiled=True,
    ).astype(jnp.float32)
    query_raw, forget_raw, value, out_gate = jnp.split(projected, 4, axis=1)
    heads = old_state.shape[1]
    head_size = old_state.shape[2]
    shape_heads = (seqs, heads, head_size)
    forget = lower_bound + (1.0 - lower_bound) * jax.nn.sigmoid(forget_raw)
    key_in = (1.0 - lower_bound) * jax.nn.sigmoid(-forget_raw)
    new_state = forget.reshape(shape_heads)[..., None] * old_state + key_in.reshape(shape_heads)[
        ..., None
    ] * value.reshape(seqs, heads, 1, head_size)
    query = jax.nn.silu(query_raw).reshape(shape_heads)
    read = jnp.einsum("thk,thkv->thv", query, new_state, precision=highest)
    gated = (
        read
        * rms_scale(read)
        * head_gain.reshape(heads, head_size)
        * jax.nn.silu(out_gate).reshape(shape_heads)
    )
    mixed_heads = gated.reshape(seqs, heads * head_size).astype(jnp.bfloat16)
    mix_part = jnp.dot(
        mixed_heads,
        lax.all_gather(w_mix_out, "ep", axis=1, tiled=True),
        preferred_element_type=jnp.float32,
    ).astype(jnp.bfloat16)
    mix_part = lax.optimization_barrier(mix_part).astype(jnp.float32)
    mix_out = lax.psum(mix_part.astype(jnp.bfloat16), "tp")
    mix_wide = lax.optimization_barrier(mix_out).astype(jnp.float32)
    after_mix = resid + mix_wide * rms_scale(mix_wide) * norm_gains[1]
    ffn_in = (after_mix * rms_scale(after_mix) * norm_gains[2]).astype(jnp.bfloat16)
    experts = lax.axis_size("ep")
    topk = routes.shape[1]
    capacity = max(2, 2 * seqs * topk // experts)
    flat_routes = routes.reshape(-1)
    onehot = (flat_routes[:, None] == jnp.arange(experts, dtype=jnp.int32)[None, :]).astype(
        jnp.int32
    )
    before = jnp.cumsum(onehot, axis=0) - onehot
    slots = jnp.sum(onehot * before, axis=1)
    cells = flat_routes * capacity + slots
    placed = cells[None, :] == jnp.arange(experts * capacity, dtype=jnp.int32)[:, None]
    repeated = jnp.repeat(ffn_in, topk, axis=0)
    outgoing = jnp.dot(placed.astype(jnp.bfloat16), repeated, preferred_element_type=jnp.float32)
    outgoing = outgoing.astype(jnp.bfloat16).reshape(experts, capacity, width)
    arrived = lax.all_to_all(outgoing, "ep", split_axis=0, concat_axis=0, tiled=True)
    sources, items, _ = arrived.shape
    expert_rows = arrived.reshape(sources * items, width)
    gate_pre = jnp.dot(expert_rows, w_exp_gate[0], preferred_element_type=jnp.float32)
    up_pre = jnp.dot(expert_rows, w_exp_up[0], preferred_element_type=jnp.float32)
    hidden = (jax.nn.silu(gate_pre) * up_pre).astype(jnp.bfloat16)
    partial_rows = jnp.dot(hidden, w_exp_down[0], preferred_element_type=jnp.float32).astype(
        jnp.bfloat16
    )
    partial_rows = lax.optimization_barrier(partial_rows).astype(jnp.float32)
    partial_rows = partial_rows.reshape(sources, items, width)
    summed = lax.psum_scatter(
        partial_rows.astype(jnp.bfloat16), "tp", scatter_dimension=2, tiled=True
    )
    returned = lax.all_to_all(summed, "ep", split_axis=0, concat_axis=0, tiled=True)
    first = jax.nn.sigmoid(route_scores[:, 0] - route_scores[:, 1])
    second = jax.nn.sigmoid(route_scores[:, 1] - route_scores[:, 0])
    route_weight = jnp.stack([first, second], axis=1).reshape(-1)
    weight_table = jnp.sum(
        (placed.astype(jnp.float32) * route_weight[None, :]).reshape(
            experts * capacity, seqs, topk
        ),
        axis=2,
    )
    expert_sum = jnp.dot(
        weight_table.T,
        returned.reshape(experts * capacity, part_width).astype(jnp.float32),
        precision=highest,
    )
    dense_weights = jnp.concatenate([w_dense_gate, w_dense_up], axis=1)
    dense_rows = lax.all_to_all(ffn_in, "ep", split_axis=1, concat_axis=0, tiled=True)
    dense_pre = lax.psum_scatter(
        jnp.dot(dense_rows, dense_weights, preferred_element_type=jnp.float32).astype(jnp.bfloat16),
        "ep",
        scatter_dimension=0,
        tiled=True,
    ).astype(jnp.float32)
    dense_gate_pre, dense_up_pre = jnp.split(dense_pre, 2, axis=1)
    dense_hidden = (jax.nn.silu(dense_gate_pre) * dense_up_pre).astype(jnp.bfloat16)
    dense_partial = jnp.dot(
        dense_hidden,
        lax.all_gather(w_dense_down, "ep", axis=1, tiled=True),
        preferred_element_type=jnp.float32,
    )
    dense_out = lax.psum_scatter(
        dense_partial.astype(jnp.bfloat16), "tp", scatter_dimension=1, tiled=True
    ).astype(jnp.float32)
    mix_weight = jax.nn.sigmoid(jnp.dot(ffn_in, dense_mix, preferred_element_type=jnp.float32))
    ffn_out = expert_sum + mix_weight[:, None] * dense_out
    squares = lax.psum(jnp.sum(ffn_out * ffn_out, axis=1), "tp")
    out_scale = lax.rsqrt(squares / width + EPS)
    gain_part = lax.dynamic_slice_in_dim(norm_gains[3], column_index * part_width, part_width, 0)
    resid_part = lax.dynamic_slice_in_dim(after_mix, column_index * part_width, part_width, 1)
    layer_out = (resid_part + ffn_out * out_scale[:, None] * gain_part).astype(jnp.bfloat16)
    return (layer_out, new_state)


def dot32(a, b):
    return jnp.dot(a, b, preferred_element_type=jnp.float32)


def silu(x):
    return x * jax.nn.sigmoid(x)


MESH = pl.DeviceIdType.MESH


class Sems:
    def __init__(self):
        self.used = 0

    def take(self, count):
        first = self.used
        self.used += count
        return first


def chips_by_distance(q, half):
    if half == 4:
        return [q, q + 1 - 2 * lax.rem(q, 2), 2 - q // 2, 3 - 3 * (q // 2)]
    return [q] + [lax.rem(q + k, half) for k in range(1, half)]


CHUNKS = 2


def fused_layer(
    tokens,
    old_state,
    bounds,
    head_gain,
    norm_gains,
    in_weights,
    w_mix,
    routes,
    scores,
    experts,
    dense,
    mix_row,
    n_ep,
    n_tp,
):
    bf16, f32, i32 = jnp.bfloat16, jnp.float32, jnp.int32
    seqs, width = tokens.shape
    heads, hs = old_state.shape[1:3]
    block, part = width // n_ep, width // n_tp
    chans = heads * hs
    topk = routes.shape[1]
    cap = max(2, 2 * seqs * topk // n_ep)
    cells, rows = n_ep * cap, n_ep * seqs
    eff, dff = experts[0].shape[2], dense[0].shape[1]
    half, ratio = n_ep // 2, n_ep // n_tp
    duo = 2 * seqs
    lanes = 128
    tile = 128
    chunk = dff // CHUNKS

    send_at, recv_at = Sems(), Sems()

    def pair(count):
        return send_at.take(count), recv_at.take(count)

    P_TOK, P_ROUTE = pair(n_ep), pair(n_ep)
    P_PAIR, P_HEAD = pair(heads), pair(heads * half)
    P_MIX = pair(heads * n_ep)
    P_TP = pair(half * n_tp)
    P_STAT, P_OWN = pair(n_ep), pair(n_ep)
    P_DPAIR, P_DENSE = pair(CHUNKS), pair(CHUNKS * half)
    P_EXP = pair(n_ep)
    P_RTP, P_RET = pair(n_tp), pair(n_ep)
    P_GATH, P_HAND = pair(CHUNKS * (half + 1)), pair(CHUNKS * (half + 1))
    P_COLS = send_at.take(n_ep), recv_at.take(ratio * n_tp)
    P_SQ = pair(n_tp)
    n_load = 16 + 4 * heads + 2 * CHUNKS + 2 * (eff // tile)

    def kernel(
        tok_h, st_h, lb_h, hg_h, gn_h, wq_h, wf_h, wv_h, wo_h, wm_h, rt_h, sc_h,
        eg_h, eu_h, ed_h, dg_h, du_h, dd_h, mr_h,
        out, ns,
        tok, st, lb, hg, gn, win, wm, rt0, sc, wgu, wed, wd, wdd, mrow,
        R, RT, X, Y, Z, PR, rd, MA, TX, TR, MV, STAT, SX, SR, COL, OWN, SEL, MO, MR,
        DX, DY, DZ, DR, DH, OX, ER, hid, RX, RR, RB, RG, dd, ddr, sq, sqr,
        send, recv, lsem,
    ):
        me_e, me_t = lax.axis_index("ep"), lax.axis_index("tp")
        q, c = me_e // 2, lax.rem(me_e, 2)
        partner = 2 * q + 1 - c
        chips = chips_by_distance(q, half)
        away = chips[:0:-1]
        ep_peers = [(de, lax.rem(me_e + de, n_ep)) for de in range(1, n_ep)]
        tp_peers = [(dt, lax.rem(me_t + dt, n_tp)) for dt in range(1, n_tp)]

        barrier = pltpu.get_barrier_semaphore()
        for _, e in ep_peers:
            pl.semaphore_signal(barrier, inc=1, device_id=(e, me_t), device_id_type=MESH)
        for _, t in tp_peers:
            pl.semaphore_signal(barrier, inc=1, device_id=(me_e, t), device_id_type=MESH)

        count = [0]

        def load(src, dst):
            copy = pltpu.make_async_copy(src, dst, lsem.at[count[0]])
            count[0] += 1
            copy.start()
            return copy

        l_tok = load(tok_h, tok)
        l_gn = load(gn_h, gn)
        l_rt = load(rt_h, rt0)
        l_in = [
            [
                load(w.at[:, h * hs : (h + 1) * hs], win.at[h, :, i * hs : (i + 1) * hs])
                for i, w in enumerate((wq_h, wf_h, wv_h, wo_h))
            ]
            for h in range(heads)
        ]
        l_small = [load(lb_h, lb), load(hg_h, hg), load(sc_h, sc), load(mr_h, mrow)]
        l_st = load(st_h, st)
        l_wm = load(wm_h, wm)
        l_wd = [
            [
                load(w.at[:, j * chunk : (j + 1) * chunk], wd.at[j, :, i * chunk : (i + 1) * chunk])
                for i, w in enumerate((dg_h, du_h))
            ]
            for j in range(CHUNKS)
        ]
        l_exp = []
        for i in range(eff // tile):
            for k, w in enumerate((eg_h, eu_h)):
                at = (2 * i + k) * tile
                l_exp.append(load(w.at[0, :, i * tile : (i + 1) * tile], wgu.at[:, at : at + tile]))
        l_exp.append(load(ed_h.at[0], wed))
        l_wdd = load(dd_h, wdd)

        sent = []

        def put(src, dst, device, s, r):
            copy = pltpu.make_async_remote_copy(
                src_ref=src,
                dst_ref=dst,
                send_sem=send.at[s],
                recv_sem=recv.at[r],
                device_id=device,
                device_id_type=MESH,
            )
            copy.start()
            sent.append(copy.wait_send)

        def arrive(like, dst, r):
            pltpu.make_async_copy(like, dst, recv.at[r]).wait()

        def cut(first, size):
            return pl.ds(pl.multiple_of(first, 128), size)

        mine = cut(me_e * block, block)
        own_rows = pl.ds(pl.multiple_of(me_e * seqs, seqs), seqs)

        l_tok.wait()
        l_gn.wait()
        l_rt.wait()
        pl.semaphore_wait(barrier, n_ep + n_tp - 2)
        for de, e in ep_peers:
            put(tok.at[:, cut(e * block, block)], R.at[me_e], (e, me_t), P_TOK[0] + de, P_TOK[1] + de)
        for de, e in ep_peers:
            put(rt0, RT.at[me_e], (e, me_t), P_ROUTE[0] + de, P_ROUTE[1] + de)
        R[me_e] = tok[:, mine]
        RT[me_e] = rt0[...]
        resid = tok[...].astype(f32)
        scale0 = rms_scale(resid)
        g0 = gn[0:1, mine]
        g1 = gn[1:2, mine]
        g2 = gn[2:3, mine]
        for group in l_in:
            for copy in group:
                copy.wait()
        for de, _ in ep_peers:
            arrive(rt0, RT.at[0], P_ROUTE[1] + de)
            arrive(tok.at[:, 0:block], R.at[0], P_TOK[1] + de)

        scaled = (R[...].reshape(rows, block).astype(f32) * g0).astype(bf16)
        for h in range(heads):
            piece = dot32(scaled, win[h]).astype(bf16)
            for e in range(n_ep):
                X[h, e % 2, e // 2] = piece[e * seqs : (e + 1) * seqs]
            put(X.at[h, 1 - c], Y.at[h], (partner, me_t), P_PAIR[0] + h, P_PAIR[1] + h)
        for h in range(heads):
            arrive(X.at[h, 0], Y.at[h], P_PAIR[1] + h)
            for k, kk in enumerate(away):
                Z[h, kk] = (X[h, c, kk].astype(f32) + Y[h, kk].astype(f32)).astype(bf16)
                put(
                    Z.at[h, kk],
                    PR.at[h, q],
                    (2 * kk + c, me_t),
                    P_HEAD[0] + h * half + k,
                    P_HEAD[1] + h * half + q,
                )
            PR[h, q] = (X[h, c, q].astype(f32) + Y[h, q].astype(f32)).astype(bf16)

        named = RT[...].reshape(rows, topk)
        lane = lax.broadcasted_iota(i32, (rows, lanes), 1)
        row = lax.broadcasted_iota(i32, (rows, lanes), 0)
        ones = [(lane == named[:, k : k + 1]).astype(f32) for k in range(topk)]
        earlier = ((lane < row) & (lane >= (row // seqs) * seqs)).astype(bf16)
        before = dot32(earlier, sum(ones).astype(bf16))
        slots = [
            jnp.sum(o * before, axis=1, keepdims=True).astype(i32) for o in ones
        ]
        spot = lax.broadcasted_iota(i32, (rows, 1), 0) // seqs
        wide = lax.broadcasted_iota(i32, (rows, n_ep * cells), 1)
        chosen = jnp.zeros((rows, n_ep * cells), f32)
        for k in range(topk):
            place = named[:, k : k + 1] * cells + spot * cap + slots[k]
            chosen = chosen + (wide == place).astype(f32)
        for i in range(n_ep * cells // lanes):
            SEL[i * lanes : (i + 1) * lanes, :] = chosen[:, i * lanes : (i + 1) * lanes].T.astype(bf16)
        ours = jnp.zeros((rows, lanes), i32)
        for k in range(topk):
            ours = ours + jnp.where(lane == k, named[:, k : k + 1] * cap + slots[k], 0)
        OWN[...] = ours
        for copy in l_small:
            copy.wait()
        at_own = OWN[own_rows, :]
        spread = lax.broadcasted_iota(i32, (seqs, cells), 1)
        gap = sc[:, 0:1] - sc[:, 1:2]
        table = jnp.where(spread == at_own[:, 0:1], jax.nn.sigmoid(gap), 0.0)
        table = table + jnp.where(spread == at_own[:, 1:2], jax.nn.sigmoid(-gap), 0.0)

        l_st.wait()
        for h in range(heads):
            for kk in chips[1:]:
                arrive(Z.at[h, 0], PR.at[h, 0], P_HEAD[1] + h * half + kk)
            total = PR[h, 0].astype(f32)
            for kk in range(1, half):
                total = total + PR[h, kk].astype(f32)
            total = total * scale0
            at = slice(h * hs, (h + 1) * hs)
            bound = lb[0:1, at]
            raw = total[:, hs : 2 * hs]
            forget = bound + (1.0 - bound) * jax.nn.sigmoid(raw)
            key_in = (1.0 - bound) * jax.nn.sigmoid(-raw)
            query = silu(total[:, 0:hs])
            value = total[:, 2 * hs : 3 * hs]
            columns = jnp.concatenate(
                [forget, key_in, query, jnp.zeros((hs - 3 * seqs, hs), f32)], axis=0
            ).T
            for s in range(seqs):
                new = (
                    columns[:, s : s + 1] * st[s, h]
                    + columns[:, seqs + s : seqs + s + 1] * value[s : s + 1, :]
                )
                ns[s, h] = new
                rd[s : s + 1, :] = jnp.sum(
                    columns[:, 2 * seqs + s : 2 * seqs + s + 1] * new, axis=0, keepdims=True
                )
            read = rd[...]
            gated = read * rms_scale(read) * hg[0:1, at] * silu(total[:, 3 * hs :])
            MA[h, me_e] = gated.astype(bf16)
            for de, e in ep_peers:
                put(
                    MA.at[h, me_e],
                    MA.at[h, me_e],
                    (e, me_t),
                    P_MIX[0] + h * n_ep + de,
                    P_MIX[1] + h * n_ep + me_e,
                )

        l_wm.wait()
        for g, kk in enumerate(chips):
            for e in (2 * kk, 2 * kk + 1):
                if g == 0:
                    continue
                for h in range(heads):
                    arrive(MA.at[h, 0], MA.at[h, 1], P_MIX[1] + h * n_ep + e)
            if g == 0:
                for h in range(heads):
                    arrive(MA.at[h, 0], MA.at[h, 1], P_MIX[1] + h * n_ep + partner)
            lhs = jnp.concatenate(
                [MA[h, pl.ds(2 * kk, 2)].reshape(duo, hs) for h in range(heads)], axis=1
            )
            piece = dot32(lhs, wm[...]).astype(bf16)
            TX[kk] = piece
            TR[me_t, kk] = piece
            for dt, t in tp_peers:
                put(
                    TX.at[kk],
                    TR.at[me_t, kk],
                    (me_e, t),
                    P_TP[0] + g * n_tp + dt,
                    P_TP[1] + kk * n_tp + me_t,
                )
        lane_duo = lax.broadcasted_iota(i32, (duo, lanes), 1)
        mixer = mrow[0:1, mine].astype(f32)
        for kk in chips:
            for _, t in tp_peers:
                arrive(TX.at[0], TR.at[0, 0], P_TP[1] + kk * n_tp + t)
            total = TR[0, kk].astype(f32)
            for t in range(1, n_tp):
                total = total + TR[t, kk].astype(f32)
            narrow = total.astype(bf16)
            MO[pl.ds(2 * kk, 2)] = narrow.reshape(2, seqs, block)
            mixed = narrow.astype(f32)
            MV[kk] = mixed
            base = R[pl.ds(2 * kk, 2)].reshape(duo, block).astype(f32)
            lifted = mixed * g1
            figures = (
                base * base,
                mixed * mixed,
                base * lifted,
                lifted * lifted,
                base * g2 * mixer,
                lifted * g2 * mixer,
            )
            stat = jnp.zeros((duo, lanes), f32)
            for i, figure in enumerate(figures):
                stat = stat + jnp.where(
                    lane_duo == i, jnp.sum(figure, axis=1, keepdims=True), 0.0
                )
            STAT[kk] = stat
        SX[...] = STAT[...].reshape(rows, lanes).T[0:8, :]
        SR[me_e] = SX[...]
        for de, e in ep_peers:
            put(SX, SR.at[me_e], (e, me_t), P_STAT[0] + de, P_STAT[1] + de)

        def send_own():
            for de, e in ep_peers:
                pltpu.make_async_remote_copy(
                    src_ref=MO.at[e],
                    dst_ref=MR.at[lax.rem(me_e, ratio)],
                    send_sem=send.at[P_OWN[0] + de],
                    recv_sem=recv.at[P_OWN[1] + lax.rem(me_e, ratio)],
                    device_id=(e, me_t),
                    device_id_type=MESH,
                ).start()
            MR[lax.rem(me_e, ratio)] = MO[me_e]

        def sent_own():
            for de, e in ep_peers:
                pltpu.make_async_remote_copy(
                    src_ref=MO.at[e],
                    dst_ref=MR.at[lax.rem(me_e, ratio)],
                    send_sem=send.at[P_OWN[0] + de],
                    recv_sem=recv.at[P_OWN[1] + lax.rem(me_e, ratio)],
                    device_id=(e, me_t),
                    device_id_type=MESH,
                ).wait_send()

        holds = me_e // ratio == me_t
        pl.when(holds)(send_own)

        for de, _ in ep_peers:
            arrive(SX, SR.at[0], P_STAT[1] + de)
        total = SR[0]
        for e in range(1, n_ep):
            total = total + SR[e]
        inv_mix = lax.rsqrt(total[1:2] / width + EPS)
        squares = total[0:1] + 2.0 * inv_mix * total[2:3] + inv_mix * inv_mix * total[3:4]
        inv_after = lax.rsqrt(jnp.maximum(squares, 0.0) / width + EPS)
        weight = jax.nn.sigmoid(inv_after * (total[4:5] + inv_mix * total[5:6]))
        back = jnp.where(row == 0, inv_mix, jnp.where(row == 1, inv_after, jnp.where(row == 2, weight, 0.0)))
        back = back.T
        COL[...] = back
        after = R[...].reshape(rows, block).astype(f32) + MV[...].reshape(rows, block) * back[:, 0:1] * g1
        ffn_in = (after * back[:, 1:2] * g2).astype(bf16)

        step = 256
        for j in range(CHUNKS):
            for copy in l_wd[j]:
                copy.wait()
            for a in range(0, 2 * chunk, step):
                piece = dot32(ffn_in, wd[j, :, a : a + step]).astype(bf16)
                for e in range(n_ep):
                    DX[j, e % 2, e // 2, :, a : a + step] = piece[e * seqs : (e + 1) * seqs]
            put(DX.at[j, 1 - c], DY.at[j], (partner, me_t), P_DPAIR[0] + j, P_DPAIR[1] + j)
            if j == 0:
                routed = dot32(SEL[...], ffn_in).astype(bf16)
                for e in range(n_ep):
                    OX[e] = routed[e * cells : (e + 1) * cells]
                for de, e in ep_peers:
                    put(OX.at[e], ER.at[:, mine], (e, me_t), P_EXP[0] + de, P_EXP[1] + de)
                ER[:, mine] = OX[me_e]
        for j in range(CHUNKS):
            arrive(DX.at[j, 0], DY.at[j], P_DPAIR[1] + j)
            for k, kk in enumerate(away):
                DZ[j, kk] = (DX[j, c, kk].astype(f32) + DY[j, kk].astype(f32)).astype(bf16)
                put(
                    DZ.at[j, kk],
                    DR.at[j, q],
                    (2 * kk + c, me_t),
                    P_DENSE[0] + j * half + k,
                    P_DENSE[1] + j * half + q,
                )
            DR[j, q] = (DX[j, c, q].astype(f32) + DY[j, q].astype(f32)).astype(bf16)

        for copy in l_exp:
            copy.wait()
        for de, _ in ep_peers:
            arrive(OX.at[0], ER.at[:, 0:block], P_EXP[1] + de)

        @pl.loop(0, eff // tile)
        def _(i):
            both = dot32(ER[...], wgu[:, cut(i * 2 * tile, 2 * tile)])
            hid[:, cut(i * tile, tile)] = (silu(both[:, :tile]) * both[:, tile:]).astype(bf16)

        for dt, t in tp_peers + [(0, me_t)]:
            piece = dot32(hid[...], wed[:, cut(t * part, part)]).astype(bf16)
            if dt:
                RX[dt] = piece
                put(RX.at[dt], RR.at[me_t], (me_e, t), P_RTP[0] + dt, P_RTP[1] + dt)
            else:
                RR[me_t] = piece

        def hidden(j):
            for kk in chips[1:]:
                arrive(DZ.at[j, 0], DR.at[j, 0], P_DENSE[1] + j * half + kk)
            for a in range(0, chunk, step):
                gate = DR[j, 0, :, a : a + step].astype(f32)
                up = DR[j, 0, :, chunk + a : chunk + a + step].astype(f32)
                for kk in range(1, half):
                    gate = gate + DR[j, kk, :, a : a + step].astype(f32)
                    up = up + DR[j, kk, :, chunk + a : chunk + a + step].astype(f32)
                DH[j, me_e, :, a : a + step] = (silu(gate) * up).astype(bf16)
            base = j * (half + 1)
            for k, kk in enumerate(away):
                put(
                    DH.at[j, me_e],
                    DH.at[j, me_e],
                    (2 * kk + c, me_t),
                    P_GATH[0] + base + k,
                    P_GATH[1] + base + q,
                )
            put(
                DH.at[j, me_e],
                DH.at[j, me_e],
                (partner, me_t),
                P_GATH[0] + base + half,
                P_GATH[1] + base + half,
            )

        def hand_over(j):
            base = j * (half + 1)
            for k, kk in enumerate(chips[1:]):
                arrive(DH.at[j, 0], DH.at[j, 1], P_GATH[1] + base + kk)
                here = DH.at[j, 2 * kk + c]
                put(here, here, (partner, me_t), P_HAND[0] + base + k, P_HAND[1] + base + kk)

        def gathered(j):
            base = j * (half + 1)
            arrive(DH.at[j, 0], DH.at[j, 1], P_GATH[1] + base + half)
            for kk in chips[1:]:
                arrive(DH.at[j, 0], DH.at[j, 1], P_HAND[1] + base + kk)
            return dot32(DH[j].reshape(rows, chunk), wdd[j * chunk : (j + 1) * chunk, :])

        def give_back():
            for dt, _ in tp_peers:
                arrive(RX.at[0], RR.at[0], P_RTP[1] + dt)
            total = RR[0].astype(f32)
            for t in range(1, n_tp):
                total = total + RR[t].astype(f32)
            total = total.astype(bf16)
            for e in range(n_ep):
                RB[e] = total[e * cap : (e + 1) * cap]
            RG[me_e] = RB[me_e]
            for de, e in ep_peers:
                put(RB.at[e], RG.at[me_e], (e, me_t), P_RET[0] + de, P_RET[1] + de)

        hidden(0)
        give_back()
        for j in range(1, CHUNKS):
            hidden(j)
        for j in range(CHUNKS):
            hand_over(j)
        l_wdd.wait()
        total = gathered(0)
        for j in range(1, CHUNKS):
            total = total + gathered(j)
        total = total.astype(bf16)
        for e in range(n_ep):
            dd[e] = total[e * seqs : (e + 1) * seqs]
        to = me_e // ratio
        slot = lax.rem(me_e, ratio) * n_tp + me_t
        landing = ddr.at[lax.rem(me_e, ratio), me_t]
        for de in range(n_ep):
            e = lax.rem(me_e + de, n_ep)
            remote = pltpu.make_async_remote_copy(
                src_ref=dd.at[e],
                dst_ref=landing,
                send_sem=send.at[P_COLS[0] + de],
                recv_sem=recv.at[P_COLS[1] + slot],
                device_id=(e, to),
                device_id_type=MESH,
            )
            if de == 0:
                own = pltpu.make_async_copy(dd.at[e], landing, recv.at[P_COLS[1] + slot])
                pl.when(to == me_t)(own.start)
                pl.when(to != me_t)(remote.start)
                sent.append(lambda remote=remote: pl.when(to != me_t)(remote.wait_send))
            else:
                remote.start()
                sent.append(remote.wait_send)

        for de, _ in ep_peers:
            arrive(RB.at[0], RG.at[0], P_RET[1] + de)
        expert_sum = jnp.dot(
            table,
            RG[...].astype(f32).reshape(cells, part),
            precision=lax.Precision.HIGHEST,
            preferred_element_type=f32,
        )
        own_cols = COL[own_rows, :]
        part_at = cut(me_t * part, part)
        for j in range(ratio):
            source = me_t * ratio + j

            def wait_own(j=j):
                arrive(MO.at[0], MR.at[j], P_OWN[1] + j)

            pl.when(source != me_e)(wait_own)
        mix_own = jnp.concatenate([MR[j].astype(f32) for j in range(ratio)], axis=1)
        after_own = tok[:, part_at].astype(f32) + mix_own * own_cols[:, 0:1] * gn[1:2, part_at]
        for i in range(ratio * n_tp):
            arrive(dd.at[0], ddr.at[i // n_tp, i % n_tp], P_COLS[1] + i)
        pieces = []
        for j in range(ratio):
            total = ddr[j, 0].astype(f32)
            for t in range(1, n_tp):
                total = total + ddr[j, t].astype(f32)
            pieces.append(total)
        ffn_out = expert_sum + own_cols[:, 2:3] * jnp.concatenate(pieces, axis=1)
        mass = jnp.sum(ffn_out * ffn_out, axis=1, keepdims=True)
        sq[...] = jnp.broadcast_to(mass, (seqs, lanes))
        sqr[me_t] = sq[...]
        for dt, t in tp_peers:
            put(sq, sqr.at[me_t], (me_e, t), P_SQ[0] + dt, P_SQ[1] + dt)
        for dt, _ in tp_peers:
            arrive(sq, sqr.at[0], P_SQ[1] + dt)
        total = sqr[0]
        for t in range(1, n_tp):
            total = total + sqr[t]
        scale = lax.rsqrt(total[:, 0:1] / width + EPS)
        out[...] = (after_own + ffn_out * scale * gn[3:4, part_at]).astype(bf16)
        pl.when(holds)(sent_own)
        for wait in sent:
            wait()

    vmem = pl.BlockSpec(memory_space=pltpu.VMEM)
    hbm = pl.BlockSpec(memory_space=pltpu.HBM)
    b = lambda *s: pltpu.VMEM(s, bf16)
    f = lambda *s: pltpu.VMEM(s, f32)
    n = lambda *s: pltpu.VMEM(s, i32)
    return pl.pallas_call(
        kernel,
        out_shape=(
            jax.ShapeDtypeStruct((seqs, part), bf16),
            jax.ShapeDtypeStruct(old_state.shape, f32),
        ),
        in_specs=[hbm] * 19,
        out_specs=(vmem, vmem),
        scratch_shapes=[
            b(seqs, width),
            f(*old_state.shape),
            f(1, chans),
            f(1, chans),
            f(*norm_gains.shape),
            b(heads, block, 4 * hs),
            b(chans, block),
            n(seqs, topk),
            f(seqs, topk),
            b(width, 2 * eff),
            b(eff, width),
            b(CHUNKS, block, 2 * chunk),
            b(dff, block),
            b(1, width),
            b(n_ep, seqs, block),
            n(n_ep, seqs, topk),
            b(heads, 2, half, seqs, 4 * hs),
            b(heads, half, seqs, 4 * hs),
            b(heads, half, seqs, 4 * hs),
            b(heads, half, seqs, 4 * hs),
            f(seqs, hs),
            b(heads, n_ep, seqs, hs),
            b(half, duo, block),
            b(n_tp, half, duo, block),
            f(half, duo, block),
            f(half, duo, lanes),
            f(8, lanes),
            f(n_ep, 8, lanes),
            f(rows, lanes),
            n(rows, lanes),
            b(n_ep * cells, rows),
            b(n_ep, seqs, block),
            b(ratio, seqs, block),
            b(CHUNKS, 2, half, seqs, 2 * chunk),
            b(CHUNKS, half, seqs, 2 * chunk),
            b(CHUNKS, half, seqs, 2 * chunk),
            b(CHUNKS, half, seqs, 2 * chunk),
            b(CHUNKS, n_ep, seqs, chunk),
            b(n_ep, cells, block),
            b(cells, width),
            b(cells, eff),
            b(n_tp, cells, part),
            b(n_tp, cells, part),
            b(n_ep, cap, part),
            b(n_ep, cap, part),
            b(n_ep, seqs, block),
            b(ratio, n_tp, seqs, block),
            f(seqs, lanes),
            f(n_tp, seqs, lanes),
            pltpu.SemaphoreType.DMA((send_at.used,)),
            pltpu.SemaphoreType.DMA((recv_at.used,)),
            pltpu.SemaphoreType.DMA((n_load,)),
        ],
        compiler_params=pltpu.CompilerParams(
            collective_id=1, has_side_effects=True, vmem_limit_bytes=48 * 1024 * 1024
        ),
        name="fused_layer",
    )(
        tokens,
        old_state,
        bounds,
        head_gain,
        norm_gains,
        *in_weights,
        w_mix,
        routes,
        scores,
        *experts,
        *dense,
        mix_row,
    )


def fast_body(
    tokens,
    old_state,
    lower_bound,
    head_gain,
    norm_gains,
    w_query,
    w_forget,
    w_value,
    w_outgate,
    w_mix_out,
    routes,
    route_scores,
    w_exp_gate,
    w_exp_up,
    w_exp_down,
    w_dense_gate,
    w_dense_up,
    w_dense_down,
    dense_mix,
):
    return fused_layer(
        tokens,
        old_state,
        lower_bound[None, :],
        head_gain[None, :],
        norm_gains,
        (w_query, w_forget, w_value, w_outgate),
        w_mix_out,
        routes,
        route_scores,
        (w_exp_gate, w_exp_up, w_exp_down),
        (w_dense_gate, w_dense_up, w_dense_down),
        dense_mix[None, :],
        lax.axis_size("ep"),
        lax.axis_size("tp"),
    )


def solution(mesh):
    n_ep, n_tp = mesh.shape['ep'], mesh.shape['tp']
    fits = n_ep % n_tp == 0 and n_ep % 2 == 0 and n_ep * n_tp <= 64
    return jax.shard_map(
        fast_body if fits else body,
        mesh=mesh,
        in_specs=(
            P("ep", None),
            P("ep", "tp", None, None),
            P("tp"),
            P("tp"),
            P(),
            P("ep", "tp"),
            P("ep", "tp"),
            P("ep", "tp"),
            P("ep", "tp"),
            P("tp", "ep"),
            P("ep", None),
            P("ep", None),
            P("ep", None, "tp"),
            P("ep", None, "tp"),
            P("ep", "tp", None),
            P("ep", "tp"),
            P("ep", "tp"),
            P("tp", "ep"),
            P(),
        ),
        out_specs=(P("ep", "tp"), P("ep", "tp", None, None)),
        check_vma=False,
    )
```

```python
import jax
import jax.numpy as jnp
from jax import lax
from jax.experimental import pallas as pl
from jax.experimental.pallas import tpu as pltpu
from jax.sharding import PartitionSpec as P

EPS = 1e-06


def rms_scale(values):
    return lax.rsqrt(jnp.mean(values * values, axis=-1, keepdims=True) + EPS)


def body(
    tokens,
    old_state,
    lower_bound,
    head_gain,
    norm_gains,
    w_query,
    w_forget,
    w_value,
    w_outgate,
    w_mix_out,
    routes,
    route_scores,
    w_exp_gate,
    w_exp_up,
    w_exp_down,
    w_dense_gate,
    w_dense_up,
    w_dense_down,
    dense_mix,
):
    highest = lax.Precision.HIGHEST
    seqs, width = tokens.shape
    column_index = lax.axis_index("tp")
    part_width = width // lax.axis_size("tp")
    resid = tokens.astype(jnp.float32)
    normed = (resid * rms_scale(resid) * norm_gains[0]).astype(jnp.bfloat16)
    in_weights = jnp.concatenate([w_query, w_forget, w_value, w_outgate], axis=1)
    mix_rows = lax.all_to_all(normed, "ep", split_axis=1, concat_axis=0, tiled=True)
    projected = lax.psum_scatter(
        jnp.dot(mix_rows, in_weights, preferred_element_type=jnp.float32).astype(jnp.bfloat16),
        "ep",
        scatter_dimension=0,
        tiled=True,
    ).astype(jnp.float32)
    query_raw, forget_raw, value, out_gate = jnp.split(projected, 4, axis=1)
    heads = old_state.shape[1]
    head_size = old_state.shape[2]
    shape_heads = (seqs, heads, head_size)
    forget = lower_bound + (1.0 - lower_bound) * jax.nn.sigmoid(forget_raw)
    key_in = (1.0 - lower_bound) * jax.nn.sigmoid(-forget_raw)
    new_state = forget.reshape(shape_heads)[..., None] * old_state + key_in.reshape(shape_heads)[
        ..., None
    ] * value.reshape(seqs, heads, 1, head_size)
    query = jax.nn.silu(query_raw).reshape(shape_heads)
    read = jnp.einsum("thk,thkv->thv", query, new_state, precision=highest)
    gated = (
        read
        * rms_scale(read)
        * head_gain.reshape(heads, head_size)
        * jax.nn.silu(out_gate).reshape(shape_heads)
    )
    mixed_heads = gated.reshape(seqs, heads * head_size).astype(jnp.bfloat16)
    mix_part = jnp.dot(
        mixed_heads,
        lax.all_gather(w_mix_out, "ep", axis=1, tiled=True),
        preferred_element_type=jnp.float32,
    ).astype(jnp.bfloat16)
    mix_part = lax.optimization_barrier(mix_part).astype(jnp.float32)
    mix_out = lax.psum(mix_part.astype(jnp.bfloat16), "tp")
    mix_wide = lax.optimization_barrier(mix_out).astype(jnp.float32)
    after_mix = resid + mix_wide * rms_scale(mix_wide) * norm_gains[1]
    ffn_in = (after_mix * rms_scale(after_mix) * norm_gains[2]).astype(jnp.bfloat16)
    experts = lax.axis_size("ep")
    topk = routes.shape[1]
    capacity = max(2, 2 * seqs * topk // experts)
    flat_routes = routes.reshape(-1)
    onehot = (flat_routes[:, None] == jnp.arange(experts, dtype=jnp.int32)[None, :]).astype(
        jnp.int32
    )
    before = jnp.cumsum(onehot, axis=0) - onehot
    slots = jnp.sum(onehot * before, axis=1)
    cells = flat_routes * capacity + slots
    placed = cells[None, :] == jnp.arange(experts * capacity, dtype=jnp.int32)[:, None]
    repeated = jnp.repeat(ffn_in, topk, axis=0)
    outgoing = jnp.dot(placed.astype(jnp.bfloat16), repeated, preferred_element_type=jnp.float32)
    outgoing = outgoing.astype(jnp.bfloat16).reshape(experts, capacity, width)
    arrived = lax.all_to_all(outgoing, "ep", split_axis=0, concat_axis=0, tiled=True)
    sources, items, _ = arrived.shape
    expert_rows = arrived.reshape(sources * items, width)
    gate_pre = jnp.dot(expert_rows, w_exp_gate[0], preferred_element_type=jnp.float32)
    up_pre = jnp.dot(expert_rows, w_exp_up[0], preferred_element_type=jnp.float32)
    hidden = (jax.nn.silu(gate_pre) * up_pre).astype(jnp.bfloat16)
    partial_rows = jnp.dot(hidden, w_exp_down[0], preferred_element_type=jnp.float32).astype(
        jnp.bfloat16
    )
    partial_rows = lax.optimization_barrier(partial_rows).astype(jnp.float32)
    partial_rows = partial_rows.reshape(sources, items, width)
    summed = lax.psum_scatter(
        partial_rows.astype(jnp.bfloat16), "tp", scatter_dimension=2, tiled=True
    )
    returned = lax.all_to_all(summed, "ep", split_axis=0, concat_axis=0, tiled=True)
    first = jax.nn.sigmoid(route_scores[:, 0] - route_scores[:, 1])
    second = jax.nn.sigmoid(route_scores[:, 1] - route_scores[:, 0])
    route_weight = jnp.stack([first, second], axis=1).reshape(-1)
    weight_table = jnp.sum(
        (placed.astype(jnp.float32) * route_weight[None, :]).reshape(
            experts * capacity, seqs, topk
        ),
        axis=2,
    )
    expert_sum = jnp.dot(
        weight_table.T,
        returned.reshape(experts * capacity, part_width).astype(jnp.float32),
        precision=highest,
    )
    dense_weights = jnp.concatenate([w_dense_gate, w_dense_up], axis=1)
    dense_rows = lax.all_to_all(ffn_in, "ep", split_axis=1, concat_axis=0, tiled=True)
    dense_pre = lax.psum_scatter(
        jnp.dot(dense_rows, dense_weights, preferred_element_type=jnp.float32).astype(jnp.bfloat16),
        "ep",
        scatter_dimension=0,
        tiled=True,
    ).astype(jnp.float32)
    dense_gate_pre, dense_up_pre = jnp.split(dense_pre, 2, axis=1)
    dense_hidden = (jax.nn.silu(dense_gate_pre) * dense_up_pre).astype(jnp.bfloat16)
    dense_partial = jnp.dot(
        dense_hidden,
        lax.all_gather(w_dense_down, "ep", axis=1, tiled=True),
        preferred_element_type=jnp.float32,
    )
    dense_out = lax.psum_scatter(
        dense_partial.astype(jnp.bfloat16), "tp", scatter_dimension=1, tiled=True
    ).astype(jnp.float32)
    mix_weight = jax.nn.sigmoid(jnp.dot(ffn_in, dense_mix, preferred_element_type=jnp.float32))
    ffn_out = expert_sum + mix_weight[:, None] * dense_out
    squares = lax.psum(jnp.sum(ffn_out * ffn_out, axis=1), "tp")
    out_scale = lax.rsqrt(squares / width + EPS)
    gain_part = lax.dynamic_slice_in_dim(norm_gains[3], column_index * part_width, part_width, 0)
    resid_part = lax.dynamic_slice_in_dim(after_mix, column_index * part_width, part_width, 1)
    layer_out = (resid_part + ffn_out * out_scale[:, None] * gain_part).astype(jnp.bfloat16)
    return (layer_out, new_state)


def dot32(a, b):
    return jnp.dot(a, b, preferred_element_type=jnp.float32)


def silu(x):
    return x * jax.nn.sigmoid(x)


MESH = pl.DeviceIdType.MESH


class Sems:
    def __init__(self):
        self.used = 0

    def take(self, count):
        first = self.used
        self.used += count
        return first


def chips_by_distance(q, half):
    if half == 4:
        return [q, q + 1 - 2 * lax.rem(q, 2), 2 - q // 2, 3 - 3 * (q // 2)]
    return [q] + [lax.rem(q + k, half) for k in range(1, half)]


CHUNKS = 2


def fused_layer(
    tokens,
    old_state,
    bounds,
    head_gain,
    norm_gains,
    in_weights,
    w_mix,
    routes,
    scores,
    experts,
    dense,
    mix_row,
    n_ep,
    n_tp,
):
    bf16, f32, i32 = jnp.bfloat16, jnp.float32, jnp.int32
    seqs, width = tokens.shape
    heads, hs = old_state.shape[1:3]
    block, part = width // n_ep, width // n_tp
    chans = heads * hs
    topk = routes.shape[0]
    cap = max(2, 2 * seqs * topk // n_ep)
    cells, rows = n_ep * cap, n_ep * seqs
    eff, dff = experts[0].shape[2], dense[0].shape[1]
    half, ratio = n_ep // 2, n_ep // n_tp
    duo = 2 * seqs
    lanes = 128
    tile = 128
    chunk = dff // CHUNKS

    send_at, recv_at = Sems(), Sems()

    def pair(count):
        return send_at.take(count), recv_at.take(count)

    P_TOK, P_ROUTE = pair(n_ep), pair(n_ep)
    P_PAIR, P_HEAD = pair(heads), pair(heads * half)
    P_MIX = pair(heads * n_ep)
    P_TP = pair(half * n_tp)
    P_STAT, P_OWN = pair(n_ep), pair(n_ep)
    P_DPAIR, P_DENSE = pair(CHUNKS), pair(CHUNKS * half)
    P_EXP = pair(n_ep)
    P_RTP, P_RET = pair(n_tp), pair(n_ep)
    P_GATH, P_HAND = pair(CHUNKS * (half + 1)), pair(CHUNKS * (half + 1))
    P_COLS = send_at.take(n_ep), recv_at.take(ratio * n_tp)
    P_SQ = pair(n_tp)
    n_load = 16 + 4 * heads + 2 * CHUNKS + 2 * (eff // tile)

    def kernel(
        tok_h, st_h, lb_h, hg_h, gn_h, wq_h, wf_h, wv_h, wo_h, wm_h, rt_h, sc_h,
        eg_h, eu_h, ed_h, dg_h, du_h, dd_h, mr_h,
        out, ns,
        tok, st, lb, hg, gn, win, wm, rt0, sc, wgu, wed, wd, wdd, mrow, wide_row,
        R, RT, X, Y, Z, PR, rd, MA, TX, TR, MV, STAT, SX, SR, COL, OWN, SEL, MO, MR,
        DX, DY, DZ, DR, DH, OX, ER, hid, RX, RR, RB, RG, dd, ddr, sq, sqr,
        send, recv, lsem,
    ):
        me_e, me_t = lax.axis_index("ep"), lax.axis_index("tp")
        q, c = me_e // 2, lax.rem(me_e, 2)
        partner = 2 * q + 1 - c
        chips = chips_by_distance(q, half)
        away = chips[:0:-1]
        ep_peers = [(de, lax.rem(me_e + de, n_ep)) for de in range(1, n_ep)]
        tp_peers = [(dt, lax.rem(me_t + dt, n_tp)) for dt in range(1, n_tp)]

        barrier = pltpu.get_barrier_semaphore()
        for _, e in ep_peers:
            pl.semaphore_signal(barrier, inc=1, device_id=(e, me_t), device_id_type=MESH)
        for _, t in tp_peers:
            pl.semaphore_signal(barrier, inc=1, device_id=(me_e, t), device_id_type=MESH)

        count = [0]

        def load(src, dst):
            copy = pltpu.make_async_copy(src, dst, lsem.at[count[0]])
            count[0] += 1
            copy.start()
            return copy

        l_tok = load(tok_h, tok)
        l_gn = load(gn_h, gn)
        l_rt = load(rt_h, rt0)
        l_in = [
            [
                load(w.at[:, h * hs : (h + 1) * hs], win.at[h, :, i * hs : (i + 1) * hs])
                for i, w in enumerate((wq_h, wf_h, wv_h, wo_h))
            ]
            for h in range(heads)
        ]
        l_small = [load(lb_h, lb), load(hg_h, hg), load(sc_h, sc), load(mr_h, mrow)]
        l_st = load(st_h, st)
        l_wm = load(wm_h, wm)
        l_wd = [
            [
                load(w.at[:, j * chunk : (j + 1) * chunk], wd.at[j, :, i * chunk : (i + 1) * chunk])
                for i, w in enumerate((dg_h, du_h))
            ]
            for j in range(CHUNKS)
        ]
        l_exp = []
        for i in range(eff // tile):
            for k, w in enumerate((eg_h, eu_h)):
                at = (2 * i + k) * tile
                l_exp.append(load(w.at[0, :, i * tile : (i + 1) * tile], wgu.at[:, at : at + tile]))
        l_exp.append(load(ed_h.at[0], wed))
        l_wdd = load(dd_h, wdd)

        sent = []

        def put(src, dst, device, s, r):
            copy = pltpu.make_async_remote_copy(
                src_ref=src,
                dst_ref=dst,
                send_sem=send.at[s],
                recv_sem=recv.at[r],
                device_id=device,
                device_id_type=MESH,
            )
            copy.start()
            sent.append(copy.wait_send)

        def arrive(like, dst, r):
            pltpu.make_async_copy(like, dst, recv.at[r]).wait()

        def cut(first, size):
            return pl.ds(pl.multiple_of(first, 128), size)

        mine = cut(me_e * block, block)
        own_rows = pl.ds(pl.multiple_of(me_e * seqs, seqs), seqs)

        l_tok.wait()
        l_gn.wait()
        l_rt.wait()
        pl.semaphore_wait(barrier, n_ep + n_tp - 2)
        for de, e in ep_peers:
            put(tok.at[:, cut(e * block, block)], R.at[me_e], (e, me_t), P_TOK[0] + de, P_TOK[1] + de)
        for de, e in ep_peers:
            put(rt0, RT.at[me_e], (e, me_t), P_ROUTE[0] + de, P_ROUTE[1] + de)
        R[me_e] = tok[:, mine]
        RT[me_e] = rt0[...]
        resid = tok[...].astype(f32)
        scale0 = rms_scale(resid)
        g0 = gn[0:1, mine]
        g1 = gn[1:2, mine]
        g2 = gn[2:3, mine]
        for group in l_in:
            for copy in group:
                copy.wait()
        for de, _ in ep_peers:
            arrive(rt0, RT.at[0], P_ROUTE[1] + de)
            arrive(tok.at[:, 0:block], R.at[0], P_TOK[1] + de)

        scaled = (R[...].reshape(rows, block).astype(f32) * g0).astype(bf16)
        for h in range(heads):
            piece = dot32(scaled, win[h]).astype(bf16)
            for e in range(n_ep):
                X[h, e % 2, e // 2] = piece[e * seqs : (e + 1) * seqs]
            put(X.at[h, 1 - c], Y.at[h], (partner, me_t), P_PAIR[0] + h, P_PAIR[1] + h)
        for h in range(heads):
            arrive(X.at[h, 0], Y.at[h], P_PAIR[1] + h)
            for k, kk in enumerate(away):
                Z[h, kk] = (X[h, c, kk].astype(f32) + Y[h, kk].astype(f32)).astype(bf16)
                put(
                    Z.at[h, kk],
                    PR.at[h, q],
                    (2 * kk + c, me_t),
                    P_HEAD[0] + h * half + k,
                    P_HEAD[1] + h * half + q,
                )
            PR[h, q] = (X[h, c, q].astype(f32) + Y[h, q].astype(f32)).astype(bf16)

        short = lax.broadcasted_iota(i32, (rows, seqs), 1)
        turn = lax.broadcasted_iota(i32, (rows, seqs), 0)
        diagonal = short == turn - (turn // seqs) * seqs
        named = []
        for k in range(topk):
            across = jnp.concatenate(
                [jnp.broadcast_to(RT[e, k : k + 1, :], (seqs, seqs)) for e in range(n_ep)], axis=0
            )
            named.append(jnp.sum(jnp.where(diagonal, across, 0), axis=1, keepdims=True))
        lane = lax.broadcasted_iota(i32, (rows, lanes), 1)
        row = lax.broadcasted_iota(i32, (rows, lanes), 0)
        ones = [(lane == named[k]).astype(f32) for k in range(topk)]
        earlier = ((lane < row) & (lane >= (row // seqs) * seqs)).astype(bf16)
        before = dot32(earlier, sum(ones).astype(bf16))
        slots = [
            jnp.sum(o * before, axis=1, keepdims=True).astype(i32) for o in ones
        ]
        spot = lax.broadcasted_iota(i32, (rows, 1), 0) // seqs
        wide = lax.broadcasted_iota(i32, (rows, n_ep * cells), 1)
        chosen = jnp.zeros((rows, n_ep * cells), f32)
        for k in range(topk):
            place = named[k] * cells + spot * cap + slots[k]
            chosen = chosen + (wide == place).astype(f32)
        for i in range(n_ep * cells // lanes):
            SEL[i * lanes : (i + 1) * lanes, :] = chosen[:, i * lanes : (i + 1) * lanes].T.astype(bf16)
        ours = jnp.zeros((rows, lanes), i32)
        for k in range(topk):
            ours = ours + jnp.where(lane == k, named[k] * cap + slots[k], 0)
        OWN[...] = ours
        for copy in l_small:
            copy.wait()
        wide_row[...] = mrow[...].astype(f32)
        at_own = OWN[own_rows, :]
        spread = lax.broadcasted_iota(i32, (seqs, cells), 1)
        gap = jnp.sum(
            jnp.where(diagonal[0:seqs], jnp.broadcast_to(sc[0:1, :] - sc[1:2, :], (seqs, seqs)), 0.0),
            axis=1,
            keepdims=True,
        )
        table = jnp.where(spread == at_own[:, 0:1], jax.nn.sigmoid(gap), 0.0)
        table = table + jnp.where(spread == at_own[:, 1:2], jax.nn.sigmoid(-gap), 0.0)

        l_st.wait()
        for h in range(heads):
            for kk in chips[1:]:
                arrive(Z.at[h, 0], PR.at[h, 0], P_HEAD[1] + h * half + kk)
            total = PR[h, 0].astype(f32)
            for kk in range(1, half):
                total = total + PR[h, kk].astype(f32)
            total = total * scale0
            at = slice(h * hs, (h + 1) * hs)
            bound = lb[0:1, at]
            raw = total[:, hs : 2 * hs]
            forget = bound + (1.0 - bound) * jax.nn.sigmoid(raw)
            key_in = (1.0 - bound) * jax.nn.sigmoid(-raw)
            query = silu(total[:, 0:hs])
            value = total[:, 2 * hs : 3 * hs]
            columns = jnp.concatenate(
                [forget, key_in, query, jnp.zeros((hs - 3 * seqs, hs), f32)], axis=0
            ).T
            for s in range(seqs):
                new = (
                    columns[:, s : s + 1] * st[s, h]
                    + columns[:, seqs + s : seqs + s + 1] * value[s : s + 1, :]
                )
                ns[s, h] = new
                rd[s : s + 1, :] = jnp.sum(
                    columns[:, 2 * seqs + s : 2 * seqs + s + 1] * new, axis=0, keepdims=True
                )
            read = rd[...]
            gated = read * rms_scale(read) * hg[0:1, at] * silu(total[:, 3 * hs :])
            MA[h, me_e] = gated.astype(bf16)
            for de, e in ep_peers:
                put(
                    MA.at[h, me_e],
                    MA.at[h, me_e],
                    (e, me_t),
                    P_MIX[0] + h * n_ep + de,
                    P_MIX[1] + h * n_ep + me_e,
                )

        l_wm.wait()
        for g, kk in enumerate(chips):
            for e in (2 * kk, 2 * kk + 1):
                if g == 0:
                    continue
                for h in range(heads):
                    arrive(MA.at[h, 0], MA.at[h, 1], P_MIX[1] + h * n_ep + e)
            if g == 0:
                for h in range(heads):
                    arrive(MA.at[h, 0], MA.at[h, 1], P_MIX[1] + h * n_ep + partner)
            lhs = jnp.concatenate(
                [MA[h, pl.ds(2 * kk, 2)].reshape(duo, hs) for h in range(heads)], axis=1
            )
            piece = dot32(lhs, wm[...]).astype(bf16)
            TX[kk] = piece
            TR[me_t, kk] = piece
            for dt, t in tp_peers:
                put(
                    TX.at[kk],
                    TR.at[me_t, kk],
                    (me_e, t),
                    P_TP[0] + g * n_tp + dt,
                    P_TP[1] + kk * n_tp + me_t,
                )
        lane_duo = lax.broadcasted_iota(i32, (duo, lanes), 1)
        mixer = jnp.concatenate(
            [
                wide_row[pl.ds(me_e * (block // lanes) + i, 1), :]
                for i in range(block // lanes)
            ],
            axis=1,
        )
        for kk in chips:
            for _, t in tp_peers:
                arrive(TX.at[0], TR.at[0, 0], P_TP[1] + kk * n_tp + t)
            total = TR[0, kk].astype(f32)
            for t in range(1, n_tp):
                total = total + TR[t, kk].astype(f32)
            narrow = total.astype(bf16)
            MO[pl.ds(2 * kk, 2)] = narrow.reshape(2, seqs, block)
            mixed = narrow.astype(f32)
            MV[kk] = mixed
            base = R[pl.ds(2 * kk, 2)].reshape(duo, block).astype(f32)
            lifted = mixed * g1
            figures = (
                base * base,
                mixed * mixed,
                base * lifted,
                lifted * lifted,
                base * g2 * mixer,
                lifted * g2 * mixer,
            )
            stat = jnp.zeros((duo, lanes), f32)
            for i, figure in enumerate(figures):
                stat = stat + jnp.where(
                    lane_duo == i, jnp.sum(figure, axis=1, keepdims=True), 0.0
                )
            STAT[kk] = stat
        SX[...] = STAT[...].reshape(rows, lanes).T[0:8, :]
        SR[me_e] = SX[...]
        for de, e in ep_peers:
            put(SX, SR.at[me_e], (e, me_t), P_STAT[0] + de, P_STAT[1] + de)

        def send_own():
            for de, e in ep_peers:
                pltpu.make_async_remote_copy(
                    src_ref=MO.at[e],
                    dst_ref=MR.at[lax.rem(me_e, ratio)],
                    send_sem=send.at[P_OWN[0] + de],
                    recv_sem=recv.at[P_OWN[1] + lax.rem(me_e, ratio)],
                    device_id=(e, me_t),
                    device_id_type=MESH,
                ).start()
            MR[lax.rem(me_e, ratio)] = MO[me_e]

        def sent_own():
            for de, e in ep_peers:
                pltpu.make_async_remote_copy(
                    src_ref=MO.at[e],
                    dst_ref=MR.at[lax.rem(me_e, ratio)],
                    send_sem=send.at[P_OWN[0] + de],
                    recv_sem=recv.at[P_OWN[1] + lax.rem(me_e, ratio)],
                    device_id=(e, me_t),
                    device_id_type=MESH,
                ).wait_send()

        holds = me_e // ratio == me_t
        pl.when(holds)(send_own)

        for de, _ in ep_peers:
            arrive(SX, SR.at[0], P_STAT[1] + de)
        total = SR[0]
        for e in range(1, n_ep):
            total = total + SR[e]
        inv_mix = lax.rsqrt(total[1:2] / width + EPS)
        squares = total[0:1] + 2.0 * inv_mix * total[2:3] + inv_mix * inv_mix * total[3:4]
        inv_after = lax.rsqrt(jnp.maximum(squares, 0.0) / width + EPS)
        weight = jax.nn.sigmoid(inv_after * (total[4:5] + inv_mix * total[5:6]))
        back = jnp.where(row == 0, inv_mix, jnp.where(row == 1, inv_after, jnp.where(row == 2, weight, 0.0)))
        back = back.T
        COL[...] = back
        after = R[...].reshape(rows, block).astype(f32) + MV[...].reshape(rows, block) * back[:, 0:1] * g1
        ffn_in = (after * back[:, 1:2] * g2).astype(bf16)

        step = 256
        for j in range(CHUNKS):
            for copy in l_wd[j]:
                copy.wait()
            for a in range(0, 2 * chunk, step):
                piece = dot32(ffn_in, wd[j, :, a : a + step]).astype(bf16)
                for e in range(n_ep):
                    DX[j, e % 2, e // 2, :, a : a + step] = piece[e * seqs : (e + 1) * seqs]
            put(DX.at[j, 1 - c], DY.at[j], (partner, me_t), P_DPAIR[0] + j, P_DPAIR[1] + j)
            if j == 0:
                routed = dot32(SEL[...], ffn_in).astype(bf16)
                for e in range(n_ep):
                    OX[e] = routed[e * cells : (e + 1) * cells]
                for de, e in ep_peers:
                    put(OX.at[e], ER.at[:, mine], (e, me_t), P_EXP[0] + de, P_EXP[1] + de)
                ER[:, mine] = OX[me_e]
        for j in range(CHUNKS):
            arrive(DX.at[j, 0], DY.at[j], P_DPAIR[1] + j)
            for k, kk in enumerate(away):
                DZ[j, kk] = (DX[j, c, kk].astype(f32) + DY[j, kk].astype(f32)).astype(bf16)
                put(
                    DZ.at[j, kk],
                    DR.at[j, q],
                    (2 * kk + c, me_t),
                    P_DENSE[0] + j * half + k,
                    P_DENSE[1] + j * half + q,
                )
            DR[j, q] = (DX[j, c, q].astype(f32) + DY[j, q].astype(f32)).astype(bf16)

        for copy in l_exp:
            copy.wait()
        for de, _ in ep_peers:
            arrive(OX.at[0], ER.at[:, 0:block], P_EXP[1] + de)

        @pl.loop(0, eff // tile)
        def _(i):
            both = dot32(ER[...], wgu[:, cut(i * 2 * tile, 2 * tile)])
            hid[:, cut(i * tile, tile)] = (silu(both[:, :tile]) * both[:, tile:]).astype(bf16)

        for dt, t in tp_peers + [(0, me_t)]:
            piece = dot32(hid[...], wed[:, cut(t * part, part)]).astype(bf16)
            if dt:
                RX[dt] = piece
                put(RX.at[dt], RR.at[me_t], (me_e, t), P_RTP[0] + dt, P_RTP[1] + dt)
            else:
                RR[me_t] = piece

        def hidden(j):
            for kk in chips[1:]:
                arrive(DZ.at[j, 0], DR.at[j, 0], P_DENSE[1] + j * half + kk)
            for a in range(0, chunk, step):
                gate = DR[j, 0, :, a : a + step].astype(f32)
                up = DR[j, 0, :, chunk + a : chunk + a + step].astype(f32)
                for kk in range(1, half):
                    gate = gate + DR[j, kk, :, a : a + step].astype(f32)
                    up = up + DR[j, kk, :, chunk + a : chunk + a + step].astype(f32)
                DH[j, me_e, :, a : a + step] = (silu(gate) * up).astype(bf16)
            base = j * (half + 1)
            for k, kk in enumerate(away):
                put(
                    DH.at[j, me_e],
                    DH.at[j, me_e],
                    (2 * kk + c, me_t),
                    P_GATH[0] + base + k,
                    P_GATH[1] + base + q,
                )
            put(
                DH.at[j, me_e],
                DH.at[j, me_e],
                (partner, me_t),
                P_GATH[0] + base + half,
                P_GATH[1] + base + half,
            )

        def hand_over(j):
            base = j * (half + 1)
            for k, kk in enumerate(chips[1:]):
                arrive(DH.at[j, 0], DH.at[j, 1], P_GATH[1] + base + kk)
                here = DH.at[j, 2 * kk + c]
                put(here, here, (partner, me_t), P_HAND[0] + base + k, P_HAND[1] + base + kk)

        def gathered(j):
            base = j * (half + 1)
            arrive(DH.at[j, 0], DH.at[j, 1], P_GATH[1] + base + half)
            for kk in chips[1:]:
                arrive(DH.at[j, 0], DH.at[j, 1], P_HAND[1] + base + kk)
            return dot32(DH[j].reshape(rows, chunk), wdd[j * chunk : (j + 1) * chunk, :])

        def give_back():
            for dt, _ in tp_peers:
                arrive(RX.at[0], RR.at[0], P_RTP[1] + dt)
            total = RR[0].astype(f32)
            for t in range(1, n_tp):
                total = total + RR[t].astype(f32)
            total = total.astype(bf16)
            for e in range(n_ep):
                RB[e] = total[e * cap : (e + 1) * cap]
            RG[me_e] = RB[me_e]
            for de, e in ep_peers:
                put(RB.at[e], RG.at[me_e], (e, me_t), P_RET[0] + de, P_RET[1] + de)

        hidden(0)
        give_back()
        for j in range(1, CHUNKS):
            hidden(j)
        for j in range(CHUNKS):
            hand_over(j)
        l_wdd.wait()
        total = gathered(0)
        for j in range(1, CHUNKS):
            total = total + gathered(j)
        total = total.astype(bf16)
        for e in range(n_ep):
            dd[e] = total[e * seqs : (e + 1) * seqs]
        to = me_e // ratio
        slot = lax.rem(me_e, ratio) * n_tp + me_t
        landing = ddr.at[lax.rem(me_e, ratio), me_t]
        for de in range(n_ep):
            e = lax.rem(me_e + de, n_ep)
            remote = pltpu.make_async_remote_copy(
                src_ref=dd.at[e],
                dst_ref=landing,
                send_sem=send.at[P_COLS[0] + de],
                recv_sem=recv.at[P_COLS[1] + slot],
                device_id=(e, to),
                device_id_type=MESH,
            )
            if de == 0:
                own = pltpu.make_async_copy(dd.at[e], landing, recv.at[P_COLS[1] + slot])
                pl.when(to == me_t)(own.start)
                pl.when(to != me_t)(remote.start)
                sent.append(lambda remote=remote: pl.when(to != me_t)(remote.wait_send))
            else:
                remote.start()
                sent.append(remote.wait_send)

        for de, _ in ep_peers:
            arrive(RB.at[0], RG.at[0], P_RET[1] + de)
        expert_sum = jnp.dot(
            table,
            RG[...].astype(f32).reshape(cells, part),
            precision=lax.Precision.HIGHEST,
            preferred_element_type=f32,
        )
        own_cols = COL[own_rows, :]
        part_at = cut(me_t * part, part)
        for j in range(ratio):
            source = me_t * ratio + j

            def wait_own(j=j):
                arrive(MO.at[0], MR.at[j], P_OWN[1] + j)

            pl.when(source != me_e)(wait_own)
        mix_own = jnp.concatenate([MR[j].astype(f32) for j in range(ratio)], axis=1)
        after_own = tok[:, part_at].astype(f32) + mix_own * own_cols[:, 0:1] * gn[1:2, part_at]
        for i in range(ratio * n_tp):
            arrive(dd.at[0], ddr.at[i // n_tp, i % n_tp], P_COLS[1] + i)
        pieces = []
        for j in range(ratio):
            total = ddr[j, 0].astype(f32)
            for t in range(1, n_tp):
                total = total + ddr[j, t].astype(f32)
            pieces.append(total)
        ffn_out = expert_sum + own_cols[:, 2:3] * jnp.concatenate(pieces, axis=1)
        mass = jnp.sum(ffn_out * ffn_out, axis=1, keepdims=True)
        sq[...] = jnp.broadcast_to(mass, (seqs, lanes))
        sqr[me_t] = sq[...]
        for dt, t in tp_peers:
            put(sq, sqr.at[me_t], (me_e, t), P_SQ[0] + dt, P_SQ[1] + dt)
        for dt, _ in tp_peers:
            arrive(sq, sqr.at[0], P_SQ[1] + dt)
        total = sqr[0]
        for t in range(1, n_tp):
            total = total + sqr[t]
        scale = lax.rsqrt(total[:, 0:1] / width + EPS)
        out[...] = (after_own + ffn_out * scale * gn[3:4, part_at]).astype(bf16)
        pl.when(holds)(sent_own)
        for wait in sent:
            wait()

    vmem = pl.BlockSpec(memory_space=pltpu.VMEM)
    hbm = pl.BlockSpec(memory_space=pltpu.HBM)
    b = lambda *s: pltpu.VMEM(s, bf16)
    f = lambda *s: pltpu.VMEM(s, f32)
    n = lambda *s: pltpu.VMEM(s, i32)
    return pl.pallas_call(
        kernel,
        out_shape=(
            jax.ShapeDtypeStruct((seqs, part), bf16),
            jax.ShapeDtypeStruct(old_state.shape, f32),
        ),
        in_specs=[hbm] * 19,
        out_specs=(vmem, vmem),
        scratch_shapes=[
            b(seqs, width),
            f(*old_state.shape),
            f(1, chans),
            f(1, chans),
            f(*norm_gains.shape),
            b(heads, block, 4 * hs),
            b(chans, block),
            n(topk, seqs),
            f(topk, seqs),
            b(width, 2 * eff),
            b(eff, width),
            b(CHUNKS, block, 2 * chunk),
            b(dff, block),
            b(width // lanes, lanes),
            f(width // lanes, lanes),
            b(n_ep, seqs, block),
            n(n_ep, topk, seqs),
            b(heads, 2, half, seqs, 4 * hs),
            b(heads, half, seqs, 4 * hs),
            b(heads, half, seqs, 4 * hs),
            b(heads, half, seqs, 4 * hs),
            f(seqs, hs),
            b(heads, n_ep, seqs, hs),
            b(half, duo, block),
            b(n_tp, half, duo, block),
            f(half, duo, block),
            f(half, duo, lanes),
            f(8, lanes),
            f(n_ep, 8, lanes),
            f(rows, lanes),
            n(rows, lanes),
            b(n_ep * cells, rows),
            b(n_ep, seqs, block),
            b(ratio, seqs, block),
            b(CHUNKS, 2, half, seqs, 2 * chunk),
            b(CHUNKS, half, seqs, 2 * chunk),
            b(CHUNKS, half, seqs, 2 * chunk),
            b(CHUNKS, half, seqs, 2 * chunk),
            b(CHUNKS, n_ep, seqs, chunk),
            b(n_ep, cells, block),
            b(cells, width),
            b(cells, eff),
            b(n_tp, cells, part),
            b(n_tp, cells, part),
            b(n_ep, cap, part),
            b(n_ep, cap, part),
            b(n_ep, seqs, block),
            b(ratio, n_tp, seqs, block),
            f(seqs, lanes),
            f(n_tp, seqs, lanes),
            pltpu.SemaphoreType.DMA((send_at.used,)),
            pltpu.SemaphoreType.DMA((recv_at.used,)),
            pltpu.SemaphoreType.DMA((n_load,)),
        ],
        compiler_params=pltpu.CompilerParams(
            collective_id=1, has_side_effects=True, vmem_limit_bytes=40 * 1024 * 1024
        ),
        name="fused_layer",
    )(
        *(
            pltpu.with_memory_space_constraint(x, pltpu.HBM)
            for x in (
                tokens,
                old_state,
                bounds,
                head_gain,
                norm_gains,
                *in_weights,
                w_mix,
                routes,
                scores,
                *experts,
                *dense,
                mix_row,
            )
        )
    )


def fast_body(
    tokens,
    old_state,
    lower_bound,
    head_gain,
    norm_gains,
    w_query,
    w_forget,
    w_value,
    w_outgate,
    w_mix_out,
    routes,
    route_scores,
    w_exp_gate,
    w_exp_up,
    w_exp_down,
    w_dense_gate,
    w_dense_up,
    w_dense_down,
    dense_mix,
):
    return fused_layer(
        tokens,
        old_state,
        lower_bound[None, :],
        head_gain[None, :],
        norm_gains,
        (w_query, w_forget, w_value, w_outgate),
        w_mix_out,
        routes.T,
        route_scores.T,
        (w_exp_gate, w_exp_up, w_exp_down),
        (w_dense_gate, w_dense_up, w_dense_down),
        dense_mix.reshape(-1, 128),
        lax.axis_size("ep"),
        lax.axis_size("tp"),
    )


def solution(mesh):
    n_ep, n_tp = mesh.shape['ep'], mesh.shape['tp']
    fits = n_ep % n_tp == 0 and n_ep % 2 == 0 and n_ep * n_tp <= 64
    return jax.shard_map(
        fast_body if fits else body,
        mesh=mesh,
        in_specs=(
            P("ep", None),
            P("ep", "tp", None, None),
            P("tp"),
            P("tp"),
            P(),
            P("ep", "tp"),
            P("ep", "tp"),
            P("ep", "tp"),
            P("ep", "tp"),
            P("tp", "ep"),
            P("ep", None),
            P("ep", None),
            P("ep", None, "tp"),
            P("ep", None, "tp"),
            P("ep", "tp", None),
            P("ep", "tp"),
            P("ep", "tp"),
            P("tp", "ep"),
            P(),
        ),
        out_specs=(P("ep", "tp"), P("ep", "tp", None, None)),
        check_vma=False,
    )
```

```python
import jax
import jax.numpy as jnp
from jax import lax
from jax.experimental import pallas as pl
from jax.experimental.pallas import tpu as pltpu
from jax.sharding import PartitionSpec as P

EPS = 1e-06


def rms_scale(values):
    return lax.rsqrt(jnp.mean(values * values, axis=-1, keepdims=True) + EPS)


def body(
    tokens,
    old_state,
    lower_bound,
    head_gain,
    norm_gains,
    w_query,
    w_forget,
    w_value,
    w_outgate,
    w_mix_out,
    routes,
    route_scores,
    w_exp_gate,
    w_exp_up,
    w_exp_down,
    w_dense_gate,
    w_dense_up,
    w_dense_down,
    dense_mix,
):
    highest = lax.Precision.HIGHEST
    seqs, width = tokens.shape
    column_index = lax.axis_index("tp")
    part_width = width // lax.axis_size("tp")
    resid = tokens.astype(jnp.float32)
    normed = (resid * rms_scale(resid) * norm_gains[0]).astype(jnp.bfloat16)
    in_weights = jnp.concatenate([w_query, w_forget, w_value, w_outgate], axis=1)
    mix_rows = lax.all_to_all(normed, "ep", split_axis=1, concat_axis=0, tiled=True)
    projected = lax.psum_scatter(
        jnp.dot(mix_rows, in_weights, preferred_element_type=jnp.float32).astype(jnp.bfloat16),
        "ep",
        scatter_dimension=0,
        tiled=True,
    ).astype(jnp.float32)
    query_raw, forget_raw, value, out_gate = jnp.split(projected, 4, axis=1)
    heads = old_state.shape[1]
    head_size = old_state.shape[2]
    shape_heads = (seqs, heads, head_size)
    forget = lower_bound + (1.0 - lower_bound) * jax.nn.sigmoid(forget_raw)
    key_in = (1.0 - lower_bound) * jax.nn.sigmoid(-forget_raw)
    new_state = forget.reshape(shape_heads)[..., None] * old_state + key_in.reshape(shape_heads)[
        ..., None
    ] * value.reshape(seqs, heads, 1, head_size)
    query = jax.nn.silu(query_raw).reshape(shape_heads)
    read = jnp.einsum("thk,thkv->thv", query, new_state, precision=highest)
    gated = (
        read
        * rms_scale(read)
        * head_gain.reshape(heads, head_size)
        * jax.nn.silu(out_gate).reshape(shape_heads)
    )
    mixed_heads = gated.reshape(seqs, heads * head_size).astype(jnp.bfloat16)
    mix_part = jnp.dot(
        mixed_heads,
        lax.all_gather(w_mix_out, "ep", axis=1, tiled=True),
        preferred_element_type=jnp.float32,
    ).astype(jnp.bfloat16)
    mix_part = lax.optimization_barrier(mix_part).astype(jnp.float32)
    mix_out = lax.psum(mix_part.astype(jnp.bfloat16), "tp")
    mix_wide = lax.optimization_barrier(mix_out).astype(jnp.float32)
    after_mix = resid + mix_wide * rms_scale(mix_wide) * norm_gains[1]
    ffn_in = (after_mix * rms_scale(after_mix) * norm_gains[2]).astype(jnp.bfloat16)
    experts = lax.axis_size("ep")
    topk = routes.shape[1]
    capacity = max(2, 2 * seqs * topk // experts)
    flat_routes = routes.reshape(-1)
    onehot = (flat_routes[:, None] == jnp.arange(experts, dtype=jnp.int32)[None, :]).astype(
        jnp.int32
    )
    before = jnp.cumsum(onehot, axis=0) - onehot
    slots = jnp.sum(onehot * before, axis=1)
    cells = flat_routes * capacity + slots
    placed = cells[None, :] == jnp.arange(experts * capacity, dtype=jnp.int32)[:, None]
    repeated = jnp.repeat(ffn_in, topk, axis=0)
    outgoing = jnp.dot(placed.astype(jnp.bfloat16), repeated, preferred_element_type=jnp.float32)
    outgoing = outgoing.astype(jnp.bfloat16).reshape(experts, capacity, width)
    arrived = lax.all_to_all(outgoing, "ep", split_axis=0, concat_axis=0, tiled=True)
    sources, items, _ = arrived.shape
    expert_rows = arrived.reshape(sources * items, width)
    gate_pre = jnp.dot(expert_rows, w_exp_gate[0], preferred_element_type=jnp.float32)
    up_pre = jnp.dot(expert_rows, w_exp_up[0], preferred_element_type=jnp.float32)
    hidden = (jax.nn.silu(gate_pre) * up_pre).astype(jnp.bfloat16)
    partial_rows = jnp.dot(hidden, w_exp_down[0], preferred_element_type=jnp.float32).astype(
        jnp.bfloat16
    )
    partial_rows = lax.optimization_barrier(partial_rows).astype(jnp.float32)
    partial_rows = partial_rows.reshape(sources, items, width)
    summed = lax.psum_scatter(
        partial_rows.astype(jnp.bfloat16), "tp", scatter_dimension=2, tiled=True
    )
    returned = lax.all_to_all(summed, "ep", split_axis=0, concat_axis=0, tiled=True)
    first = jax.nn.sigmoid(route_scores[:, 0] - route_scores[:, 1])
    second = jax.nn.sigmoid(route_scores[:, 1] - route_scores[:, 0])
    route_weight = jnp.stack([first, second], axis=1).reshape(-1)
    weight_table = jnp.sum(
        (placed.astype(jnp.float32) * route_weight[None, :]).reshape(
            experts * capacity, seqs, topk
        ),
        axis=2,
    )
    expert_sum = jnp.dot(
        weight_table.T,
        returned.reshape(experts * capacity, part_width).astype(jnp.float32),
        precision=highest,
    )
    dense_weights = jnp.concatenate([w_dense_gate, w_dense_up], axis=1)
    dense_rows = lax.all_to_all(ffn_in, "ep", split_axis=1, concat_axis=0, tiled=True)
    dense_pre = lax.psum_scatter(
        jnp.dot(dense_rows, dense_weights, preferred_element_type=jnp.float32).astype(jnp.bfloat16),
        "ep",
        scatter_dimension=0,
        tiled=True,
    ).astype(jnp.float32)
    dense_gate_pre, dense_up_pre = jnp.split(dense_pre, 2, axis=1)
    dense_hidden = (jax.nn.silu(dense_gate_pre) * dense_up_pre).astype(jnp.bfloat16)
    dense_partial = jnp.dot(
        dense_hidden,
        lax.all_gather(w_dense_down, "ep", axis=1, tiled=True),
        preferred_element_type=jnp.float32,
    )
    dense_out = lax.psum_scatter(
        dense_partial.astype(jnp.bfloat16), "tp", scatter_dimension=1, tiled=True
    ).astype(jnp.float32)
    mix_weight = jax.nn.sigmoid(jnp.dot(ffn_in, dense_mix, preferred_element_type=jnp.float32))
    ffn_out = expert_sum + mix_weight[:, None] * dense_out
    squares = lax.psum(jnp.sum(ffn_out * ffn_out, axis=1), "tp")
    out_scale = lax.rsqrt(squares / width + EPS)
    gain_part = lax.dynamic_slice_in_dim(norm_gains[3], column_index * part_width, part_width, 0)
    resid_part = lax.dynamic_slice_in_dim(after_mix, column_index * part_width, part_width, 1)
    layer_out = (resid_part + ffn_out * out_scale[:, None] * gain_part).astype(jnp.bfloat16)
    return (layer_out, new_state)


def dot32(a, b):
    return jnp.dot(a, b, preferred_element_type=jnp.float32)


def silu(x):
    return x * jax.nn.sigmoid(x)


MESH = pl.DeviceIdType.MESH


class Sems:
    def __init__(self):
        self.used = 0

    def take(self, count):
        first = self.used
        self.used += count
        return first


def chips_by_distance(q, half):
    if half == 4:
        return [q, q + 1 - 2 * lax.rem(q, 2), 2 - q // 2, 3 - 3 * (q // 2)]
    return [q] + [lax.rem(q + k, half) for k in range(1, half)]


CHUNKS = 3


def fused_layer(
    tokens,
    old_state,
    bounds,
    head_gain,
    norm_gains,
    in_weights,
    w_mix,
    routes,
    scores,
    experts,
    dense,
    mix_row,
    n_ep,
    n_tp,
):
    bf16, f32, i32 = jnp.bfloat16, jnp.float32, jnp.int32
    seqs, width = tokens.shape
    heads, hs = old_state.shape[1:3]
    block, part = width // n_ep, width // n_tp
    chans = heads * hs
    topk = routes.shape[0]
    cap = max(2, 2 * seqs * topk // n_ep)
    cells, rows = n_ep * cap, n_ep * seqs
    eff, dff = experts[0].shape[2], dense[0].shape[1]
    half, ratio = n_ep // 2, n_ep // n_tp
    duo = 2 * seqs
    lanes = 128
    tile = 128
    chunk = dff // CHUNKS
    hc = chunk // 2

    send_at, recv_at = Sems(), Sems()

    def pair(count):
        return send_at.take(1), recv_at.take(count)

    P_TOK, P_ROUTE, P_PAIR, P_HEAD = pair(1), pair(1), pair(heads), pair(heads)
    P_MIX, P_TP, P_STAT, P_OWN = pair(half), pair(half), pair(1), pair(ratio)
    P_SWAP, P_TWIN, P_DENSE = pair(CHUNKS), pair(2), pair(CHUNKS)
    P_ROWS, P_EXP, P_RTP, P_RET = pair(1), pair(1), pair(1), pair(1)
    P_GATH, P_HAND, P_COLS, P_SQ = pair(CHUNKS), pair(CHUNKS), pair(1), pair(1)
    n_load = 13 + CHUNKS

    def kernel(
        tok_h, st_h, lb_h, hg_h, gn_h, wq_h, wf_h, wv_h, wo_h, wm_h, rt_h, sc_h,
        eg_h, eu_h, ed_h, dg_h, du_h, dd_h, mr_h,
        out, ns,
        tok, st, lb, hg, gn, win, wm, rt0, sc, wgu, wed, wd, wdd, mrow, wide_row,
        R, RP, RT, X, Y, Z, PR, rd, KC, VL, MA, TX, TR, STAT, SX, SR, COL, OWN, SEL, MO, MP, MR,
        FF, DX, DR, DH, OT, OX, ET, ER, EI, hid, RX, RR, RB, RG, dd, ddr, sq, sqr,
        send, recv, lsem,
    ):
        me_e, me_t = lax.axis_index("ep"), lax.axis_index("tp")
        q, c = me_e // 2, lax.rem(me_e, 2)
        partner = 2 * q + 1 - c
        chips = chips_by_distance(q, half)
        away = chips[:0:-1]
        ep_peers = [(de, lax.rem(me_e + de, n_ep)) for de in range(1, n_ep)]
        tp_peers = [(dt, lax.rem(me_t + dt, n_tp)) for dt in range(1, n_tp)]

        barrier = pltpu.get_barrier_semaphore()
        for _, e in ep_peers:
            pl.semaphore_signal(barrier, inc=1, device_id=(e, me_t), device_id_type=MESH)
        for _, t in tp_peers:
            pl.semaphore_signal(barrier, inc=1, device_id=(me_e, t), device_id_type=MESH)

        count = [0]

        def load(whole, *copies):
            at = count[0]
            count[0] += 1
            for src, dst in copies:
                pltpu.make_async_copy(src, dst, lsem.at[at]).start()
            return pltpu.make_async_copy(whole, whole, lsem.at[at])

        l_tok = load(tok, (tok_h, tok))
        l_gn = load(gn, (gn_h, gn))
        l_rt = load(rt0, (rt_h, rt0))
        l_in = load(
            win,
            *(
                (w.at[:, h * hs : (h + 1) * hs], win.at[h, :, i * hs : (i + 1) * hs])
                for h in range(heads)
                for i, w in enumerate((wq_h, wf_h, wv_h, wo_h))
            ),
        )
        l_small = [
            load(v, (h, v)) for h, v in ((lb_h, lb), (hg_h, hg), (sc_h, sc), (mr_h, mrow))
        ]
        l_st = load(st, (st_h, st))
        l_wm = load(wm, (wm_h, wm))
        l_wd = [
            load(
                wd.at[j, 0],
                *(
                    (
                        w.at[:, pl.ds(pl.multiple_of(j * chunk + c * hc, 128), hc)],
                        wd.at[j, c, :, i * hc : (i + 1) * hc],
                    )
                    for i, w in enumerate((dg_h, du_h))
                ),
            )
            for j in range(CHUNKS)
        ]
        l_exp = [
            load(
                wgu,
                *(
                    (
                        w.at[0, :, i * tile : (i + 1) * tile],
                        wgu.at[:, (2 * i + k) * tile : (2 * i + k + 1) * tile],
                    )
                    for i in range(eff // tile)
                    for k, w in enumerate((eg_h, eu_h))
                ),
            ),
            load(wed, (ed_h.at[0], wed)),
        ]
        l_wdd = load(wdd, (dd_h, wdd))

        def put(src, dst, device, s, r):
            pltpu.make_async_remote_copy(
                src_ref=src,
                dst_ref=dst,
                send_sem=send.at[s],
                recv_sem=recv.at[r],
                device_id=device,
                device_id_type=MESH,
            ).start()

        def arrive(whole, r):
            pltpu.make_async_copy(whole, whole, recv.at[r]).wait()

        def left(whole, s):
            pltpu.make_async_copy(whole, whole, send.at[s]).wait()

        others, peers, far = n_ep - 1, n_tp - 1, half - 1

        def cut(first, size):
            return pl.ds(pl.multiple_of(first, 128), size)

        mine = cut(me_e * block, block)
        own_rows = pl.ds(pl.multiple_of(me_e * seqs, seqs), seqs)

        l_tok.wait()
        l_gn.wait()
        l_rt.wait()
        pl.semaphore_wait(barrier, n_ep + n_tp - 2)
        for de, e in ep_peers:
            put(tok.at[:, cut(e * block, block)], R.at[me_e], (e, me_t), P_TOK[0], P_TOK[1])
        for de, e in ep_peers:
            put(rt0, RT.at[me_e], (e, me_t), P_ROUTE[0], P_ROUTE[1])
        for j in range(CHUNKS):
            for i, w in enumerate((dg_h, du_h)):
                put(
                    w.at[:, cut(j * chunk + (1 - c) * hc, hc)],
                    wd.at[j, c, :, i * hc : (i + 1) * hc],
                    (partner, me_t),
                    P_SWAP[0],
                    P_SWAP[1] + j,
                )
        R[me_e] = tok[:, mine]
        RT[me_e] = rt0[...]
        resid = tok[...].astype(f32)
        scale0 = rms_scale(resid)
        g0 = gn[0:1, mine]
        g1 = gn[1:2, mine]
        g2 = gn[2:3, mine]
        l_in.wait()
        arrive(R.at[0:others], P_TOK[1])

        scaled = (R[...].reshape(rows, block).astype(f32) * g0).astype(bf16)

        def project(h):
            piece = dot32(scaled, win[h]).astype(bf16)
            for e in range(n_ep):
                X[h, e % 2, e // 2] = piece[e * seqs : (e + 1) * seqs]
            put(X.at[h, 1 - c], Y.at[h], (partner, me_t), P_PAIR[0], P_PAIR[1] + h)

        def spread_head(h):
            arrive(Y.at[h], P_PAIR[1] + h)
            for kk in away:
                Z[h, kk] = (X[h, c, kk].astype(f32) + Y[h, kk].astype(f32)).astype(bf16)
                put(
                    Z.at[h, kk],
                    PR.at[h, q],
                    (2 * kk + c, me_t),
                    P_HEAD[0],
                    P_HEAD[1] + h,
                )
            PR[h, q] = (X[h, c, q].astype(f32) + Y[h, q].astype(f32)).astype(bf16)

        project(0)
        project(1)
        for h in range(heads):
            spread_head(h)
            if h + 2 < heads:
                project(h + 2)
        put(R, RP, (partner, me_t), P_TWIN[0], P_TWIN[1])

        arrive(RT.at[0:others], P_ROUTE[1])
        short = lax.broadcasted_iota(i32, (rows, seqs), 1)
        turn = lax.broadcasted_iota(i32, (rows, seqs), 0)
        diagonal = short == turn - (turn // seqs) * seqs
        named = []
        for k in range(topk):
            across = jnp.concatenate(
                [jnp.broadcast_to(RT[e, k : k + 1, :], (seqs, seqs)) for e in range(n_ep)], axis=0
            )
            named.append(jnp.sum(jnp.where(diagonal, across, 0), axis=1, keepdims=True))
        lane = lax.broadcasted_iota(i32, (rows, lanes), 1)
        row = lax.broadcasted_iota(i32, (rows, lanes), 0)
        ones = [(lane == named[k]).astype(f32) for k in range(topk)]
        earlier = ((lane < row) & (lane >= (row // seqs) * seqs)).astype(bf16)
        before = dot32(earlier, sum(ones).astype(bf16))
        slots = [
            jnp.sum(o * before, axis=1, keepdims=True).astype(i32) for o in ones
        ]
        spot = lax.broadcasted_iota(i32, (rows, 1), 0) // seqs
        wide = lax.broadcasted_iota(i32, (rows, n_ep * cells), 1)
        chosen = jnp.zeros((rows, n_ep * cells), f32)
        for k in range(topk):
            place = named[k] * cells + spot * cap + slots[k]
            chosen = chosen + (wide == place).astype(f32)
        for i in range(n_ep * cells // lanes):
            SEL[i * lanes : (i + 1) * lanes, :] = chosen[:, i * lanes : (i + 1) * lanes].T.astype(bf16)
        picked = dot32(SEL[...], R[...].reshape(rows, block)).astype(bf16)
        for e in range(n_ep):
            OT[e] = picked[e * cells : (e + 1) * cells]
        ET[:, mine] = OT[me_e]
        ours = jnp.zeros((rows, lanes), i32)
        for k in range(topk):
            ours = ours + jnp.where(lane == k, named[k] * cap + slots[k], 0)
        OWN[...] = ours
        for copy in l_small:
            copy.wait()
        wide_row[...] = mrow[...].astype(f32)
        at_own = OWN[own_rows, :]
        spread = lax.broadcasted_iota(i32, (seqs, cells), 1)
        gap = jnp.sum(
            jnp.where(diagonal[0:seqs], jnp.broadcast_to(sc[0:1, :] - sc[1:2, :], (seqs, seqs)), 0.0),
            axis=1,
            keepdims=True,
        )
        table = jnp.where(spread == at_own[:, 0:1], jax.nn.sigmoid(gap), 0.0)
        table = table + jnp.where(spread == at_own[:, 1:2], jax.nn.sigmoid(-gap), 0.0)

        l_st.wait()
        for h in range(heads):
            arrive(PR.at[h, 0:far], P_HEAD[1] + h)
            total = PR[h, 0].astype(f32)
            for kk in range(1, half):
                total = total + PR[h, kk].astype(f32)
            total = total * scale0
            at = slice(h * hs, (h + 1) * hs)
            bound = lb[0:1, at]
            raw = total[:, hs : 2 * hs]
            forget = bound + (1.0 - bound) * jax.nn.sigmoid(raw)
            key_in = (1.0 - bound) * jax.nn.sigmoid(-raw)
            query = silu(total[:, 0:hs])
            value = total[:, 2 * hs : 3 * hs]
            columns = jnp.concatenate(
                [forget, key_in, query * forget, jnp.zeros((hs - 3 * seqs, hs), f32)], axis=0
            ).T
            KC[h] = columns
            VL[h] = value
            for s in range(seqs):
                rd[s : s + 1, :] = jnp.sum(
                    columns[:, 2 * seqs + s : 2 * seqs + s + 1] * st[s, h], axis=0, keepdims=True
                )
            read = rd[...] + jnp.sum(query * key_in, axis=1, keepdims=True) * value
            gated = read * rms_scale(read) * hg[0:1, at] * silu(total[:, 3 * hs :])
            MA[h, me_e] = gated.astype(bf16)
            for de, e in ep_peers:
                put(
                    MA.at[h, me_e],
                    MA.at[h, me_e],
                    (e, me_t),
                    P_MIX[0],
                    P_MIX[1] + q,
                )

        for de, e in ep_peers:
            put(OT.at[e], ET.at[:, mine], (e, me_t), P_ROWS[0], P_ROWS[1])

        def update(h):
            for s in range(seqs):
                ns[s, h] = (
                    KC[h, :, s : s + 1] * st[s, h]
                    + KC[h, :, seqs + s : seqs + s + 1] * VL[h, s : s + 1, :]
                )

        update(0)
        update(1)

        l_wm.wait()
        for g, kk in enumerate(chips):
            arrive(MA.at[:, 0 : 2 if g else 1], P_MIX[1] + kk)
            lhs = jnp.concatenate(
                [MA[h, pl.ds(2 * kk, 2)].reshape(duo, hs) for h in range(heads)], axis=1
            )
            piece = dot32(lhs, wm[...]).astype(bf16)
            TX[kk] = piece
            TR[me_t, kk] = piece
            for dt, t in tp_peers:
                put(
                    TX.at[kk],
                    TR.at[me_t, kk],
                    (me_e, t),
                    P_TP[0],
                    P_TP[1] + kk,
                )
        lane_duo = lax.broadcasted_iota(i32, (duo, lanes), 1)
        mixer = jnp.concatenate(
            [
                wide_row[pl.ds(me_e * (block // lanes) + i, 1), :]
                for i in range(block // lanes)
            ],
            axis=1,
        )
        for kk in chips:
            arrive(TR.at[0:peers, 0], P_TP[1] + kk)
            total = TR[0, kk].astype(f32)
            for t in range(1, n_tp):
                total = total + TR[t, kk].astype(f32)
            narrow = total.astype(bf16)
            MO[pl.ds(2 * kk, 2)] = narrow.reshape(2, seqs, block)
            mixed = narrow.astype(f32)
            base = R[pl.ds(2 * kk, 2)].reshape(duo, block).astype(f32)
            lifted = mixed * g1
            figures = (
                base * base,
                mixed * mixed,
                base * lifted,
                lifted * lifted,
                base * g2 * mixer,
                lifted * g2 * mixer,
            )
            stat = jnp.zeros((duo, lanes), f32)
            for i, figure in enumerate(figures):
                stat = stat + jnp.where(
                    lane_duo == i, jnp.sum(figure, axis=1, keepdims=True), 0.0
                )
            STAT[kk] = stat
        SX[...] = STAT[...].reshape(rows, lanes).T[0:8, :]
        SR[me_e] = SX[...]
        for de, e in ep_peers:
            put(SX, SR.at[me_e], (e, me_t), P_STAT[0], P_STAT[1])
        put(MO, MP, (partner, me_t), P_TWIN[0], P_TWIN[1] + 1)
        picked = dot32(SEL[...], MO[...].reshape(rows, block)).astype(bf16)
        for e in range(n_ep):
            OX[e] = picked[e * cells : (e + 1) * cells]
        for de, e in ep_peers:
            put(OX.at[e], ER.at[:, mine], (e, me_t), P_EXP[0], P_EXP[1])
        ER[:, mine] = OX[me_e]

        def send_own():
            for _, e in ep_peers:
                put(
                    MO.at[e],
                    MR.at[lax.rem(me_e, ratio)],
                    (e, me_t),
                    P_OWN[0],
                    P_OWN[1] + lax.rem(me_e, ratio),
                )
            MR[lax.rem(me_e, ratio)] = MO[me_e]

        holds = me_e // ratio == me_t
        pl.when(holds)(send_own)
        update(2)
        update(3)
        arrive(RP, P_TWIN[1])
        arrive(MP, P_TWIN[1] + 1)

        arrive(SR.at[0:others], P_STAT[1])
        total = SR[0]
        for e in range(1, n_ep):
            total = total + SR[e]
        inv_mix = lax.rsqrt(total[1:2] / width + EPS)
        squares = total[0:1] + 2.0 * inv_mix * total[2:3] + inv_mix * inv_mix * total[3:4]
        inv_after = lax.rsqrt(jnp.maximum(squares, 0.0) / width + EPS)
        weight = jax.nn.sigmoid(inv_after * (total[4:5] + inv_mix * total[5:6]))
        back = jnp.where(row == 0, inv_mix, jnp.where(row == 1, inv_after, jnp.where(row == 2, weight, 0.0)))
        back = back.T
        COL[...] = back
        def normed(base, mixed, device):
            at = cut(device * block, block)
            after = base[...].reshape(rows, block).astype(f32)
            after = after + mixed[...].reshape(rows, block).astype(f32) * back[:, 0:1] * gn[1:2, at]
            return (after * back[:, 1:2] * gn[2:3, at]).astype(bf16)

        FF[c] = normed(R, MO, me_e)
        FF[1 - c] = normed(RP, MP, partner)

        for j in range(CHUNKS):
            l_wd[j].wait()
            arrive(wd.at[j, 0], P_SWAP[1] + j)
            piece = (dot32(FF[0], wd[j, 0]) + dot32(FF[1], wd[j, 1])).astype(bf16)
            for kk in range(half):
                DX[j, kk] = piece[kk * duo : (kk + 1) * duo]
            for kk in away:
                put(
                    DX.at[j, kk],
                    DR.at[j, q],
                    (2 * kk + c, me_t),
                    P_DENSE[0],
                    P_DENSE[1] + j,
                )
            DR[j, q] = DX[j, q]

        def hidden(j):
            arrive(DR.at[j, 0:far], P_DENSE[1] + j)
            total = DR[j, 0].astype(f32)
            for kk in range(1, half):
                total = total + DR[j, kk].astype(f32)
            here = DH.at[j, c, q]
            here[...] = (silu(total[:, :hc]) * total[:, hc:]).astype(bf16)
            for kk in away:
                put(here, here, (2 * kk + c, me_t), P_GATH[0], P_GATH[1] + j)
            put(here, here, (partner, me_t), P_HAND[0], P_HAND[1] + j)

        def hand_over(j):
            arrive(DH.at[j, 0, 0:far], P_GATH[1] + j)
            for kk in away:
                here = DH.at[j, c, kk]
                put(here, here, (partner, me_t), P_HAND[0], P_HAND[1] + j)

        def gathered(j):
            arrive(DH.at[j, 0], P_HAND[1] + j)
            total = 0.0
            for i in range(2):
                at = j * chunk + i * hc
                total = total + dot32(DH[j, i].reshape(rows, hc), wdd[at : at + hc, :])
            return total

        for copy in l_exp:
            copy.wait()
        arrive(OT.at[0:others], P_ROWS[1])
        arrive(OX.at[0:others], P_EXP[1])
        marks = jnp.dot(
            SEL[pl.ds(pl.multiple_of(me_e * cells, cells), cells), :].astype(f32),
            back,
            precision=lax.Precision.HIGHEST,
            preferred_element_type=f32,
        )
        for a in range(0, width, block):
            at = slice(a, a + block)
            after = ET[:, at].astype(f32) + ER[:, at].astype(f32) * marks[:, 0:1] * gn[1:2, at]
            EI[:, at] = (after * marks[:, 1:2] * gn[2:3, at]).astype(bf16)

        @pl.loop(0, eff // tile)
        def _(i):
            both = dot32(EI[...], wgu[:, cut(i * 2 * tile, 2 * tile)])
            hid[:, cut(i * tile, tile)] = (silu(both[:, :tile]) * both[:, tile:]).astype(bf16)

        for dt, t in tp_peers + [(0, me_t)]:
            piece = dot32(hid[...], wed[:, cut(t * part, part)]).astype(bf16)
            if dt:
                RX[dt] = piece
                put(RX.at[dt], RR.at[me_t], (me_e, t), P_RTP[0], P_RTP[1])
            else:
                RR[me_t] = piece

        def give_back():
            arrive(RR.at[0:peers], P_RTP[1])
            total = RR[0].astype(f32)
            for t in range(1, n_tp):
                total = total + RR[t].astype(f32)
            total = total.astype(bf16)
            for e in range(n_ep):
                RB[e] = total[e * cap : (e + 1) * cap]
            RG[me_e] = RB[me_e]
            for de, e in ep_peers:
                put(RB.at[e], RG.at[me_e], (e, me_t), P_RET[0], P_RET[1])

        for j in range(CHUNKS):
            hidden(j)
        give_back()
        for j in range(CHUNKS):
            hand_over(j)
        l_wdd.wait()
        total = gathered(0)
        for j in range(1, CHUNKS):
            total = total + gathered(j)
        total = total.astype(bf16)
        for e in range(n_ep):
            dd[e] = total[e * seqs : (e + 1) * seqs]
        to = me_e // ratio
        landing = ddr.at[lax.rem(me_e, ratio), me_t]
        for _, e in ep_peers:
            put(dd.at[e], landing, (e, to), P_COLS[0], P_COLS[1])

        def keep():
            landing[...] = dd[me_e]

        pl.when(holds)(keep)
        pl.when(jnp.logical_not(holds))(
            lambda: put(dd.at[me_e], landing, (me_e, to), P_COLS[0], P_COLS[1])
        )

        arrive(RG.at[0:others], P_RET[1])
        expert_sum = jnp.dot(
            table,
            RG[...].astype(f32).reshape(cells, part),
            precision=lax.Precision.HIGHEST,
            preferred_element_type=f32,
        )
        own_cols = COL[own_rows, :]
        part_at = cut(me_t * part, part)
        for j in range(ratio):
            source = me_t * ratio + j

            def wait_own(j=j):
                arrive(MR.at[j], P_OWN[1] + j)

            pl.when(source != me_e)(wait_own)
        mix_own = jnp.concatenate([MR[j].astype(f32) for j in range(ratio)], axis=1)
        after_own = tok[:, part_at].astype(f32) + mix_own * own_cols[:, 0:1] * gn[1:2, part_at]
        pl.when(holds)(lambda: arrive(dd.at[0:others], P_COLS[1]))
        pl.when(jnp.logical_not(holds))(lambda: arrive(dd, P_COLS[1]))
        pieces = []
        for j in range(ratio):
            total = ddr[j, 0].astype(f32)
            for t in range(1, n_tp):
                total = total + ddr[j, t].astype(f32)
            pieces.append(total)
        ffn_out = expert_sum + own_cols[:, 2:3] * jnp.concatenate(pieces, axis=1)
        mass = jnp.sum(ffn_out * ffn_out, axis=1, keepdims=True)
        sq[...] = jnp.broadcast_to(mass, (seqs, lanes))
        sqr[me_t] = sq[...]
        for dt, t in tp_peers:
            put(sq, sqr.at[me_t], (me_e, t), P_SQ[0], P_SQ[1])
        arrive(sqr.at[0:peers], P_SQ[1])
        total = sqr[0]
        for t in range(1, n_tp):
            total = total + sqr[t]
        scale = lax.rsqrt(total[:, 0:1] / width + EPS)
        out[...] = (after_own + ffn_out * scale * gn[3:4, part_at]).astype(bf16)
        pl.when(holds)(lambda: left(MO.at[0:others], P_OWN[0]))
        pl.when(holds)(lambda: left(dd.at[0:others], P_COLS[0]))
        pl.when(jnp.logical_not(holds))(lambda: left(dd, P_COLS[0]))
        for whole, ends in (
            (R.at[0:others], P_TOK),
            (RT.at[0:others], P_ROUTE),
            (Y, P_PAIR),
            (Z.at[:, 0:far], P_HEAD),
            (MA.at[:, 0:others], P_MIX),
            (TR.at[0:peers], P_TP),
            (SR.at[0:others], P_STAT),
            (wd.at[:, 0], P_SWAP),
            (FF, P_TWIN),
            (OT.at[0:others], P_ROWS),
            (OX.at[0:others], P_EXP),
            (DX.at[:, 0:far], P_DENSE),
            (DH.at[:, 0, 0:far], P_GATH),
            (DH.at[:, 0], P_HAND),
            (RR.at[0:peers], P_RTP),
            (RB.at[0:others], P_RET),
            (sqr.at[0:peers], P_SQ),
        ):
            left(whole, ends[0])

    vmem = pl.BlockSpec(memory_space=pltpu.VMEM)
    hbm = pl.BlockSpec(memory_space=pltpu.HBM)
    b = lambda *s: pltpu.VMEM(s, bf16)
    f = lambda *s: pltpu.VMEM(s, f32)
    n = lambda *s: pltpu.VMEM(s, i32)
    return pl.pallas_call(
        kernel,
        out_shape=(
            jax.ShapeDtypeStruct((seqs, part), bf16),
            pltpu.VMEM(old_state.shape, f32),
        ),
        in_specs=[hbm] * 19,
        out_specs=(vmem, vmem),
        scratch_shapes=[
            b(seqs, width),
            f(*old_state.shape),
            f(1, chans),
            f(1, chans),
            f(*norm_gains.shape),
            b(heads, block, 4 * hs),
            b(chans, block),
            n(topk, seqs),
            f(topk, seqs),
            b(width, 2 * eff),
            b(eff, width),
            b(CHUNKS, 2, block, chunk),
            b(dff, block),
            b(width // lanes, lanes),
            f(width // lanes, lanes),
            b(n_ep, seqs, block),
            b(n_ep, seqs, block),
            n(n_ep, topk, seqs),
            b(heads, 2, half, seqs, 4 * hs),
            b(heads, half, seqs, 4 * hs),
            b(heads, half, seqs, 4 * hs),
            b(heads, half, seqs, 4 * hs),
            f(seqs, hs),
            f(heads, hs, hs),
            f(heads, seqs, hs),
            b(heads, n_ep, seqs, hs),
            b(half, duo, block),
            b(n_tp, half, duo, block),
            f(half, duo, lanes),
            f(8, lanes),
            f(n_ep, 8, lanes),
            f(rows, lanes),
            n(rows, lanes),
            b(n_ep * cells, rows),
            b(n_ep, seqs, block),
            b(n_ep, seqs, block),
            b(ratio, seqs, block),
            b(2, rows, block),
            b(CHUNKS, half, duo, chunk),
            b(CHUNKS, half, duo, chunk),
            b(CHUNKS, 2, half, duo, hc),
            b(n_ep, cells, block),
            b(n_ep, cells, block),
            b(cells, width),
            b(cells, width),
            b(cells, width),
            b(cells, eff),
            b(n_tp, cells, part),
            b(n_tp, cells, part),
            b(n_ep, cap, part),
            b(n_ep, cap, part),
            b(n_ep, seqs, block),
            b(ratio, n_tp, seqs, block),
            f(seqs, lanes),
            f(n_tp, seqs, lanes),
            pltpu.SemaphoreType.DMA((send_at.used,)),
            pltpu.SemaphoreType.DMA((recv_at.used,)),
            pltpu.SemaphoreType.DMA((n_load,)),
        ],
        compiler_params=pltpu.CompilerParams(
            collective_id=1, has_side_effects=True, vmem_limit_bytes=40 * 1024 * 1024
        ),
        name="fused_layer",
    )(
        *(
            pltpu.with_memory_space_constraint(x, pltpu.HBM)
            for x in (
                tokens,
                old_state,
                bounds,
                head_gain,
                norm_gains,
                *in_weights,
                w_mix,
                routes,
                scores,
                *experts,
                *dense,
                mix_row,
            )
        )
    )


PIECES = 16


def write_out(layer_out, new_state):
    per = new_state.shape[0] // PIECES

    def kernel(small, big, small_to, big_to, sems):
        copies = [pltpu.make_async_copy(small, small_to, sems.at[PIECES])]
        for i in range(PIECES):
            at = pl.ds(i * per, per)
            copies.append(pltpu.make_async_copy(big.at[at], big_to.at[at], sems.at[i]))
        for copy in copies:
            copy.start()
        for copy in copies:
            copy.wait()

    vmem = pl.BlockSpec(memory_space=pltpu.VMEM)
    hbm = pl.BlockSpec(memory_space=pltpu.HBM)
    return pl.pallas_call(
        kernel,
        out_shape=(
            pltpu.HBM(layer_out.shape, layer_out.dtype),
            pltpu.HBM(new_state.shape, new_state.dtype),
        ),
        in_specs=[vmem] * 2,
        out_specs=(hbm, hbm),
        scratch_shapes=[pltpu.SemaphoreType.DMA((PIECES + 1,))],
        compiler_params=pltpu.CompilerParams(vmem_limit_bytes=1024 * 1024),
        name="write_out",
    )(
        pltpu.with_memory_space_constraint(layer_out, pltpu.VMEM),
        pltpu.with_memory_space_constraint(new_state, pltpu.VMEM),
    )


def fast_body(
    tokens,
    old_state,
    lower_bound,
    head_gain,
    norm_gains,
    w_query,
    w_forget,
    w_value,
    w_outgate,
    w_mix_out,
    routes,
    route_scores,
    w_exp_gate,
    w_exp_up,
    w_exp_down,
    w_dense_gate,
    w_dense_up,
    w_dense_down,
    dense_mix,
):
    layer_out, new_state = fused_layer(
        tokens,
        old_state,
        lower_bound[None, :],
        head_gain[None, :],
        norm_gains,
        (w_query, w_forget, w_value, w_outgate),
        w_mix_out,
        routes.T,
        route_scores.T,
        (w_exp_gate, w_exp_up, w_exp_down),
        (w_dense_gate, w_dense_up, w_dense_down),
        dense_mix.reshape(-1, 128),
        lax.axis_size("ep"),
        lax.axis_size("tp"),
    )
    return write_out(layer_out, new_state)


def solution(mesh):
    n_ep, n_tp = mesh.shape['ep'], mesh.shape['tp']
    fits = n_ep % n_tp == 0 and n_ep % 2 == 0 and n_ep * n_tp <= 64
    return jax.shard_map(
        fast_body if fits else body,
        mesh=mesh,
        in_specs=(
            P("ep", None),
            P("ep", "tp", None, None),
            P("tp"),
            P("tp"),
            P(),
            P("ep", "tp"),
            P("ep", "tp"),
            P("ep", "tp"),
            P("ep", "tp"),
            P("tp", "ep"),
            P("ep", None),
            P("ep", None),
            P("ep", None, "tp"),
            P("ep", None, "tp"),
            P("ep", "tp", None),
            P("ep", "tp"),
            P("ep", "tp"),
            P("tp", "ep"),
            P(),
        ),
        out_specs=(P("ep", "tp"), P("ep", "tp", None, None)),
        check_vma=False,
    )
```

```python
import jax
import jax.numpy as jnp
from jax import lax
from jax.experimental import pallas as pl
from jax.experimental.pallas import tpu as pltpu
from jax.sharding import PartitionSpec as P

EPS = 1e-06


def rms_scale(values):
    return lax.rsqrt(jnp.mean(values * values, axis=-1, keepdims=True) + EPS)


def body(
    tokens,
    old_state,
    lower_bound,
    head_gain,
    norm_gains,
    w_query,
    w_forget,
    w_value,
    w_outgate,
    w_mix_out,
    routes,
    route_scores,
    w_exp_gate,
    w_exp_up,
    w_exp_down,
    w_dense_gate,
    w_dense_up,
    w_dense_down,
    dense_mix,
):
    highest = lax.Precision.HIGHEST
    seqs, width = tokens.shape
    column_index = lax.axis_index("tp")
    part_width = width // lax.axis_size("tp")
    resid = tokens.astype(jnp.float32)
    normed = (resid * rms_scale(resid) * norm_gains[0]).astype(jnp.bfloat16)
    in_weights = jnp.concatenate([w_query, w_forget, w_value, w_outgate], axis=1)
    mix_rows = lax.all_to_all(normed, "ep", split_axis=1, concat_axis=0, tiled=True)
    projected = lax.psum_scatter(
        jnp.dot(mix_rows, in_weights, preferred_element_type=jnp.float32).astype(jnp.bfloat16),
        "ep",
        scatter_dimension=0,
        tiled=True,
    ).astype(jnp.float32)
    query_raw, forget_raw, value, out_gate = jnp.split(projected, 4, axis=1)
    heads = old_state.shape[1]
    head_size = old_state.shape[2]
    shape_heads = (seqs, heads, head_size)
    forget = lower_bound + (1.0 - lower_bound) * jax.nn.sigmoid(forget_raw)
    key_in = (1.0 - lower_bound) * jax.nn.sigmoid(-forget_raw)
    new_state = forget.reshape(shape_heads)[..., None] * old_state + key_in.reshape(shape_heads)[
        ..., None
    ] * value.reshape(seqs, heads, 1, head_size)
    query = jax.nn.silu(query_raw).reshape(shape_heads)
    read = jnp.einsum("thk,thkv->thv", query, new_state, precision=highest)
    gated = (
        read
        * rms_scale(read)
        * head_gain.reshape(heads, head_size)
        * jax.nn.silu(out_gate).reshape(shape_heads)
    )
    mixed_heads = gated.reshape(seqs, heads * head_size).astype(jnp.bfloat16)
    mix_part = jnp.dot(
        mixed_heads,
        lax.all_gather(w_mix_out, "ep", axis=1, tiled=True),
        preferred_element_type=jnp.float32,
    ).astype(jnp.bfloat16)
    mix_part = lax.optimization_barrier(mix_part).astype(jnp.float32)
    mix_out = lax.psum(mix_part.astype(jnp.bfloat16), "tp")
    mix_wide = lax.optimization_barrier(mix_out).astype(jnp.float32)
    after_mix = resid + mix_wide * rms_scale(mix_wide) * norm_gains[1]
    ffn_in = (after_mix * rms_scale(after_mix) * norm_gains[2]).astype(jnp.bfloat16)
    experts = lax.axis_size("ep")
    topk = routes.shape[1]
    capacity = max(2, 2 * seqs * topk // experts)
    flat_routes = routes.reshape(-1)
    onehot = (flat_routes[:, None] == jnp.arange(experts, dtype=jnp.int32)[None, :]).astype(
        jnp.int32
    )
    before = jnp.cumsum(onehot, axis=0) - onehot
    slots = jnp.sum(onehot * before, axis=1)
    cells = flat_routes * capacity + slots
    placed = cells[None, :] == jnp.arange(experts * capacity, dtype=jnp.int32)[:, None]
    repeated = jnp.repeat(ffn_in, topk, axis=0)
    outgoing = jnp.dot(placed.astype(jnp.bfloat16), repeated, preferred_element_type=jnp.float32)
    outgoing = outgoing.astype(jnp.bfloat16).reshape(experts, capacity, width)
    arrived = lax.all_to_all(outgoing, "ep", split_axis=0, concat_axis=0, tiled=True)
    sources, items, _ = arrived.shape
    expert_rows = arrived.reshape(sources * items, width)
    gate_pre = jnp.dot(expert_rows, w_exp_gate[0], preferred_element_type=jnp.float32)
    up_pre = jnp.dot(expert_rows, w_exp_up[0], preferred_element_type=jnp.float32)
    hidden = (jax.nn.silu(gate_pre) * up_pre).astype(jnp.bfloat16)
    partial_rows = jnp.dot(hidden, w_exp_down[0], preferred_element_type=jnp.float32).astype(
        jnp.bfloat16
    )
    partial_rows = lax.optimization_barrier(partial_rows).astype(jnp.float32)
    partial_rows = partial_rows.reshape(sources, items, width)
    summed = lax.psum_scatter(
        partial_rows.astype(jnp.bfloat16), "tp", scatter_dimension=2, tiled=True
    )
    returned = lax.all_to_all(summed, "ep", split_axis=0, concat_axis=0, tiled=True)
    first = jax.nn.sigmoid(route_scores[:, 0] - route_scores[:, 1])
    second = jax.nn.sigmoid(route_scores[:, 1] - route_scores[:, 0])
    route_weight = jnp.stack([first, second], axis=1).reshape(-1)
    weight_table = jnp.sum(
        (placed.astype(jnp.float32) * route_weight[None, :]).reshape(
            experts * capacity, seqs, topk
        ),
        axis=2,
    )
    expert_sum = jnp.dot(
        weight_table.T,
        returned.reshape(experts * capacity, part_width).astype(jnp.float32),
        precision=highest,
    )
    dense_weights = jnp.concatenate([w_dense_gate, w_dense_up], axis=1)
    dense_rows = lax.all_to_all(ffn_in, "ep", split_axis=1, concat_axis=0, tiled=True)
    dense_pre = lax.psum_scatter(
        jnp.dot(dense_rows, dense_weights, preferred_element_type=jnp.float32).astype(jnp.bfloat16),
        "ep",
        scatter_dimension=0,
        tiled=True,
    ).astype(jnp.float32)
    dense_gate_pre, dense_up_pre = jnp.split(dense_pre, 2, axis=1)
    dense_hidden = (jax.nn.silu(dense_gate_pre) * dense_up_pre).astype(jnp.bfloat16)
    dense_partial = jnp.dot(
        dense_hidden,
        lax.all_gather(w_dense_down, "ep", axis=1, tiled=True),
        preferred_element_type=jnp.float32,
    )
    dense_out = lax.psum_scatter(
        dense_partial.astype(jnp.bfloat16), "tp", scatter_dimension=1, tiled=True
    ).astype(jnp.float32)
    mix_weight = jax.nn.sigmoid(jnp.dot(ffn_in, dense_mix, preferred_element_type=jnp.float32))
    ffn_out = expert_sum + mix_weight[:, None] * dense_out
    squares = lax.psum(jnp.sum(ffn_out * ffn_out, axis=1), "tp")
    out_scale = lax.rsqrt(squares / width + EPS)
    gain_part = lax.dynamic_slice_in_dim(norm_gains[3], column_index * part_width, part_width, 0)
    resid_part = lax.dynamic_slice_in_dim(after_mix, column_index * part_width, part_width, 1)
    layer_out = (resid_part + ffn_out * out_scale[:, None] * gain_part).astype(jnp.bfloat16)
    return (layer_out, new_state)


def dot32(a, b):
    return jnp.dot(a, b, preferred_element_type=jnp.float32)


def silu(x):
    return x * jax.nn.sigmoid(x)


MESH = pl.DeviceIdType.MESH


class Sems:
    def __init__(self):
        self.used = 0

    def take(self, count):
        first = self.used
        self.used += count
        return first


def chips_by_distance(q, half):
    if half == 4:
        return [q, q + 1 - 2 * lax.rem(q, 2), 2 - q // 2, 3 - 3 * (q // 2)]
    return [q] + [lax.rem(q + k, half) for k in range(1, half)]


CHUNKS = 3


def fused_layer(
    tokens,
    old_state,
    bounds,
    head_gain,
    norm_gains,
    in_weights,
    w_mix,
    routes,
    scores,
    experts,
    dense,
    mix_row,
    n_ep,
    n_tp,
):
    bf16, f32, i32 = jnp.bfloat16, jnp.float32, jnp.int32
    seqs, width = tokens.shape
    heads, hs = old_state.shape[1:3]
    block, part = width // n_ep, width // n_tp
    chans = heads * hs
    topk = routes.shape[0]
    cap = max(2, 2 * seqs * topk // n_ep)
    cells, rows = n_ep * cap, n_ep * seqs
    eff, dff = experts[0].shape[2], dense[0].shape[1]
    half, ratio = n_ep // 2, n_ep // n_tp
    duo = 2 * seqs
    lanes = 128
    tile = 128
    chunk = dff // CHUNKS
    hc = chunk // 2
    few = ratio * cap

    send_at, recv_at = Sems(), Sems()

    def pair(count):
        return send_at.take(1), recv_at.take(count)

    P_TOK, P_ROUTE, P_PAIR, P_HEAD = pair(1), pair(1), pair(heads), pair(heads)
    P_MIX, P_TP, P_STAT, P_OWN = pair(half), pair(half), pair(1), pair(ratio)
    P_SWAP, P_TWIN, P_BASE, P_DENSE = pair(CHUNKS), pair(2), pair(1), pair(CHUNKS)
    P_ROWS, P_EXP, P_ALL = pair(1), pair(1), pair(1)
    P_RTP, P_RET = pair(1), pair(1)
    P_GATH, P_HAND, P_COLS, P_SQ = pair(CHUNKS), pair(CHUNKS), pair(1), pair(1)
    n_load = 13 + CHUNKS

    def kernel(
        tok_h, st_h, lb_h, hg_h, gn_h, wq_h, wf_h, wv_h, wo_h, wm_h, rt_h, sc_h,
        eg_h, eu_h, ed_h, dg_h, du_h, dd_h, mr_h,
        out, ns,
        tok, st, lb, hg, gn, win, wm, rt0, sc, wgu, wed, wd, wdd, mrow, wide_row,
        R, RP, RT, X, Y, Z, PR, rd, KC, VL, MA, TX, TR, STAT, SX, SR, COL, OWN, SEL, MO, MP, MR,
        FF, AX, AR, DX, DR, DH, OT, OX, ET, ER, EI, hid, RX, RR, RB, RG, dd, ddr, sq, sqr,
        send, recv, lsem,
    ):
        me_e, me_t = lax.axis_index("ep"), lax.axis_index("tp")
        q, c = me_e // 2, lax.rem(me_e, 2)
        partner = 2 * q + 1 - c
        chips = chips_by_distance(q, half)
        away = chips[:0:-1]
        ep_peers = [(de, lax.rem(me_e + de, n_ep)) for de in range(1, n_ep)]
        tp_peers = [(dt, lax.rem(me_t + dt, n_tp)) for dt in range(1, n_tp)]

        barrier = pltpu.get_barrier_semaphore()
        for _, e in ep_peers:
            pl.semaphore_signal(barrier, inc=1, device_id=(e, me_t), device_id_type=MESH)
        for _, t in tp_peers:
            pl.semaphore_signal(barrier, inc=1, device_id=(me_e, t), device_id_type=MESH)

        count = [0]

        def load(whole, *copies):
            at = count[0]
            count[0] += 1
            for src, dst in copies:
                pltpu.make_async_copy(src, dst, lsem.at[at]).start()
            return pltpu.make_async_copy(whole, whole, lsem.at[at])

        l_tok = load(tok, (tok_h, tok))
        l_gn = load(gn, (gn_h, gn))
        l_rt = load(rt0, (rt_h, rt0))
        l_in = load(
            win,
            *(
                (w.at[:, h * hs : (h + 1) * hs], win.at[h, :, i * hs : (i + 1) * hs])
                for h in range(heads)
                for i, w in enumerate((wq_h, wf_h, wv_h, wo_h))
            ),
        )
        l_small = [
            load(v, (h, v)) for h, v in ((lb_h, lb), (hg_h, hg), (sc_h, sc), (mr_h, mrow))
        ]
        l_st = load(st, (st_h, st))
        l_wm = load(wm, (wm_h, wm))
        l_wd = [
            load(
                wd.at[j, 0],
                *(
                    (
                        w.at[:, pl.ds(pl.multiple_of(j * chunk + c * hc, 128), hc)],
                        wd.at[j, c, :, i * hc : (i + 1) * hc],
                    )
                    for i, w in enumerate((dg_h, du_h))
                ),
            )
            for j in range(CHUNKS)
        ]
        l_exp = [
            load(
                wgu,
                *(
                    (
                        w.at[0, :, i * tile : (i + 1) * tile],
                        wgu.at[:, (2 * i + k) * tile : (2 * i + k + 1) * tile],
                    )
                    for i in range(eff // tile)
                    for k, w in enumerate((eg_h, eu_h))
                ),
            ),
            load(wed, (ed_h.at[0], wed)),
        ]
        l_wdd = load(wdd, (dd_h, wdd))

        def put(src, dst, device, s, r):
            pltpu.make_async_remote_copy(
                src_ref=src,
                dst_ref=dst,
                send_sem=send.at[s],
                recv_sem=recv.at[r],
                device_id=device,
                device_id_type=MESH,
            ).start()

        def arrive(whole, r):
            pltpu.make_async_copy(whole, whole, recv.at[r]).wait()

        def left(whole, s):
            pltpu.make_async_copy(whole, whole, send.at[s]).wait()

        others, peers, far = n_ep - 1, n_tp - 1, half - 1

        def cut(first, size):
            return pl.ds(pl.multiple_of(first, 128), size)

        mine = cut(me_e * block, block)
        own_rows = pl.ds(pl.multiple_of(me_e * seqs, seqs), seqs)

        l_tok.wait()
        l_gn.wait()
        l_rt.wait()
        pl.semaphore_wait(barrier, n_ep + n_tp - 2)
        for de, e in ep_peers:
            put(tok.at[:, cut(e * block, block)], R.at[me_e], (e, me_t), P_TOK[0], P_TOK[1])
        for de, e in ep_peers:
            put(rt0, RT.at[me_e], (e, me_t), P_ROUTE[0], P_ROUTE[1])
        for j in range(CHUNKS):
            for i, w in enumerate((dg_h, du_h)):
                put(
                    w.at[:, cut(j * chunk + (1 - c) * hc, hc)],
                    wd.at[j, c, :, i * hc : (i + 1) * hc],
                    (partner, me_t),
                    P_SWAP[0],
                    P_SWAP[1] + j,
                )
        R[me_e] = tok[:, mine]
        RT[me_e] = rt0[...]
        resid = tok[...].astype(f32)
        scale0 = rms_scale(resid)
        g0 = gn[0:1, mine]
        g1 = gn[1:2, mine]
        g2 = gn[2:3, mine]
        l_in.wait()
        arrive(R.at[0:others], P_TOK[1])

        put(R, RP, (partner, me_t), P_TWIN[0], P_TWIN[1])
        scaled = (R[...].reshape(rows, block).astype(f32) * g0).astype(bf16)

        def project(h):
            piece = dot32(scaled, win[h]).astype(bf16)
            for e in range(n_ep):
                X[h, e % 2, e // 2] = piece[e * seqs : (e + 1) * seqs]
            put(X.at[h, 1 - c], Y.at[h], (partner, me_t), P_PAIR[0], P_PAIR[1] + h)

        def spread_head(h):
            arrive(Y.at[h], P_PAIR[1] + h)
            for kk in away:
                Z[h, kk] = (X[h, c, kk].astype(f32) + Y[h, kk].astype(f32)).astype(bf16)
                put(
                    Z.at[h, kk],
                    PR.at[h, q],
                    (2 * kk + c, me_t),
                    P_HEAD[0],
                    P_HEAD[1] + h,
                )
            PR[h, q] = (X[h, c, q].astype(f32) + Y[h, q].astype(f32)).astype(bf16)

        project(0)
        project(1)
        for h in range(heads):
            spread_head(h)
            if h + 2 < heads:
                project(h + 2)

        arrive(RT.at[0:others], P_ROUTE[1])
        short = lax.broadcasted_iota(i32, (rows, seqs), 1)
        turn = lax.broadcasted_iota(i32, (rows, seqs), 0)
        diagonal = short == turn - (turn // seqs) * seqs
        named = []
        for k in range(topk):
            across = jnp.concatenate(
                [jnp.broadcast_to(RT[e, k : k + 1, :], (seqs, seqs)) for e in range(n_ep)], axis=0
            )
            named.append(jnp.sum(jnp.where(diagonal, across, 0), axis=1, keepdims=True))
        lane = lax.broadcasted_iota(i32, (rows, lanes), 1)
        row = lax.broadcasted_iota(i32, (rows, lanes), 0)
        ones = [(lane == named[k]).astype(f32) for k in range(topk)]
        earlier = ((lane < row) & (lane >= (row // seqs) * seqs)).astype(bf16)
        before = dot32(earlier, sum(ones).astype(bf16))
        slots = [
            jnp.sum(o * before, axis=1, keepdims=True).astype(i32) for o in ones
        ]
        spot = lax.broadcasted_iota(i32, (rows, 1), 0) // seqs
        wide = lax.broadcasted_iota(i32, (rows, n_ep * cells), 1)
        chosen = jnp.zeros((rows, n_ep * cells), f32)
        for k in range(topk):
            place = named[k] * cells + spot * cap + slots[k]
            chosen = chosen + (wide == place).astype(f32)
        per = lanes // cells
        for i in range(n_ep // per):
            flipped = chosen[:, i * lanes : (i + 1) * lanes].T.astype(bf16)
            SEL[i * per : (i + 1) * per] = flipped.reshape(per, n_tp, few, rows)

        def pick(base, ox):
            lhs = SEL[:, pl.ds(me_t, 1)].reshape(n_ep * few, rows)
            picked = dot32(lhs, base[...].reshape(rows, block)).astype(bf16)
            for e in range(n_ep):
                ox[e] = picked[e * few : (e + 1) * few]

        pick(R, OT)
        ET[:, mine] = OT[me_e]
        ours = jnp.zeros((rows, lanes), i32)
        for k in range(topk):
            ours = ours + jnp.where(lane == k, named[k] * cap + slots[k], 0)
        OWN[...] = ours
        for copy in l_small:
            copy.wait()
        wide_row[...] = mrow[...].astype(f32)
        at_own = OWN[own_rows, :]
        spread = lax.broadcasted_iota(i32, (seqs, cells), 1)
        gap = jnp.sum(
            jnp.where(diagonal[0:seqs], jnp.broadcast_to(sc[0:1, :] - sc[1:2, :], (seqs, seqs)), 0.0),
            axis=1,
            keepdims=True,
        )
        table = jnp.where(spread == at_own[:, 0:1], jax.nn.sigmoid(gap), 0.0)
        table = table + jnp.where(spread == at_own[:, 1:2], jax.nn.sigmoid(-gap), 0.0)

        arrive(RP, P_TWIN[1])

        def gains_of(device):
            return gn[2:3, cut(device * block, block)]

        FF[c] = (R[...].reshape(rows, block).astype(f32) * g2).astype(bf16)
        FF[1 - c] = (RP[...].reshape(rows, block).astype(f32) * gains_of(partner)).astype(bf16)

        def dense_part(j, ox, to):
            piece = (dot32(FF[0], wd[j, 0]) + dot32(FF[1], wd[j, 1])).astype(bf16)
            for kk in range(half):
                ox[kk] = piece[kk * duo : (kk + 1) * duo]
            to[q] = ox[q]

        def dense_send(ox, to, s, r):
            for kk in away:
                put(ox.at[kk], to.at[q], (2 * kk + c, me_t), s, r)

        for j in range(CHUNKS):
            l_wd[j].wait()
            arrive(wd.at[j, 0], P_SWAP[1] + j)
        dense_part(0, AX, AR)

        l_st.wait()
        for h in range(heads):
            arrive(PR.at[h, 0:far], P_HEAD[1] + h)
            total = PR[h, 0].astype(f32)
            for kk in range(1, half):
                total = total + PR[h, kk].astype(f32)
            total = total * scale0
            at = slice(h * hs, (h + 1) * hs)
            bound = lb[0:1, at]
            raw = total[:, hs : 2 * hs]
            forget = bound + (1.0 - bound) * jax.nn.sigmoid(raw)
            key_in = (1.0 - bound) * jax.nn.sigmoid(-raw)
            query = silu(total[:, 0:hs])
            value = total[:, 2 * hs : 3 * hs]
            columns = jnp.concatenate(
                [forget, key_in, query * forget, jnp.zeros((hs - 3 * seqs, hs), f32)], axis=0
            ).T
            KC[h] = columns
            VL[h] = value
            for s in range(seqs):
                rd[s : s + 1, :] = jnp.sum(
                    columns[:, 2 * seqs + s : 2 * seqs + s + 1] * st[s, h], axis=0, keepdims=True
                )
            read = rd[...] + jnp.sum(query * key_in, axis=1, keepdims=True) * value
            gated = read * rms_scale(read) * hg[0:1, at] * silu(total[:, 3 * hs :])
            MA[h, me_e] = gated.astype(bf16)
            for de, e in ep_peers:
                put(
                    MA.at[h, me_e],
                    MA.at[h, me_e],
                    (e, me_t),
                    P_MIX[0],
                    P_MIX[1] + q,
                )

        def update(h):
            for s in range(seqs):
                ns[s, h] = (
                    KC[h, :, s : s + 1] * st[s, h]
                    + KC[h, :, seqs + s : seqs + s + 1] * VL[h, s : s + 1, :]
                )

        update(0)
        update(1)

        l_wm.wait()
        for g, kk in enumerate(chips):
            arrive(MA.at[:, 0 : 2 if g else 1], P_MIX[1] + kk)
            lhs = jnp.concatenate(
                [MA[h, pl.ds(2 * kk, 2)].reshape(duo, hs) for h in range(heads)], axis=1
            )
            piece = dot32(lhs, wm[...]).astype(bf16)
            TX[kk] = piece
            TR[me_t, kk] = piece
            for dt, t in tp_peers:
                put(
                    TX.at[kk],
                    TR.at[me_t, kk],
                    (me_e, t),
                    P_TP[0],
                    P_TP[1] + kk,
                )
        dense_send(AX, AR, *P_BASE)
        for de, e in ep_peers:
            put(OT.at[e], ET.at[:, mine], (e, me_t), P_ROWS[0], P_ROWS[1])
        lane_duo = lax.broadcasted_iota(i32, (duo, lanes), 1)
        mixer = jnp.concatenate(
            [
                wide_row[pl.ds(me_e * (block // lanes) + i, 1), :]
                for i in range(block // lanes)
            ],
            axis=1,
        )
        for kk in chips:
            arrive(TR.at[0:peers, 0], P_TP[1] + kk)
            total = TR[0, kk].astype(f32)
            for t in range(1, n_tp):
                total = total + TR[t, kk].astype(f32)
            narrow = total.astype(bf16)
            MO[pl.ds(2 * kk, 2)] = narrow.reshape(2, seqs, block)
            mixed = narrow.astype(f32)
            base = R[pl.ds(2 * kk, 2)].reshape(duo, block).astype(f32)
            lifted = mixed * g1
            figures = (
                base * base,
                mixed * mixed,
                base * lifted,
                lifted * lifted,
                base * g2 * mixer,
                lifted * g2 * mixer,
            )
            stat = jnp.zeros((duo, lanes), f32)
            for i, figure in enumerate(figures):
                stat = stat + jnp.where(
                    lane_duo == i, jnp.sum(figure, axis=1, keepdims=True), 0.0
                )
            STAT[kk] = stat
        put(MO, MP, (partner, me_t), P_TWIN[0], P_TWIN[1] + 1)
        SX[...] = STAT[...].reshape(rows, lanes).T[0:8, :]
        SR[me_e] = SX[...]
        for de, e in ep_peers:
            put(SX, SR.at[me_e], (e, me_t), P_STAT[0], P_STAT[1])
        pick(MO, OX)
        for de, e in ep_peers:
            put(OX.at[e], ER.at[:, mine], (e, me_t), P_EXP[0], P_EXP[1])
        ER[:, mine] = OX[me_e]

        FF[c] = (MO[...].reshape(rows, block).astype(f32) * (g1 * g2)).astype(bf16)
        arrive(MP, P_TWIN[1] + 1)
        both = gn[1:2, cut(partner * block, block)] * gains_of(partner)
        FF[1 - c] = (MP[...].reshape(rows, block).astype(f32) * both).astype(bf16)
        dense_part(0, DX.at[0], DR.at[0])
        dense_send(DX.at[0], DR.at[0], *P_DENSE)

        def send_own():
            for _, e in ep_peers:
                put(
                    MO.at[e],
                    MR.at[lax.rem(me_e, ratio)],
                    (e, me_t),
                    P_OWN[0],
                    P_OWN[1] + lax.rem(me_e, ratio),
                )
            MR[lax.rem(me_e, ratio)] = MO[me_e]

        holds = me_e // ratio == me_t
        pl.when(holds)(send_own)
        update(2)
        update(3)

        arrive(SR.at[0:others], P_STAT[1])
        total = SR[0]
        for e in range(1, n_ep):
            total = total + SR[e]
        inv_mix = lax.rsqrt(total[1:2] / width + EPS)
        squares = total[0:1] + 2.0 * inv_mix * total[2:3] + inv_mix * inv_mix * total[3:4]
        inv_after = lax.rsqrt(jnp.maximum(squares, 0.0) / width + EPS)
        weight = jax.nn.sigmoid(inv_after * (total[4:5] + inv_mix * total[5:6]))
        back = jnp.where(row == 0, inv_mix, jnp.where(row == 1, inv_after, jnp.where(row == 2, weight, 0.0)))
        back = back.T
        COL[...] = back
        def normed(base, mixed, device):
            at = cut(device * block, block)
            after = base[...].reshape(rows, block).astype(f32)
            after = after + mixed[...].reshape(rows, block).astype(f32) * back[:, 0:1] * gn[1:2, at]
            return (after * back[:, 1:2] * gn[2:3, at]).astype(bf16)

        FF[c] = normed(R, MO, me_e)
        FF[1 - c] = normed(RP, MP, partner)
        for j in range(1, CHUNKS):
            dense_part(j, DX.at[j], DR.at[j])
            dense_send(DX.at[j], DR.at[j], P_DENSE[0], P_DENSE[1] + j)

        arrive(OT.at[0:others], P_ROWS[1])
        arrive(OX.at[0:others], P_EXP[1])
        marks = jnp.dot(
            SEL[me_e, me_t].astype(f32),
            back,
            precision=lax.Precision.HIGHEST,
            preferred_element_type=f32,
        )
        share = pl.ds(pl.multiple_of(me_t * few, few), few)
        after = ET[...].astype(f32) + ER[...].astype(f32) * marks[:, 0:1] * gn[1:2, :]
        EI[share, :] = (after * marks[:, 1:2] * gn[2:3, :]).astype(bf16)
        for dt, t in tp_peers:
            put(EI.at[share], EI.at[share], (me_e, t), P_ALL[0], P_ALL[1])

        chip_rows = pl.ds(pl.multiple_of(q * duo, duo), duo)

        def hidden(j):
            arrive(DR.at[j, 0:far], P_DENSE[1] + j)
            total = DR[j, 0].astype(f32)
            for kk in range(1, half):
                total = total + DR[j, kk].astype(f32)
            if j == 0:
                arrive(AR.at[0:far], P_BASE[1])
                base = AR[0].astype(f32)
                for kk in range(1, half):
                    base = base + AR[kk].astype(f32)
                own = COL[chip_rows, :]
                total = (base + own[:, 0:1] * total) * own[:, 1:2]
            here = DH.at[j, c, q]
            here[...] = (silu(total[:, :hc]) * total[:, hc:]).astype(bf16)
            for kk in away:
                put(here, here, (2 * kk + c, me_t), P_GATH[0], P_GATH[1] + j)
            put(here, here, (partner, me_t), P_HAND[0], P_HAND[1] + j)

        def hand_over(j):
            arrive(DH.at[j, 0, 0:far], P_GATH[1] + j)
            for kk in away:
                here = DH.at[j, c, kk]
                put(here, here, (partner, me_t), P_HAND[0], P_HAND[1] + j)

        def gathered(j):
            arrive(DH.at[j, 0], P_HAND[1] + j)
            total = 0.0
            for i in range(2):
                at = j * chunk + i * hc
                total = total + dot32(DH[j, i].reshape(rows, hc), wdd[at : at + hc, :])
            return total

        for copy in l_exp:
            copy.wait()
        hidden(0)
        hidden(1)
        arrive(EI.at[0 : peers * few], P_ALL[1])

        @pl.loop(0, eff // tile)
        def _(i):
            both = dot32(EI[...], wgu[:, cut(i * 2 * tile, 2 * tile)])
            hid[:, cut(i * tile, tile)] = (silu(both[:, :tile]) * both[:, tile:]).astype(bf16)

        for j in range(2, CHUNKS):
            hidden(j)
        for dt, t in tp_peers + [(0, me_t)]:
            piece = dot32(hid[...], wed[:, cut(t * part, part)]).astype(bf16)
            if dt:
                RX[dt] = piece
                put(RX.at[dt], RR.at[me_t], (me_e, t), P_RTP[0], P_RTP[1])
            else:
                RR[me_t] = piece

        def give_back():
            arrive(RR.at[0:peers], P_RTP[1])
            total = RR[0].astype(f32)
            for t in range(1, n_tp):
                total = total + RR[t].astype(f32)
            total = total.astype(bf16)
            for e in range(n_ep):
                RB[e] = total[e * cap : (e + 1) * cap]
            RG[me_e] = RB[me_e]
            for de, e in ep_peers:
                put(RB.at[e], RG.at[me_e], (e, me_t), P_RET[0], P_RET[1])

        for j in range(CHUNKS):
            hand_over(j)
        l_wdd.wait()
        total = gathered(0)
        for j in range(1, CHUNKS):
            total = total + gathered(j)
        total = total.astype(bf16)
        for e in range(n_ep):
            dd[e] = total[e * seqs : (e + 1) * seqs]
        to = me_e // ratio
        landing = ddr.at[lax.rem(me_e, ratio), me_t]
        for _, e in ep_peers:
            put(dd.at[e], landing, (e, to), P_COLS[0], P_COLS[1])

        def keep():
            landing[...] = dd[me_e]

        pl.when(holds)(keep)
        pl.when(jnp.logical_not(holds))(
            lambda: put(dd.at[me_e], landing, (me_e, to), P_COLS[0], P_COLS[1])
        )

        give_back()

        arrive(RG.at[0:others], P_RET[1])
        expert_sum = jnp.dot(
            table,
            RG[...].astype(f32).reshape(cells, part),
            precision=lax.Precision.HIGHEST,
            preferred_element_type=f32,
        )
        own_cols = COL[own_rows, :]
        part_at = cut(me_t * part, part)
        for j in range(ratio):
            source = me_t * ratio + j

            def wait_own(j=j):
                arrive(MR.at[j], P_OWN[1] + j)

            pl.when(source != me_e)(wait_own)
        mix_own = jnp.concatenate([MR[j].astype(f32) for j in range(ratio)], axis=1)
        after_own = tok[:, part_at].astype(f32) + mix_own * own_cols[:, 0:1] * gn[1:2, part_at]
        pl.when(holds)(lambda: arrive(dd.at[0:others], P_COLS[1]))
        pl.when(jnp.logical_not(holds))(lambda: arrive(dd, P_COLS[1]))
        pieces = []
        for j in range(ratio):
            total = ddr[j, 0].astype(f32)
            for t in range(1, n_tp):
                total = total + ddr[j, t].astype(f32)
            pieces.append(total)
        ffn_out = expert_sum + own_cols[:, 2:3] * jnp.concatenate(pieces, axis=1)
        mass = jnp.sum(ffn_out * ffn_out, axis=1, keepdims=True)
        sq[...] = jnp.broadcast_to(mass, (seqs, lanes))
        sqr[me_t] = sq[...]
        for dt, t in tp_peers:
            put(sq, sqr.at[me_t], (me_e, t), P_SQ[0], P_SQ[1])
        arrive(sqr.at[0:peers], P_SQ[1])
        total = sqr[0]
        for t in range(1, n_tp):
            total = total + sqr[t]
        scale = lax.rsqrt(total[:, 0:1] / width + EPS)
        out[...] = (after_own + ffn_out * scale * gn[3:4, part_at]).astype(bf16)
        pl.when(holds)(lambda: left(MO.at[0:others], P_OWN[0]))
        pl.when(holds)(lambda: left(dd.at[0:others], P_COLS[0]))
        pl.when(jnp.logical_not(holds))(lambda: left(dd, P_COLS[0]))
        for whole, ends in (
            (R.at[0:others], P_TOK),
            (RT.at[0:others], P_ROUTE),
            (Y, P_PAIR),
            (Z.at[:, 0:far], P_HEAD),
            (MA.at[:, 0:others], P_MIX),
            (TR.at[0:peers], P_TP),
            (SR.at[0:others], P_STAT),
            (wd.at[:, 0], P_SWAP),
            (FF, P_TWIN),
            (AX.at[0:far], P_BASE),
            (EI.at[0 : peers * few], P_ALL),
            (OT.at[0:others], P_ROWS),
            (OX.at[0:others], P_EXP),
            (DX.at[:, 0:far], P_DENSE),
            (DH.at[:, 0, 0:far], P_GATH),
            (DH.at[:, 0], P_HAND),
            (RR.at[0:peers], P_RTP),
            (RB.at[0:others], P_RET),
            (sqr.at[0:peers], P_SQ),
        ):
            left(whole, ends[0])

    vmem = pl.BlockSpec(memory_space=pltpu.VMEM)
    hbm = pl.BlockSpec(memory_space=pltpu.HBM)
    b = lambda *s: pltpu.VMEM(s, bf16)
    f = lambda *s: pltpu.VMEM(s, f32)
    n = lambda *s: pltpu.VMEM(s, i32)
    return pl.pallas_call(
        kernel,
        out_shape=(
            jax.ShapeDtypeStruct((seqs, part), bf16),
            pltpu.VMEM(old_state.shape, f32),
        ),
        in_specs=[hbm] * 19,
        out_specs=(vmem, vmem),
        scratch_shapes=[
            b(seqs, width),
            f(*old_state.shape),
            f(1, chans),
            f(1, chans),
            f(*norm_gains.shape),
            b(heads, block, 4 * hs),
            b(chans, block),
            n(topk, seqs),
            f(topk, seqs),
            b(width, 2 * eff),
            b(eff, width),
            b(CHUNKS, 2, block, chunk),
            b(dff, block),
            b(width // lanes, lanes),
            f(width // lanes, lanes),
            b(n_ep, seqs, block),
            b(n_ep, seqs, block),
            n(n_ep, topk, seqs),
            b(heads, 2, half, seqs, 4 * hs),
            b(heads, half, seqs, 4 * hs),
            b(heads, half, seqs, 4 * hs),
            b(heads, half, seqs, 4 * hs),
            f(seqs, hs),
            f(heads, hs, hs),
            f(heads, seqs, hs),
            b(heads, n_ep, seqs, hs),
            b(half, duo, block),
            b(n_tp, half, duo, block),
            f(half, duo, lanes),
            f(8, lanes),
            f(n_ep, 8, lanes),
            f(rows, lanes),
            n(rows, lanes),
            b(n_ep, n_tp, few, rows),
            b(n_ep, seqs, block),
            b(n_ep, seqs, block),
            b(ratio, seqs, block),
            b(2, rows, block),
            b(half, duo, chunk),
            b(half, duo, chunk),
            b(CHUNKS, half, duo, chunk),
            b(CHUNKS, half, duo, chunk),
            b(CHUNKS, 2, half, duo, hc),
            b(n_ep, few, block),
            b(n_ep, few, block),
            b(few, width),
            b(few, width),
            b(cells, width),
            b(cells, eff),
            b(n_tp, cells, part),
            b(n_tp, cells, part),
            b(n_ep, cap, part),
            b(n_ep, cap, part),
            b(n_ep, seqs, block),
            b(ratio, n_tp, seqs, block),
            f(seqs, lanes),
            f(n_tp, seqs, lanes),
            pltpu.SemaphoreType.DMA((send_at.used,)),
            pltpu.SemaphoreType.DMA((recv_at.used,)),
            pltpu.SemaphoreType.DMA((n_load,)),
        ],
        compiler_params=pltpu.CompilerParams(
            collective_id=1, has_side_effects=True, vmem_limit_bytes=40 * 1024 * 1024
        ),
        name="fused_layer",
    )(
        *(
            pltpu.with_memory_space_constraint(x, pltpu.HBM)
            for x in (
                tokens,
                old_state,
                bounds,
                head_gain,
                norm_gains,
                *in_weights,
                w_mix,
                routes,
                scores,
                *experts,
                *dense,
                mix_row,
            )
        )
    )


PIECES = 16


def write_out(layer_out, new_state):
    per = new_state.shape[0] // PIECES

    def kernel(small, big, small_to, big_to, sems):
        copies = [pltpu.make_async_copy(small, small_to, sems.at[PIECES])]
        for i in range(PIECES):
            at = pl.ds(i * per, per)
            copies.append(pltpu.make_async_copy(big.at[at], big_to.at[at], sems.at[i]))
        for copy in copies:
            copy.start()
        for copy in copies:
            copy.wait()

    vmem = pl.BlockSpec(memory_space=pltpu.VMEM)
    hbm = pl.BlockSpec(memory_space=pltpu.HBM)
    return pl.pallas_call(
        kernel,
        out_shape=(
            pltpu.HBM(layer_out.shape, layer_out.dtype),
            pltpu.HBM(new_state.shape, new_state.dtype),
        ),
        in_specs=[vmem] * 2,
        out_specs=(hbm, hbm),
        scratch_shapes=[pltpu.SemaphoreType.DMA((PIECES + 1,))],
        compiler_params=pltpu.CompilerParams(vmem_limit_bytes=1024 * 1024),
        name="write_out",
    )(
        pltpu.with_memory_space_constraint(layer_out, pltpu.VMEM),
        pltpu.with_memory_space_constraint(new_state, pltpu.VMEM),
    )


def fast_body(
    tokens,
    old_state,
    lower_bound,
    head_gain,
    norm_gains,
    w_query,
    w_forget,
    w_value,
    w_outgate,
    w_mix_out,
    routes,
    route_scores,
    w_exp_gate,
    w_exp_up,
    w_exp_down,
    w_dense_gate,
    w_dense_up,
    w_dense_down,
    dense_mix,
):
    layer_out, new_state = fused_layer(
        tokens,
        old_state,
        lower_bound[None, :],
        head_gain[None, :],
        norm_gains,
        (w_query, w_forget, w_value, w_outgate),
        w_mix_out,
        routes.T,
        route_scores.T,
        (w_exp_gate, w_exp_up, w_exp_down),
        (w_dense_gate, w_dense_up, w_dense_down),
        dense_mix.reshape(-1, 128),
        lax.axis_size("ep"),
        lax.axis_size("tp"),
    )
    return write_out(layer_out, new_state)


def solution(mesh):
    n_ep, n_tp = mesh.shape['ep'], mesh.shape['tp']
    fits = n_ep % n_tp == 0 and n_ep % 2 == 0 and n_ep * n_tp <= 64
    return jax.shard_map(
        fast_body if fits else body,
        mesh=mesh,
        in_specs=(
            P("ep", None),
            P("ep", "tp", None, None),
            P("tp"),
            P("tp"),
            P(),
            P("ep", "tp"),
            P("ep", "tp"),
            P("ep", "tp"),
            P("ep", "tp"),
            P("tp", "ep"),
            P("ep", None),
            P("ep", None),
            P("ep", None, "tp"),
            P("ep", None, "tp"),
            P("ep", "tp", None),
            P("ep", "tp"),
            P("ep", "tp"),
            P("tp", "ep"),
            P(),
        ),
        out_specs=(P("ep", "tp"), P("ep", "tp", None, None)),
        check_vma=False,
    )
```

```python
import jax
import jax.numpy as jnp
from jax import lax
from jax.experimental import pallas as pl
from jax.experimental.pallas import tpu as pltpu
from jax.sharding import PartitionSpec as P

EPS = 1e-06


def rms_scale(values):
    return lax.rsqrt(jnp.mean(values * values, axis=-1, keepdims=True) + EPS)


def body(
    tokens,
    old_state,
    lower_bound,
    head_gain,
    norm_gains,
    w_query,
    w_forget,
    w_value,
    w_outgate,
    w_mix_out,
    routes,
    route_scores,
    w_exp_gate,
    w_exp_up,
    w_exp_down,
    w_dense_gate,
    w_dense_up,
    w_dense_down,
    dense_mix,
):
    highest = lax.Precision.HIGHEST
    seqs, width = tokens.shape
    column_index = lax.axis_index("tp")
    part_width = width // lax.axis_size("tp")
    resid = tokens.astype(jnp.float32)
    normed = (resid * rms_scale(resid) * norm_gains[0]).astype(jnp.bfloat16)
    in_weights = jnp.concatenate([w_query, w_forget, w_value, w_outgate], axis=1)
    mix_rows = lax.all_to_all(normed, "ep", split_axis=1, concat_axis=0, tiled=True)
    projected = lax.psum_scatter(
        jnp.dot(mix_rows, in_weights, preferred_element_type=jnp.float32).astype(jnp.bfloat16),
        "ep",
        scatter_dimension=0,
        tiled=True,
    ).astype(jnp.float32)
    query_raw, forget_raw, value, out_gate = jnp.split(projected, 4, axis=1)
    heads = old_state.shape[1]
    head_size = old_state.shape[2]
    shape_heads = (seqs, heads, head_size)
    forget = lower_bound + (1.0 - lower_bound) * jax.nn.sigmoid(forget_raw)
    key_in = (1.0 - lower_bound) * jax.nn.sigmoid(-forget_raw)
    new_state = forget.reshape(shape_heads)[..., None] * old_state + key_in.reshape(shape_heads)[
        ..., None
    ] * value.reshape(seqs, heads, 1, head_size)
    query = jax.nn.silu(query_raw).reshape(shape_heads)
    read = jnp.einsum("thk,thkv->thv", query, new_state, precision=highest)
    gated = (
        read
        * rms_scale(read)
        * head_gain.reshape(heads, head_size)
        * jax.nn.silu(out_gate).reshape(shape_heads)
    )
    mixed_heads = gated.reshape(seqs, heads * head_size).astype(jnp.bfloat16)
    mix_part = jnp.dot(
        mixed_heads,
        lax.all_gather(w_mix_out, "ep", axis=1, tiled=True),
        preferred_element_type=jnp.float32,
    ).astype(jnp.bfloat16)
    mix_part = lax.optimization_barrier(mix_part).astype(jnp.float32)
    mix_out = lax.psum(mix_part.astype(jnp.bfloat16), "tp")
    mix_wide = lax.optimization_barrier(mix_out).astype(jnp.float32)
    after_mix = resid + mix_wide * rms_scale(mix_wide) * norm_gains[1]
    ffn_in = (after_mix * rms_scale(after_mix) * norm_gains[2]).astype(jnp.bfloat16)
    experts = lax.axis_size("ep")
    topk = routes.shape[1]
    capacity = max(2, 2 * seqs * topk // experts)
    flat_routes = routes.reshape(-1)
    onehot = (flat_routes[:, None] == jnp.arange(experts, dtype=jnp.int32)[None, :]).astype(
        jnp.int32
    )
    before = jnp.cumsum(onehot, axis=0) - onehot
    slots = jnp.sum(onehot * before, axis=1)
    cells = flat_routes * capacity + slots
    placed = cells[None, :] == jnp.arange(experts * capacity, dtype=jnp.int32)[:, None]
    repeated = jnp.repeat(ffn_in, topk, axis=0)
    outgoing = jnp.dot(placed.astype(jnp.bfloat16), repeated, preferred_element_type=jnp.float32)
    outgoing = outgoing.astype(jnp.bfloat16).reshape(experts, capacity, width)
    arrived = lax.all_to_all(outgoing, "ep", split_axis=0, concat_axis=0, tiled=True)
    sources, items, _ = arrived.shape
    expert_rows = arrived.reshape(sources * items, width)
    gate_pre = jnp.dot(expert_rows, w_exp_gate[0], preferred_element_type=jnp.float32)
    up_pre = jnp.dot(expert_rows, w_exp_up[0], preferred_element_type=jnp.float32)
    hidden = (jax.nn.silu(gate_pre) * up_pre).astype(jnp.bfloat16)
    partial_rows = jnp.dot(hidden, w_exp_down[0], preferred_element_type=jnp.float32).astype(
        jnp.bfloat16
    )
    partial_rows = lax.optimization_barrier(partial_rows).astype(jnp.float32)
    partial_rows = partial_rows.reshape(sources, items, width)
    summed = lax.psum_scatter(
        partial_rows.astype(jnp.bfloat16), "tp", scatter_dimension=2, tiled=True
    )
    returned = lax.all_to_all(summed, "ep", split_axis=0, concat_axis=0, tiled=True)
    first = jax.nn.sigmoid(route_scores[:, 0] - route_scores[:, 1])
    second = jax.nn.sigmoid(route_scores[:, 1] - route_scores[:, 0])
    route_weight = jnp.stack([first, second], axis=1).reshape(-1)
    weight_table = jnp.sum(
        (placed.astype(jnp.float32) * route_weight[None, :]).reshape(
            experts * capacity, seqs, topk
        ),
        axis=2,
    )
    expert_sum = jnp.dot(
        weight_table.T,
        returned.reshape(experts * capacity, part_width).astype(jnp.float32),
        precision=highest,
    )
    dense_weights = jnp.concatenate([w_dense_gate, w_dense_up], axis=1)
    dense_rows = lax.all_to_all(ffn_in, "ep", split_axis=1, concat_axis=0, tiled=True)
    dense_pre = lax.psum_scatter(
        jnp.dot(dense_rows, dense_weights, preferred_element_type=jnp.float32).astype(jnp.bfloat16),
        "ep",
        scatter_dimension=0,
        tiled=True,
    ).astype(jnp.float32)
    dense_gate_pre, dense_up_pre = jnp.split(dense_pre, 2, axis=1)
    dense_hidden = (jax.nn.silu(dense_gate_pre) * dense_up_pre).astype(jnp.bfloat16)
    dense_partial = jnp.dot(
        dense_hidden,
        lax.all_gather(w_dense_down, "ep", axis=1, tiled=True),
        preferred_element_type=jnp.float32,
    )
    dense_out = lax.psum_scatter(
        dense_partial.astype(jnp.bfloat16), "tp", scatter_dimension=1, tiled=True
    ).astype(jnp.float32)
    mix_weight = jax.nn.sigmoid(jnp.dot(ffn_in, dense_mix, preferred_element_type=jnp.float32))
    ffn_out = expert_sum + mix_weight[:, None] * dense_out
    squares = lax.psum(jnp.sum(ffn_out * ffn_out, axis=1), "tp")
    out_scale = lax.rsqrt(squares / width + EPS)
    gain_part = lax.dynamic_slice_in_dim(norm_gains[3], column_index * part_width, part_width, 0)
    resid_part = lax.dynamic_slice_in_dim(after_mix, column_index * part_width, part_width, 1)
    layer_out = (resid_part + ffn_out * out_scale[:, None] * gain_part).astype(jnp.bfloat16)
    return (layer_out, new_state)


def dot32(a, b):
    return jnp.dot(a, b, preferred_element_type=jnp.float32)


def silu(x):
    return x * jax.nn.sigmoid(x)


MESH = pl.DeviceIdType.MESH


class Sems:
    def __init__(self):
        self.used = 0

    def take(self, count):
        first = self.used
        self.used += count
        return first


def chips_by_distance(q, half):
    if half == 4:
        return [q, q + 1 - 2 * lax.rem(q, 2), 2 - q // 2, 3 - 3 * (q // 2)]
    return [q] + [lax.rem(q + k, half) for k in range(1, half)]


CHUNKS = 3
EARLY = 1


def fused_layer(
    tokens,
    old_state,
    bounds,
    head_gain,
    norm_gains,
    in_weights,
    w_mix,
    routes,
    scores,
    experts,
    dense,
    mix_row,
    n_ep,
    n_tp,
):
    bf16, f32, i32 = jnp.bfloat16, jnp.float32, jnp.int32
    seqs, width = tokens.shape
    heads, hs = old_state.shape[1:3]
    block, part = width // n_ep, width // n_tp
    chans = heads * hs
    topk = routes.shape[0]
    cap = max(2, 2 * seqs * topk // n_ep)
    cells, rows = n_ep * cap, n_ep * seqs
    eff, dff = experts[0].shape[2], dense[0].shape[1]
    half, ratio = n_ep // 2, n_ep // n_tp
    duo = 2 * seqs
    lanes = 128
    tile = 128
    chunk = dff // CHUNKS
    hc = chunk // 2
    few = ratio * cap

    send_at, recv_at = Sems(), Sems()

    def pair(count):
        return send_at.take(1), recv_at.take(count)

    P_TOK, P_ROUTE, P_PAIR, P_HEAD = pair(1), pair(1), pair(heads), pair(heads)
    P_MIX, P_TP, P_STAT, P_OWN = pair(half), pair(half), pair(1), pair(ratio)
    P_SWAP, P_TWIN, P_BASE, P_DENSE = pair(CHUNKS), pair(2), pair(1), pair(CHUNKS)
    P_ROWS, P_EXP, P_ALL = pair(1), pair(1), pair(1)
    P_RTP, P_RET = pair(1), pair(1)
    P_GATH, P_HAND, P_COLS, P_SQ = pair(CHUNKS), pair(CHUNKS), pair(1), pair(1)
    n_load = 13 + CHUNKS

    def kernel(
        tok_h, st_h, lb_h, hg_h, gn_h, wq_h, wf_h, wv_h, wo_h, wm_h, rt_h, sc_h,
        eg_h, eu_h, ed_h, dg_h, du_h, dd_h, mr_h,
        out, ns,
        tok, st, lb, hg, gn, win, wm, rt0, sc, wgu, wed, wd, wdd, mrow, wide_row,
        R, RP, RT, X, Y, Z, PR, rd, KC, VL, MA, TX, TR, STAT, SX, SR, COL, OWN, SEL, MO, MP, MR,
        FF, AX, AR, DX, DR, DH, OT, OX, ET, ER, EI, hid, RX, RR, RB, RG, dd, ddr, sq, sqr,
        send, recv, lsem,
    ):
        me_e, me_t = lax.axis_index("ep"), lax.axis_index("tp")
        q, c = me_e // 2, lax.rem(me_e, 2)
        partner = 2 * q + 1 - c
        chips = chips_by_distance(q, half)
        away = chips[:0:-1]
        far_first = [2 * kk + d for kk in away for d in (c, 1 - c)] + [partner]
        ep_peers = list(enumerate(far_first, 1))
        if n_tp == 4:
            turn_tp = [n_tp - 1 - me_t, lax.rem(me_t + 2, n_tp), me_t + 1 - 2 * lax.rem(me_t, 2)]
        else:
            turn_tp = [lax.rem(me_t + dt, n_tp) for dt in range(1, n_tp)]
        tp_peers = list(enumerate(turn_tp, 1))

        barrier = pltpu.get_barrier_semaphore()
        for _, e in ep_peers:
            pl.semaphore_signal(barrier, inc=1, device_id=(e, me_t), device_id_type=MESH)
        for _, t in tp_peers:
            pl.semaphore_signal(barrier, inc=1, device_id=(me_e, t), device_id_type=MESH)

        count = [0]

        def load(whole, *copies):
            at = count[0]
            count[0] += 1
            for src, dst in copies:
                pltpu.make_async_copy(src, dst, lsem.at[at]).start()
            return pltpu.make_async_copy(whole, whole, lsem.at[at])

        l_tok = load(tok, (tok_h, tok))
        l_gn = load(gn, (gn_h, gn))
        l_rt = load(rt0, (rt_h, rt0))
        l_in = load(
            win,
            *(
                (w.at[:, h * hs : (h + 1) * hs], win.at[h, :, i * hs : (i + 1) * hs])
                for h in range(heads)
                for i, w in enumerate((wq_h, wf_h, wv_h, wo_h))
            ),
        )
        l_small = [
            load(v, (h, v)) for h, v in ((lb_h, lb), (hg_h, hg), (sc_h, sc), (mr_h, mrow))
        ]
        l_st = load(st, (st_h, st))
        l_wm = load(wm, (wm_h, wm))
        l_wd = [
            load(
                wd.at[j, 0],
                *(
                    (
                        w.at[:, pl.ds(pl.multiple_of(j * chunk + c * hc, 128), hc)],
                        wd.at[j, c, :, i * hc : (i + 1) * hc],
                    )
                    for i, w in enumerate((dg_h, du_h))
                ),
            )
            for j in range(CHUNKS)
        ]
        l_exp = [
            load(
                wgu,
                *(
                    (
                        w.at[0, :, i * tile : (i + 1) * tile],
                        wgu.at[:, (2 * i + k) * tile : (2 * i + k + 1) * tile],
                    )
                    for i in range(eff // tile)
                    for k, w in enumerate((eg_h, eu_h))
                ),
            ),
            load(wed, (ed_h.at[0], wed)),
        ]
        l_wdd = load(wdd, (dd_h, wdd))

        def put(src, dst, device, s, r):
            pltpu.make_async_remote_copy(
                src_ref=src,
                dst_ref=dst,
                send_sem=send.at[s],
                recv_sem=recv.at[r],
                device_id=device,
                device_id_type=MESH,
            ).start()

        def arrive(whole, r):
            pltpu.make_async_copy(whole, whole, recv.at[r]).wait()

        def left(whole, s):
            pltpu.make_async_copy(whole, whole, send.at[s]).wait()

        others, peers, far = n_ep - 1, n_tp - 1, half - 1

        def cut(first, size):
            return pl.ds(pl.multiple_of(first, 128), size)

        mine = cut(me_e * block, block)
        own_rows = pl.ds(pl.multiple_of(me_e * seqs, seqs), seqs)

        l_tok.wait()
        l_gn.wait()
        l_rt.wait()
        pl.semaphore_wait(barrier, n_ep + n_tp - 2)
        for de, e in ep_peers:
            put(tok.at[:, cut(e * block, block)], R.at[me_e], (e, me_t), P_TOK[0], P_TOK[1])
        for de, e in ep_peers:
            put(rt0, RT.at[me_e], (e, me_t), P_ROUTE[0], P_ROUTE[1])
        for j in range(CHUNKS):
            for i, w in enumerate((dg_h, du_h)):
                put(
                    w.at[:, cut(j * chunk + (1 - c) * hc, hc)],
                    wd.at[j, c, :, i * hc : (i + 1) * hc],
                    (partner, me_t),
                    P_SWAP[0],
                    P_SWAP[1] + j,
                )
        R[me_e] = tok[:, mine]
        RT[me_e] = rt0[...]
        resid = tok[...].astype(f32)
        scale0 = rms_scale(resid)
        g0 = gn[0:1, mine]
        g1 = gn[1:2, mine]
        g2 = gn[2:3, mine]
        l_in.wait()
        arrive(R.at[0:others], P_TOK[1])

        put(R, RP, (partner, me_t), P_TWIN[0], P_TWIN[1])
        scaled = (R[...].reshape(rows, block).astype(f32) * g0).astype(bf16)

        def project(h):
            piece = dot32(scaled, win[h]).astype(bf16)
            for e in range(n_ep):
                X[h, e % 2, e // 2] = piece[e * seqs : (e + 1) * seqs]
            put(X.at[h, 1 - c], Y.at[h], (partner, me_t), P_PAIR[0], P_PAIR[1] + h)

        def spread_head(h):
            arrive(Y.at[h], P_PAIR[1] + h)
            for kk in away:
                Z[h, kk] = (X[h, c, kk].astype(f32) + Y[h, kk].astype(f32)).astype(bf16)
                put(
                    Z.at[h, kk],
                    PR.at[h, q],
                    (2 * kk + c, me_t),
                    P_HEAD[0],
                    P_HEAD[1] + h,
                )
            PR[h, q] = (X[h, c, q].astype(f32) + Y[h, q].astype(f32)).astype(bf16)

        project(0)
        project(1)
        for h in range(heads):
            spread_head(h)
            if h + 2 < heads:
                project(h + 2)

        arrive(RT.at[0:others], P_ROUTE[1])
        short = lax.broadcasted_iota(i32, (rows, seqs), 1)
        turn = lax.broadcasted_iota(i32, (rows, seqs), 0)
        diagonal = short == turn - (turn // seqs) * seqs
        named = []
        for k in range(topk):
            across = jnp.concatenate(
                [jnp.broadcast_to(RT[e, k : k + 1, :], (seqs, seqs)) for e in range(n_ep)], axis=0
            )
            named.append(jnp.sum(jnp.where(diagonal, across, 0), axis=1, keepdims=True))
        lane = lax.broadcasted_iota(i32, (rows, lanes), 1)
        row = lax.broadcasted_iota(i32, (rows, lanes), 0)
        ones = [(lane == named[k]).astype(f32) for k in range(topk)]
        earlier = ((lane < row) & (lane >= (row // seqs) * seqs)).astype(bf16)
        before = dot32(earlier, sum(ones).astype(bf16))
        slots = [
            jnp.sum(o * before, axis=1, keepdims=True).astype(i32) for o in ones
        ]
        spot = lax.broadcasted_iota(i32, (rows, 1), 0) // seqs
        wide = lax.broadcasted_iota(i32, (rows, n_ep * cells), 1)
        chosen = jnp.zeros((rows, n_ep * cells), f32)
        for k in range(topk):
            place = named[k] * cells + spot * cap + slots[k]
            chosen = chosen + (wide == place).astype(f32)
        per = lanes // cells
        for i in range(n_ep // per):
            flipped = chosen[:, i * lanes : (i + 1) * lanes].T.astype(bf16)
            SEL[i * per : (i + 1) * per] = flipped.reshape(per, n_tp, few, rows)

        def pick(base, ox):
            lhs = SEL[:, pl.ds(me_t, 1)].reshape(n_ep * few, rows)
            picked = dot32(lhs, base[...].reshape(rows, block)).astype(bf16)
            for e in range(n_ep):
                ox[e] = picked[e * few : (e + 1) * few]

        pick(R, OT)
        ET[:, mine] = OT[me_e]
        ours = jnp.zeros((rows, lanes), i32)
        for k in range(topk):
            ours = ours + jnp.where(lane == k, named[k] * cap + slots[k], 0)
        OWN[...] = ours
        for copy in l_small:
            copy.wait()
        wide_row[...] = mrow[...].astype(f32)
        at_own = OWN[own_rows, :]
        spread = lax.broadcasted_iota(i32, (seqs, cells), 1)
        gap = jnp.sum(
            jnp.where(diagonal[0:seqs], jnp.broadcast_to(sc[0:1, :] - sc[1:2, :], (seqs, seqs)), 0.0),
            axis=1,
            keepdims=True,
        )
        table = jnp.where(spread == at_own[:, 0:1], jax.nn.sigmoid(gap), 0.0)
        table = table + jnp.where(spread == at_own[:, 1:2], jax.nn.sigmoid(-gap), 0.0)

        arrive(RP, P_TWIN[1])

        def gains_of(device):
            return gn[2:3, cut(device * block, block)]

        FF[c] = (R[...].reshape(rows, block).astype(f32) * g2).astype(bf16)
        FF[1 - c] = (RP[...].reshape(rows, block).astype(f32) * gains_of(partner)).astype(bf16)

        def dense_part(j, ox, to):
            piece = (dot32(FF[0], wd[j, 0]) + dot32(FF[1], wd[j, 1])).astype(bf16)
            for kk in range(half):
                ox[kk] = piece[kk * duo : (kk + 1) * duo]
            to[q] = ox[q]

        def dense_send(ox, to, s, r):
            for kk in away:
                put(ox.at[kk], to.at[q], (2 * kk + c, me_t), s, r)

        for j in range(CHUNKS):
            l_wd[j].wait()
            arrive(wd.at[j, 0], P_SWAP[1] + j)
        for j in range(EARLY):
            dense_part(j, AX.at[j], AR.at[j])

        l_st.wait()
        for h in range(heads):
            arrive(PR.at[h, 0:far], P_HEAD[1] + h)
            total = PR[h, 0].astype(f32)
            for kk in range(1, half):
                total = total + PR[h, kk].astype(f32)
            total = total * scale0
            at = slice(h * hs, (h + 1) * hs)
            bound = lb[0:1, at]
            raw = total[:, hs : 2 * hs]
            forget = bound + (1.0 - bound) * jax.nn.sigmoid(raw)
            key_in = (1.0 - bound) * jax.nn.sigmoid(-raw)
            query = silu(total[:, 0:hs])
            value = total[:, 2 * hs : 3 * hs]
            columns = jnp.concatenate(
                [forget, key_in, query * forget, jnp.zeros((hs - 3 * seqs, hs), f32)], axis=0
            ).T
            KC[h] = columns
            VL[h] = value
            for s in range(seqs):
                rd[s : s + 1, :] = jnp.sum(
                    columns[:, 2 * seqs + s : 2 * seqs + s + 1] * st[s, h], axis=0, keepdims=True
                )
            read = rd[...] + jnp.sum(query * key_in, axis=1, keepdims=True) * value
            gated = read * rms_scale(read) * hg[0:1, at] * silu(total[:, 3 * hs :])
            MA[h, me_e] = gated.astype(bf16)
            for de, e in ep_peers:
                put(
                    MA.at[h, me_e],
                    MA.at[h, me_e],
                    (e, me_t),
                    P_MIX[0],
                    P_MIX[1] + q,
                )

        def update(h):
            for s in range(seqs):
                ns[s, h] = (
                    KC[h, :, s : s + 1] * st[s, h]
                    + KC[h, :, seqs + s : seqs + s + 1] * VL[h, s : s + 1, :]
                )

        update(0)
        update(1)
        for de, e in ep_peers:
            put(OT.at[e], ET.at[:, mine], (e, me_t), P_ROWS[0], P_ROWS[1])

        l_wm.wait()
        for g, kk in enumerate(chips):
            arrive(MA.at[:, 0 : 2 if g else 1], P_MIX[1] + kk)
            lhs = jnp.concatenate(
                [MA[h, pl.ds(2 * kk, 2)].reshape(duo, hs) for h in range(heads)], axis=1
            )
            piece = dot32(lhs, wm[...]).astype(bf16)
            TX[kk] = piece
            TR[me_t, kk] = piece
            for dt, t in tp_peers:
                put(
                    TX.at[kk],
                    TR.at[me_t, kk],
                    (me_e, t),
                    P_TP[0],
                    P_TP[1] + kk,
                )
        for j in range(EARLY):
            dense_send(AX.at[j], AR.at[j], *P_BASE)
        lane_duo = lax.broadcasted_iota(i32, (duo, lanes), 1)
        mixer = jnp.concatenate(
            [
                wide_row[pl.ds(me_e * (block // lanes) + i, 1), :]
                for i in range(block // lanes)
            ],
            axis=1,
        )
        for kk in chips:
            arrive(TR.at[0:peers, 0], P_TP[1] + kk)
            total = TR[0, kk].astype(f32)
            for t in range(1, n_tp):
                total = total + TR[t, kk].astype(f32)
            narrow = total.astype(bf16)
            MO[pl.ds(2 * kk, 2)] = narrow.reshape(2, seqs, block)
            mixed = narrow.astype(f32)
            base = R[pl.ds(2 * kk, 2)].reshape(duo, block).astype(f32)
            lifted = mixed * g1
            figures = (
                base * base,
                mixed * mixed,
                base * lifted,
                lifted * lifted,
                base * g2 * mixer,
                lifted * g2 * mixer,
            )
            stat = jnp.zeros((duo, lanes), f32)
            for i, figure in enumerate(figures):
                stat = stat + jnp.where(
                    lane_duo == i, jnp.sum(figure, axis=1, keepdims=True), 0.0
                )
            STAT[kk] = stat
        put(MO, MP, (partner, me_t), P_TWIN[0], P_TWIN[1] + 1)
        SX[...] = STAT[...].reshape(rows, lanes).T[0:8, :]
        SR[me_e] = SX[...]
        for de, e in ep_peers:
            put(SX, SR.at[me_e], (e, me_t), P_STAT[0], P_STAT[1])
        pick(MO, OX)
        for de, e in ep_peers:
            put(OX.at[e], ER.at[:, mine], (e, me_t), P_EXP[0], P_EXP[1])
        ER[:, mine] = OX[me_e]

        FF[c] = (MO[...].reshape(rows, block).astype(f32) * (g1 * g2)).astype(bf16)
        arrive(MP, P_TWIN[1] + 1)
        both = gn[1:2, cut(partner * block, block)] * gains_of(partner)
        FF[1 - c] = (MP[...].reshape(rows, block).astype(f32) * both).astype(bf16)
        for j in range(EARLY):
            dense_part(j, DX.at[j], DR.at[j])
            dense_send(DX.at[j], DR.at[j], P_DENSE[0], P_DENSE[1] + j)

        def send_own():
            for _, e in ep_peers:
                put(
                    MO.at[e],
                    MR.at[lax.rem(me_e, ratio)],
                    (e, me_t),
                    P_OWN[0],
                    P_OWN[1] + lax.rem(me_e, ratio),
                )
            MR[lax.rem(me_e, ratio)] = MO[me_e]

        holds = me_e // ratio == me_t
        pl.when(holds)(send_own)
        update(2)
        update(3)

        arrive(SR.at[0:others], P_STAT[1])
        total = SR[0]
        for e in range(1, n_ep):
            total = total + SR[e]
        inv_mix = lax.rsqrt(total[1:2] / width + EPS)
        squares = total[0:1] + 2.0 * inv_mix * total[2:3] + inv_mix * inv_mix * total[3:4]
        inv_after = lax.rsqrt(jnp.maximum(squares, 0.0) / width + EPS)
        weight = jax.nn.sigmoid(inv_after * (total[4:5] + inv_mix * total[5:6]))
        back = jnp.where(row == 0, inv_mix, jnp.where(row == 1, inv_after, jnp.where(row == 2, weight, 0.0)))
        back = back.T
        COL[...] = back
        def normed(base, mixed, device):
            at = cut(device * block, block)
            after = base[...].reshape(rows, block).astype(f32)
            after = after + mixed[...].reshape(rows, block).astype(f32) * back[:, 0:1] * gn[1:2, at]
            return (after * back[:, 1:2] * gn[2:3, at]).astype(bf16)

        FF[c] = normed(R, MO, me_e)
        FF[1 - c] = normed(RP, MP, partner)
        for j in range(EARLY, CHUNKS):
            dense_part(j, DX.at[j], DR.at[j])
            dense_send(DX.at[j], DR.at[j], P_DENSE[0], P_DENSE[1] + j)

        arrive(OT.at[0:others], P_ROWS[1])
        arrive(OX.at[0:others], P_EXP[1])
        marks = jnp.dot(
            SEL[me_e, me_t].astype(f32),
            back,
            precision=lax.Precision.HIGHEST,
            preferred_element_type=f32,
        )
        share = pl.ds(pl.multiple_of(me_t * few, few), few)
        after = ET[...].astype(f32) + ER[...].astype(f32) * marks[:, 0:1] * gn[1:2, :]
        EI[share, :] = (after * marks[:, 1:2] * gn[2:3, :]).astype(bf16)
        for dt, t in tp_peers:
            put(EI.at[share], EI.at[share], (me_e, t), P_ALL[0], P_ALL[1])

        chip_rows = pl.ds(pl.multiple_of(q * duo, duo), duo)

        def hidden(j):
            arrive(DR.at[j, 0:far], P_DENSE[1] + j)
            total = DR[j, 0].astype(f32)
            for kk in range(1, half):
                total = total + DR[j, kk].astype(f32)
            if j == 0:
                arrive(AR.at[:, 0:far], P_BASE[1])
            if j < EARLY:
                base = AR[j, 0].astype(f32)
                for kk in range(1, half):
                    base = base + AR[j, kk].astype(f32)
                own = COL[chip_rows, :]
                total = (base + own[:, 0:1] * total) * own[:, 1:2]
            here = DH.at[j, c, q]
            here[...] = (silu(total[:, :hc]) * total[:, hc:]).astype(bf16)
            for kk in away:
                put(here, here, (2 * kk + c, me_t), P_GATH[0], P_GATH[1] + j)
            put(here, here, (partner, me_t), P_HAND[0], P_HAND[1] + j)

        def hand_over(j):
            arrive(DH.at[j, 0, 0:far], P_GATH[1] + j)
            for kk in away:
                here = DH.at[j, c, kk]
                put(here, here, (partner, me_t), P_HAND[0], P_HAND[1] + j)

        def gathered(j):
            arrive(DH.at[j, 0], P_HAND[1] + j)
            total = 0.0
            for i in range(2):
                at = j * chunk + i * hc
                total = total + dot32(DH[j, i].reshape(rows, hc), wdd[at : at + hc, :])
            return total

        for copy in l_exp:
            copy.wait()
        hidden(0)
        arrive(EI.at[0 : peers * few], P_ALL[1])

        @pl.loop(0, eff // tile)
        def _(i):
            both = dot32(EI[...], wgu[:, cut(i * 2 * tile, 2 * tile)])
            hid[:, cut(i * tile, tile)] = (silu(both[:, :tile]) * both[:, tile:]).astype(bf16)

        hidden(1)
        for dt, t in tp_peers + [(0, me_t)]:
            piece = dot32(hid[...], wed[:, cut(t * part, part)]).astype(bf16)
            if dt:
                RX[dt] = piece
                put(RX.at[dt], RR.at[me_t], (me_e, t), P_RTP[0], P_RTP[1])
            else:
                RR[me_t] = piece
        hidden(2)

        def give_back():
            arrive(RR.at[0:peers], P_RTP[1])
            total = RR[0].astype(f32)
            for t in range(1, n_tp):
                total = total + RR[t].astype(f32)
            total = total.astype(bf16)
            for e in range(n_ep):
                RB[e] = total[e * cap : (e + 1) * cap]
            RG[me_e] = RB[me_e]
            for de, e in ep_peers:
                put(RB.at[e], RG.at[me_e], (e, me_t), P_RET[0], P_RET[1])

        for j in range(CHUNKS):
            hand_over(j)
        give_back()
        l_wdd.wait()
        total = gathered(0)
        for j in range(1, CHUNKS):
            total = total + gathered(j)
        total = total.astype(bf16)
        for e in range(n_ep):
            dd[e] = total[e * seqs : (e + 1) * seqs]
        to = me_e // ratio
        landing = ddr.at[lax.rem(me_e, ratio), me_t]
        for _, e in ep_peers:
            put(dd.at[e], landing, (e, to), P_COLS[0], P_COLS[1])

        def keep():
            landing[...] = dd[me_e]

        pl.when(holds)(keep)
        pl.when(jnp.logical_not(holds))(
            lambda: put(dd.at[me_e], landing, (me_e, to), P_COLS[0], P_COLS[1])
        )

        arrive(RG.at[0:others], P_RET[1])
        expert_sum = jnp.dot(
            table,
            RG[...].astype(f32).reshape(cells, part),
            precision=lax.Precision.HIGHEST,
            preferred_element_type=f32,
        )
        own_cols = COL[own_rows, :]
        part_at = cut(me_t * part, part)
        for j in range(ratio):
            source = me_t * ratio + j

            def wait_own(j=j):
                arrive(MR.at[j], P_OWN[1] + j)

            pl.when(source != me_e)(wait_own)
        mix_own = jnp.concatenate([MR[j].astype(f32) for j in range(ratio)], axis=1)
        after_own = tok[:, part_at].astype(f32) + mix_own * own_cols[:, 0:1] * gn[1:2, part_at]
        pl.when(holds)(lambda: arrive(dd.at[0:others], P_COLS[1]))
        pl.when(jnp.logical_not(holds))(lambda: arrive(dd, P_COLS[1]))
        pieces = []
        for j in range(ratio):
            total = ddr[j, 0].astype(f32)
            for t in range(1, n_tp):
                total = total + ddr[j, t].astype(f32)
            pieces.append(total)
        ffn_out = expert_sum + own_cols[:, 2:3] * jnp.concatenate(pieces, axis=1)
        mass = jnp.sum(ffn_out * ffn_out, axis=1, keepdims=True)
        sq[...] = jnp.broadcast_to(mass, (seqs, lanes))
        sqr[me_t] = sq[...]
        for dt, t in tp_peers:
            put(sq, sqr.at[me_t], (me_e, t), P_SQ[0], P_SQ[1])
        arrive(sqr.at[0:peers], P_SQ[1])
        total = sqr[0]
        for t in range(1, n_tp):
            total = total + sqr[t]
        scale = lax.rsqrt(total[:, 0:1] / width + EPS)
        out[...] = (after_own + ffn_out * scale * gn[3:4, part_at]).astype(bf16)
        pl.when(holds)(lambda: left(MO.at[0:others], P_OWN[0]))
        pl.when(holds)(lambda: left(dd.at[0:others], P_COLS[0]))
        pl.when(jnp.logical_not(holds))(lambda: left(dd, P_COLS[0]))
        for whole, ends in (
            (R.at[0:others], P_TOK),
            (RT.at[0:others], P_ROUTE),
            (Y, P_PAIR),
            (Z.at[:, 0:far], P_HEAD),
            (MA.at[:, 0:others], P_MIX),
            (TR.at[0:peers], P_TP),
            (SR.at[0:others], P_STAT),
            (wd.at[:, 0], P_SWAP),
            (FF, P_TWIN),
            (AX.at[:, 0:far], P_BASE),
            (EI.at[0 : peers * few], P_ALL),
            (OT.at[0:others], P_ROWS),
            (OX.at[0:others], P_EXP),
            (DX.at[:, 0:far], P_DENSE),
            (DH.at[:, 0, 0:far], P_GATH),
            (DH.at[:, 0], P_HAND),
            (RR.at[0:peers], P_RTP),
            (RB.at[0:others], P_RET),
            (sqr.at[0:peers], P_SQ),
        ):
            left(whole, ends[0])

    vmem = pl.BlockSpec(memory_space=pltpu.VMEM)
    hbm = pl.BlockSpec(memory_space=pltpu.HBM)
    b = lambda *s: pltpu.VMEM(s, bf16)
    f = lambda *s: pltpu.VMEM(s, f32)
    n = lambda *s: pltpu.VMEM(s, i32)
    return pl.pallas_call(
        kernel,
        out_shape=(
            jax.ShapeDtypeStruct((seqs, part), bf16),
            pltpu.VMEM(old_state.shape, f32),
        ),
        in_specs=[hbm] * 19,
        out_specs=(vmem, vmem),
        scratch_shapes=[
            b(seqs, width),
            f(*old_state.shape),
            f(1, chans),
            f(1, chans),
            f(*norm_gains.shape),
            b(heads, block, 4 * hs),
            b(chans, block),
            n(topk, seqs),
            f(topk, seqs),
            b(width, 2 * eff),
            b(eff, width),
            b(CHUNKS, 2, block, chunk),
            b(dff, block),
            b(width // lanes, lanes),
            f(width // lanes, lanes),
            b(n_ep, seqs, block),
            b(n_ep, seqs, block),
            n(n_ep, topk, seqs),
            b(heads, 2, half, seqs, 4 * hs),
            b(heads, half, seqs, 4 * hs),
            b(heads, half, seqs, 4 * hs),
            b(heads, half, seqs, 4 * hs),
            f(seqs, hs),
            f(heads, hs, hs),
            f(heads, seqs, hs),
            b(heads, n_ep, seqs, hs),
            b(half, duo, block),
            b(n_tp, half, duo, block),
            f(half, duo, lanes),
            f(8, lanes),
            f(n_ep, 8, lanes),
            f(rows, lanes),
            n(rows, lanes),
            b(n_ep, n_tp, few, rows),
            b(n_ep, seqs, block),
            b(n_ep, seqs, block),
            b(ratio, seqs, block),
            b(2, rows, block),
            b(EARLY, half, duo, chunk),
            b(EARLY, half, duo, chunk),
            b(CHUNKS, half, duo, chunk),
            b(CHUNKS, half, duo, chunk),
            b(CHUNKS, 2, half, duo, hc),
            b(n_ep, few, block),
            b(n_ep, few, block),
            b(few, width),
            b(few, width),
            b(cells, width),
            b(cells, eff),
            b(n_tp, cells, part),
            b(n_tp, cells, part),
            b(n_ep, cap, part),
            b(n_ep, cap, part),
            b(n_ep, seqs, block),
            b(ratio, n_tp, seqs, block),
            f(seqs, lanes),
            f(n_tp, seqs, lanes),
            pltpu.SemaphoreType.DMA((send_at.used,)),
            pltpu.SemaphoreType.DMA((recv_at.used,)),
            pltpu.SemaphoreType.DMA((n_load,)),
        ],
        compiler_params=pltpu.CompilerParams(
            collective_id=1, has_side_effects=True, vmem_limit_bytes=40 * 1024 * 1024
        ),
        name="fused_layer",
    )(
        *(
            pltpu.with_memory_space_constraint(x, pltpu.HBM)
            for x in (
                tokens,
                old_state,
                bounds,
                head_gain,
                norm_gains,
                *in_weights,
                w_mix,
                routes,
                scores,
                *experts,
                *dense,
                mix_row,
            )
        )
    )


PIECES = 16


def write_out(layer_out, new_state):
    per = new_state.shape[0] // PIECES

    def kernel(small, big, small_to, big_to, sems):
        copies = [pltpu.make_async_copy(small, small_to, sems.at[PIECES])]
        for i in range(PIECES):
            at = pl.ds(i * per, per)
            copies.append(pltpu.make_async_copy(big.at[at], big_to.at[at], sems.at[i]))
        for copy in copies:
            copy.start()
        for copy in copies:
            copy.wait()

    vmem = pl.BlockSpec(memory_space=pltpu.VMEM)
    hbm = pl.BlockSpec(memory_space=pltpu.HBM)
    return pl.pallas_call(
        kernel,
        out_shape=(
            pltpu.HBM(layer_out.shape, layer_out.dtype),
            pltpu.HBM(new_state.shape, new_state.dtype),
        ),
        in_specs=[vmem] * 2,
        out_specs=(hbm, hbm),
        scratch_shapes=[pltpu.SemaphoreType.DMA((PIECES + 1,))],
        compiler_params=pltpu.CompilerParams(vmem_limit_bytes=1024 * 1024),
        name="write_out",
    )(
        pltpu.with_memory_space_constraint(layer_out, pltpu.VMEM),
        pltpu.with_memory_space_constraint(new_state, pltpu.VMEM),
    )


def fast_body(
    tokens,
    old_state,
    lower_bound,
    head_gain,
    norm_gains,
    w_query,
    w_forget,
    w_value,
    w_outgate,
    w_mix_out,
    routes,
    route_scores,
    w_exp_gate,
    w_exp_up,
    w_exp_down,
    w_dense_gate,
    w_dense_up,
    w_dense_down,
    dense_mix,
):
    layer_out, new_state = fused_layer(
        tokens,
        old_state,
        lower_bound[None, :],
        head_gain[None, :],
        norm_gains,
        (w_query, w_forget, w_value, w_outgate),
        w_mix_out,
        routes.T,
        route_scores.T,
        (w_exp_gate, w_exp_up, w_exp_down),
        (w_dense_gate, w_dense_up, w_dense_down),
        dense_mix.reshape(-1, 128),
        lax.axis_size("ep"),
        lax.axis_size("tp"),
    )
    return write_out(layer_out, new_state)


def solution(mesh):
    n_ep, n_tp = mesh.shape['ep'], mesh.shape['tp']
    fits = n_ep % n_tp == 0 and n_ep % 2 == 0 and n_ep * n_tp <= 64
    return jax.shard_map(
        fast_body if fits else body,
        mesh=mesh,
        in_specs=(
            P("ep", None),
            P("ep", "tp", None, None),
            P("tp"),
            P("tp"),
            P(),
            P("ep", "tp"),
            P("ep", "tp"),
            P("ep", "tp"),
            P("ep", "tp"),
            P("tp", "ep"),
            P("ep", None),
            P("ep", None),
            P("ep", None, "tp"),
            P("ep", None, "tp"),
            P("ep", "tp", None),
            P("ep", "tp"),
            P("ep", "tp"),
            P("tp", "ep"),
            P(),
        ),
        out_specs=(P("ep", "tp"), P("ep", "tp", None, None)),
        check_vma=False,
    )
```

```python
import jax
import jax.numpy as jnp
from jax import lax
from jax.experimental import pallas as pl
from jax.experimental.pallas import tpu as pltpu
from jax.sharding import PartitionSpec as P

EPS = 1e-06


def rms_scale(values):
    return lax.rsqrt(jnp.mean(values * values, axis=-1, keepdims=True) + EPS)


def body(
    tokens,
    old_state,
    lower_bound,
    head_gain,
    norm_gains,
    w_query,
    w_forget,
    w_value,
    w_outgate,
    w_mix_out,
    routes,
    route_scores,
    w_exp_gate,
    w_exp_up,
    w_exp_down,
    w_dense_gate,
    w_dense_up,
    w_dense_down,
    dense_mix,
):
    highest = lax.Precision.HIGHEST
    seqs, width = tokens.shape
    column_index = lax.axis_index("tp")
    part_width = width // lax.axis_size("tp")
    resid = tokens.astype(jnp.float32)
    normed = (resid * rms_scale(resid) * norm_gains[0]).astype(jnp.bfloat16)
    in_weights = jnp.concatenate([w_query, w_forget, w_value, w_outgate], axis=1)
    mix_rows = lax.all_to_all(normed, "ep", split_axis=1, concat_axis=0, tiled=True)
    projected = lax.psum_scatter(
        jnp.dot(mix_rows, in_weights, preferred_element_type=jnp.float32).astype(jnp.bfloat16),
        "ep",
        scatter_dimension=0,
        tiled=True,
    ).astype(jnp.float32)
    query_raw, forget_raw, value, out_gate = jnp.split(projected, 4, axis=1)
    heads = old_state.shape[1]
    head_size = old_state.shape[2]
    shape_heads = (seqs, heads, head_size)
    forget = lower_bound + (1.0 - lower_bound) * jax.nn.sigmoid(forget_raw)
    key_in = (1.0 - lower_bound) * jax.nn.sigmoid(-forget_raw)
    new_state = forget.reshape(shape_heads)[..., None] * old_state + key_in.reshape(shape_heads)[
        ..., None
    ] * value.reshape(seqs, heads, 1, head_size)
    query = jax.nn.silu(query_raw).reshape(shape_heads)
    read = jnp.einsum("thk,thkv->thv", query, new_state, precision=highest)
    gated = (
        read
        * rms_scale(read)
        * head_gain.reshape(heads, head_size)
        * jax.nn.silu(out_gate).reshape(shape_heads)
    )
    mixed_heads = gated.reshape(seqs, heads * head_size).astype(jnp.bfloat16)
    mix_part = jnp.dot(
        mixed_heads,
        lax.all_gather(w_mix_out, "ep", axis=1, tiled=True),
        preferred_element_type=jnp.float32,
    ).astype(jnp.bfloat16)
    mix_part = lax.optimization_barrier(mix_part).astype(jnp.float32)
    mix_out = lax.psum(mix_part.astype(jnp.bfloat16), "tp")
    mix_wide = lax.optimization_barrier(mix_out).astype(jnp.float32)
    after_mix = resid + mix_wide * rms_scale(mix_wide) * norm_gains[1]
    ffn_in = (after_mix * rms_scale(after_mix) * norm_gains[2]).astype(jnp.bfloat16)
    experts = lax.axis_size("ep")
    topk = routes.shape[1]
    capacity = max(2, 2 * seqs * topk // experts)
    flat_routes = routes.reshape(-1)
    onehot = (flat_routes[:, None] == jnp.arange(experts, dtype=jnp.int32)[None, :]).astype(
        jnp.int32
    )
    before = jnp.cumsum(onehot, axis=0) - onehot
    slots = jnp.sum(onehot * before, axis=1)
    cells = flat_routes * capacity + slots
    placed = cells[None, :] == jnp.arange(experts * capacity, dtype=jnp.int32)[:, None]
    repeated = jnp.repeat(ffn_in, topk, axis=0)
    outgoing = jnp.dot(placed.astype(jnp.bfloat16), repeated, preferred_element_type=jnp.float32)
    outgoing = outgoing.astype(jnp.bfloat16).reshape(experts, capacity, width)
    arrived = lax.all_to_all(outgoing, "ep", split_axis=0, concat_axis=0, tiled=True)
    sources, items, _ = arrived.shape
    expert_rows = arrived.reshape(sources * items, width)
    gate_pre = jnp.dot(expert_rows, w_exp_gate[0], preferred_element_type=jnp.float32)
    up_pre = jnp.dot(expert_rows, w_exp_up[0], preferred_element_type=jnp.float32)
    hidden = (jax.nn.silu(gate_pre) * up_pre).astype(jnp.bfloat16)
    partial_rows = jnp.dot(hidden, w_exp_down[0], preferred_element_type=jnp.float32).astype(
        jnp.bfloat16
    )
    partial_rows = lax.optimization_barrier(partial_rows).astype(jnp.float32)
    partial_rows = partial_rows.reshape(sources, items, width)
    summed = lax.psum_scatter(
        partial_rows.astype(jnp.bfloat16), "tp", scatter_dimension=2, tiled=True
    )
    returned = lax.all_to_all(summed, "ep", split_axis=0, concat_axis=0, tiled=True)
    first = jax.nn.sigmoid(route_scores[:, 0] - route_scores[:, 1])
    second = jax.nn.sigmoid(route_scores[:, 1] - route_scores[:, 0])
    route_weight = jnp.stack([first, second], axis=1).reshape(-1)
    weight_table = jnp.sum(
        (placed.astype(jnp.float32) * route_weight[None, :]).reshape(
            experts * capacity, seqs, topk
        ),
        axis=2,
    )
    expert_sum = jnp.dot(
        weight_table.T,
        returned.reshape(experts * capacity, part_width).astype(jnp.float32),
        precision=highest,
    )
    dense_weights = jnp.concatenate([w_dense_gate, w_dense_up], axis=1)
    dense_rows = lax.all_to_all(ffn_in, "ep", split_axis=1, concat_axis=0, tiled=True)
    dense_pre = lax.psum_scatter(
        jnp.dot(dense_rows, dense_weights, preferred_element_type=jnp.float32).astype(jnp.bfloat16),
        "ep",
        scatter_dimension=0,
        tiled=True,
    ).astype(jnp.float32)
    dense_gate_pre, dense_up_pre = jnp.split(dense_pre, 2, axis=1)
    dense_hidden = (jax.nn.silu(dense_gate_pre) * dense_up_pre).astype(jnp.bfloat16)
    dense_partial = jnp.dot(
        dense_hidden,
        lax.all_gather(w_dense_down, "ep", axis=1, tiled=True),
        preferred_element_type=jnp.float32,
    )
    dense_out = lax.psum_scatter(
        dense_partial.astype(jnp.bfloat16), "tp", scatter_dimension=1, tiled=True
    ).astype(jnp.float32)
    mix_weight = jax.nn.sigmoid(jnp.dot(ffn_in, dense_mix, preferred_element_type=jnp.float32))
    ffn_out = expert_sum + mix_weight[:, None] * dense_out
    squares = lax.psum(jnp.sum(ffn_out * ffn_out, axis=1), "tp")
    out_scale = lax.rsqrt(squares / width + EPS)
    gain_part = lax.dynamic_slice_in_dim(norm_gains[3], column_index * part_width, part_width, 0)
    resid_part = lax.dynamic_slice_in_dim(after_mix, column_index * part_width, part_width, 1)
    layer_out = (resid_part + ffn_out * out_scale[:, None] * gain_part).astype(jnp.bfloat16)
    return (layer_out, new_state)


def dot32(a, b):
    return jnp.dot(a, b, preferred_element_type=jnp.float32)


def silu(x):
    return x * jax.nn.sigmoid(x)


MESH = pl.DeviceIdType.MESH


class Sems:
    def __init__(self):
        self.used = 0

    def take(self, count):
        first = self.used
        self.used += count
        return first


def chips_by_distance(q, half):
    if half == 4:
        return [q, q + 1 - 2 * lax.rem(q, 2), 2 - q // 2, 3 - 3 * (q // 2)]
    return [q] + [lax.rem(q + k, half) for k in range(1, half)]


CHUNKS = 3
EARLY = 1


def fused_layer(
    tokens,
    old_state,
    bounds,
    head_gain,
    norm_gains,
    in_weights,
    w_mix,
    routes,
    scores,
    experts,
    dense,
    mix_row,
    n_ep,
    n_tp,
):
    bf16, f32, i32 = jnp.bfloat16, jnp.float32, jnp.int32
    seqs, width = tokens.shape
    heads, hs = old_state.shape[1:3]
    block, part = width // n_ep, width // n_tp
    chans = heads * hs
    topk = routes.shape[0]
    cap = max(2, 2 * seqs * topk // n_ep)
    cells, rows = n_ep * cap, n_ep * seqs
    eff, dff = experts[0].shape[2], dense[0].shape[1]
    half, ratio = n_ep // 2, n_ep // n_tp
    duo = 2 * seqs
    lanes = 128
    tile = 128
    chunk = dff // CHUNKS
    hc = chunk // 2
    few = ratio * cap

    send_at, recv_at = Sems(), Sems()

    def pair(count):
        return send_at.take(1), recv_at.take(count)

    P_TOK, P_ROUTE, P_PAIR, P_HEAD = pair(1), pair(1), pair(heads), pair(heads)
    V_DENSE = recv_at.take(CHUNKS)
    P_MIX, P_TP, P_STAT, P_OWN = pair(half), pair(half), pair(1), pair(ratio)
    P_SWAP, P_TWIN, P_BASE, P_DENSE = pair(CHUNKS), pair(2), pair(1), pair(CHUNKS)
    P_ROWS, P_EXP, P_ALL = pair(1), pair(1), pair(1)
    P_RTP, P_RET = pair(1), pair(1)
    P_GATH, P_HAND, P_COLS, P_SQ = pair(CHUNKS), pair(CHUNKS), pair(1), pair(1)
    n_load = 13 + CHUNKS

    def kernel(
        tok_h, st_h, lb_h, hg_h, gn_h, wq_h, wf_h, wv_h, wo_h, wm_h, rt_h, sc_h,
        eg_h, eu_h, ed_h, dg_h, du_h, dd_h, mr_h,
        out, ns,
        tok, st, lb, hg, gn, win, wm, rt0, sc, wgu, wed, wd, wdd, mrow, wide_row,
        R, RP, RT, X, Y, Z, VD, PR, rd, KC, VL, MA, TX, TR, STAT, SX, SR, COL, OWN, SEL, MO, MP, MR,
        FF, AX, AR, DX, DR, DH, OT, OX, ET, ER, EI, hid, RX, RR, RB, RG, dd, ddr, sq, sqr,
        send, recv, lsem,
    ):
        me_e, me_t = lax.axis_index("ep"), lax.axis_index("tp")
        q, c = me_e // 2, lax.rem(me_e, 2)
        partner = 2 * q + 1 - c
        chips = chips_by_distance(q, half)
        away = chips[:0:-1]
        line = half == 4
        at_end = lax.rem(q, 3) == 0
        beside = 1 + q // 3
        near = away[1:] if line else away

        def landed(ref, r):
            if line:
                pl.when(at_end)(lambda: arrive(ref.at[0 : far - 1], r))
                pl.when(jnp.logical_not(at_end))(lambda: arrive(ref.at[0:far], r))
            else:
                arrive(ref.at[0:far], r)

        def through(ox, via, s, r):
            if line:
                pl.when(at_end)(
                    lambda: put(ox.at[away[0]], via, (2 * beside + c, me_t), s, r)
                )

        def relay(j):
            def run():
                arrive(VD.at[j], V_DENSE + j)
                total = DX[j, away[0]].astype(f32) + VD[j].astype(f32)
                DX[j, away[0]] = total.astype(bf16)
                put(
                    DX.at[j, away[0]],
                    DR.at[j, q],
                    (2 * away[0] + c, me_t),
                    P_DENSE[0],
                    P_DENSE[1] + j,
                )

            def clear():
                DR[j, away[0]] = jnp.zeros((duo, chunk), bf16)

            if line:
                pl.when(jnp.logical_not(at_end))(run)
                pl.when(at_end)(clear)
        far_first = [2 * kk + d for kk in away for d in (c, 1 - c)] + [partner]
        ep_peers = list(enumerate(far_first, 1))
        if n_tp == 4:
            turn_tp = [n_tp - 1 - me_t, lax.rem(me_t + 2, n_tp), me_t + 1 - 2 * lax.rem(me_t, 2)]
        else:
            turn_tp = [lax.rem(me_t + dt, n_tp) for dt in range(1, n_tp)]
        tp_peers = list(enumerate(turn_tp, 1))

        barrier = pltpu.get_barrier_semaphore()
        for _, e in ep_peers:
            pl.semaphore_signal(barrier, inc=1, device_id=(e, me_t), device_id_type=MESH)
        for _, t in tp_peers:
            pl.semaphore_signal(barrier, inc=1, device_id=(me_e, t), device_id_type=MESH)

        count = [0]

        def load(whole, *copies):
            at = count[0]
            count[0] += 1
            for src, dst in copies:
                pltpu.make_async_copy(src, dst, lsem.at[at]).start()
            return pltpu.make_async_copy(whole, whole, lsem.at[at])

        l_tok = load(tok, (tok_h, tok))
        l_gn = load(gn, (gn_h, gn))
        l_rt = load(rt0, (rt_h, rt0))
        l_in = load(
            win,
            *(
                (w.at[:, h * hs : (h + 1) * hs], win.at[h, :, i * hs : (i + 1) * hs])
                for h in range(heads)
                for i, w in enumerate((wq_h, wf_h, wv_h, wo_h))
            ),
        )
        l_small = [
            load(v, (h, v)) for h, v in ((lb_h, lb), (hg_h, hg), (sc_h, sc), (mr_h, mrow))
        ]
        l_st = load(st, (st_h, st))
        l_wm = load(wm, (wm_h, wm))
        l_wd = [
            load(
                wd.at[j, 0],
                *(
                    (
                        w.at[:, pl.ds(pl.multiple_of(j * chunk + c * hc, 128), hc)],
                        wd.at[j, c, :, i * hc : (i + 1) * hc],
                    )
                    for i, w in enumerate((dg_h, du_h))
                ),
            )
            for j in range(CHUNKS)
        ]
        l_exp = [
            load(
                wgu,
                *(
                    (
                        w.at[0, :, i * tile : (i + 1) * tile],
                        wgu.at[:, (2 * i + k) * tile : (2 * i + k + 1) * tile],
                    )
                    for i in range(eff // tile)
                    for k, w in enumerate((eg_h, eu_h))
                ),
            ),
            load(wed, (ed_h.at[0], wed)),
        ]
        l_wdd = load(wdd, (dd_h, wdd))

        def put(src, dst, device, s, r):
            pltpu.make_async_remote_copy(
                src_ref=src,
                dst_ref=dst,
                send_sem=send.at[s],
                recv_sem=recv.at[r],
                device_id=device,
                device_id_type=MESH,
            ).start()

        def arrive(whole, r):
            pltpu.make_async_copy(whole, whole, recv.at[r]).wait()

        def left(whole, s):
            pltpu.make_async_copy(whole, whole, send.at[s]).wait()

        others, peers, far = n_ep - 1, n_tp - 1, half - 1

        def cut(first, size):
            return pl.ds(pl.multiple_of(first, 128), size)

        mine = cut(me_e * block, block)
        own_rows = pl.ds(pl.multiple_of(me_e * seqs, seqs), seqs)

        l_tok.wait()
        l_gn.wait()
        l_rt.wait()
        pl.semaphore_wait(barrier, n_ep + n_tp - 2)
        for de, e in ep_peers:
            put(tok.at[:, cut(e * block, block)], R.at[me_e], (e, me_t), P_TOK[0], P_TOK[1])
        for de, e in ep_peers:
            put(rt0, RT.at[me_e], (e, me_t), P_ROUTE[0], P_ROUTE[1])
        for j in range(CHUNKS):
            for i, w in enumerate((dg_h, du_h)):
                put(
                    w.at[:, cut(j * chunk + (1 - c) * hc, hc)],
                    wd.at[j, c, :, i * hc : (i + 1) * hc],
                    (partner, me_t),
                    P_SWAP[0],
                    P_SWAP[1] + j,
                )
        R[me_e] = tok[:, mine]
        RT[me_e] = rt0[...]
        resid = tok[...].astype(f32)
        scale0 = rms_scale(resid)
        g0 = gn[0:1, mine]
        g1 = gn[1:2, mine]
        g2 = gn[2:3, mine]
        l_in.wait()
        arrive(R.at[0:others], P_TOK[1])

        put(R, RP, (partner, me_t), P_TWIN[0], P_TWIN[1])
        scaled = (R[...].reshape(rows, block).astype(f32) * g0).astype(bf16)

        def project(h):
            piece = dot32(scaled, win[h]).astype(bf16)
            for e in range(n_ep):
                X[h, e % 2, e // 2] = piece[e * seqs : (e + 1) * seqs]
            put(X.at[h, 1 - c], Y.at[h], (partner, me_t), P_PAIR[0], P_PAIR[1] + h)

        def spread_head(h):
            arrive(Y.at[h], P_PAIR[1] + h)
            for kk in away:
                Z[h, kk] = (X[h, c, kk].astype(f32) + Y[h, kk].astype(f32)).astype(bf16)
                put(
                    Z.at[h, kk],
                    PR.at[h, q],
                    (2 * kk + c, me_t),
                    P_HEAD[0],
                    P_HEAD[1] + h,
                )
            PR[h, q] = (X[h, c, q].astype(f32) + Y[h, q].astype(f32)).astype(bf16)

        project(0)
        project(1)
        for h in range(heads):
            spread_head(h)
            if h + 2 < heads:
                project(h + 2)

        arrive(RT.at[0:others], P_ROUTE[1])
        short = lax.broadcasted_iota(i32, (rows, seqs), 1)
        turn = lax.broadcasted_iota(i32, (rows, seqs), 0)
        diagonal = short == turn - (turn // seqs) * seqs
        named = []
        for k in range(topk):
            across = jnp.concatenate(
                [jnp.broadcast_to(RT[e, k : k + 1, :], (seqs, seqs)) for e in range(n_ep)], axis=0
            )
            named.append(jnp.sum(jnp.where(diagonal, across, 0), axis=1, keepdims=True))
        lane = lax.broadcasted_iota(i32, (rows, lanes), 1)
        row = lax.broadcasted_iota(i32, (rows, lanes), 0)
        ones = [(lane == named[k]).astype(f32) for k in range(topk)]
        earlier = ((lane < row) & (lane >= (row // seqs) * seqs)).astype(bf16)
        before = dot32(earlier, sum(ones).astype(bf16))
        slots = [
            jnp.sum(o * before, axis=1, keepdims=True).astype(i32) for o in ones
        ]
        spot = lax.broadcasted_iota(i32, (rows, 1), 0) // seqs
        wide = lax.broadcasted_iota(i32, (rows, n_ep * cells), 1)
        chosen = jnp.zeros((rows, n_ep * cells), f32)
        for k in range(topk):
            place = named[k] * cells + spot * cap + slots[k]
            chosen = chosen + (wide == place).astype(f32)
        per = lanes // cells
        for i in range(n_ep // per):
            flipped = chosen[:, i * lanes : (i + 1) * lanes].T.astype(bf16)
            SEL[i * per : (i + 1) * per] = flipped.reshape(per, n_tp, few, rows)

        def pick(base, ox):
            lhs = SEL[:, pl.ds(me_t, 1)].reshape(n_ep * few, rows)
            picked = dot32(lhs, base[...].reshape(rows, block)).astype(bf16)
            for e in range(n_ep):
                ox[e] = picked[e * few : (e + 1) * few]

        pick(R, OT)
        ET[:, mine] = OT[me_e]
        ours = jnp.zeros((rows, lanes), i32)
        for k in range(topk):
            ours = ours + jnp.where(lane == k, named[k] * cap + slots[k], 0)
        OWN[...] = ours
        for copy in l_small:
            copy.wait()
        wide_row[...] = mrow[...].astype(f32)
        at_own = OWN[own_rows, :]
        spread = lax.broadcasted_iota(i32, (seqs, cells), 1)
        gap = jnp.sum(
            jnp.where(diagonal[0:seqs], jnp.broadcast_to(sc[0:1, :] - sc[1:2, :], (seqs, seqs)), 0.0),
            axis=1,
            keepdims=True,
        )
        table = jnp.where(spread == at_own[:, 0:1], jax.nn.sigmoid(gap), 0.0)
        table = table + jnp.where(spread == at_own[:, 1:2], jax.nn.sigmoid(-gap), 0.0)

        arrive(RP, P_TWIN[1])

        def gains_of(device):
            return gn[2:3, cut(device * block, block)]

        FF[c] = (R[...].reshape(rows, block).astype(f32) * g2).astype(bf16)
        FF[1 - c] = (RP[...].reshape(rows, block).astype(f32) * gains_of(partner)).astype(bf16)

        def dense_part(j, ox, to):
            piece = (dot32(FF[0], wd[j, 0]) + dot32(FF[1], wd[j, 1])).astype(bf16)
            for kk in range(half):
                ox[kk] = piece[kk * duo : (kk + 1) * duo]
            to[q] = ox[q]

        def dense_send(ox, to, s, r, direct=away):
            for kk in direct:
                put(ox.at[kk], to.at[q], (2 * kk + c, me_t), s, r)

        for j in range(CHUNKS):
            l_wd[j].wait()
            arrive(wd.at[j, 0], P_SWAP[1] + j)
        for j in range(EARLY):
            dense_part(j, AX.at[j], AR.at[j])

        l_st.wait()
        for h in range(heads):
            arrive(PR.at[h, 0:far], P_HEAD[1] + h)
            total = PR[h, 0].astype(f32)
            for kk in range(1, half):
                total = total + PR[h, kk].astype(f32)
            total = total * scale0
            at = slice(h * hs, (h + 1) * hs)
            bound = lb[0:1, at]
            raw = total[:, hs : 2 * hs]
            forget = bound + (1.0 - bound) * jax.nn.sigmoid(raw)
            key_in = (1.0 - bound) * jax.nn.sigmoid(-raw)
            query = silu(total[:, 0:hs])
            value = total[:, 2 * hs : 3 * hs]
            columns = jnp.concatenate(
                [forget, key_in, query * forget, jnp.zeros((hs - 3 * seqs, hs), f32)], axis=0
            ).T
            KC[h] = columns
            VL[h] = value
            for s in range(seqs):
                rd[s : s + 1, :] = jnp.sum(
                    columns[:, 2 * seqs + s : 2 * seqs + s + 1] * st[s, h], axis=0, keepdims=True
                )
            read = rd[...] + jnp.sum(query * key_in, axis=1, keepdims=True) * value
            gated = read * rms_scale(read) * hg[0:1, at] * silu(total[:, 3 * hs :])
            MA[h, me_e] = gated.astype(bf16)
            for de, e in ep_peers:
                put(
                    MA.at[h, me_e],
                    MA.at[h, me_e],
                    (e, me_t),
                    P_MIX[0],
                    P_MIX[1] + q,
                )

        def update(h):
            for s in range(seqs):
                ns[s, h] = (
                    KC[h, :, s : s + 1] * st[s, h]
                    + KC[h, :, seqs + s : seqs + s + 1] * VL[h, s : s + 1, :]
                )

        update(0)
        update(1)
        for de, e in ep_peers:
            put(OT.at[e], ET.at[:, mine], (e, me_t), P_ROWS[0], P_ROWS[1])

        l_wm.wait()
        for g, kk in enumerate(chips):
            arrive(MA.at[:, 0 : 2 if g else 1], P_MIX[1] + kk)
            lhs = jnp.concatenate(
                [MA[h, pl.ds(2 * kk, 2)].reshape(duo, hs) for h in range(heads)], axis=1
            )
            piece = dot32(lhs, wm[...]).astype(bf16)
            TX[kk] = piece
            TR[me_t, kk] = piece
            for dt, t in tp_peers:
                put(
                    TX.at[kk],
                    TR.at[me_t, kk],
                    (me_e, t),
                    P_TP[0],
                    P_TP[1] + kk,
                )
        for j in range(EARLY):
            dense_send(AX.at[j], AR.at[j], *P_BASE)
        lane_duo = lax.broadcasted_iota(i32, (duo, lanes), 1)
        mixer = jnp.concatenate(
            [
                wide_row[pl.ds(me_e * (block // lanes) + i, 1), :]
                for i in range(block // lanes)
            ],
            axis=1,
        )
        for kk in chips:
            arrive(TR.at[0:peers, 0], P_TP[1] + kk)
            total = TR[0, kk].astype(f32)
            for t in range(1, n_tp):
                total = total + TR[t, kk].astype(f32)
            narrow = total.astype(bf16)
            MO[pl.ds(2 * kk, 2)] = narrow.reshape(2, seqs, block)
            mixed = narrow.astype(f32)
            base = R[pl.ds(2 * kk, 2)].reshape(duo, block).astype(f32)
            lifted = mixed * g1
            figures = (
                base * base,
                mixed * mixed,
                base * lifted,
                lifted * lifted,
                base * g2 * mixer,
                lifted * g2 * mixer,
            )
            stat = jnp.zeros((duo, lanes), f32)
            for i, figure in enumerate(figures):
                stat = stat + jnp.where(
                    lane_duo == i, jnp.sum(figure, axis=1, keepdims=True), 0.0
                )
            STAT[kk] = stat
        put(MO, MP, (partner, me_t), P_TWIN[0], P_TWIN[1] + 1)
        SX[...] = STAT[...].reshape(rows, lanes).T[0:8, :]
        SR[me_e] = SX[...]
        for de, e in ep_peers:
            put(SX, SR.at[me_e], (e, me_t), P_STAT[0], P_STAT[1])
        pick(MO, OX)
        for de, e in ep_peers:
            put(OX.at[e], ER.at[:, mine], (e, me_t), P_EXP[0], P_EXP[1])
        ER[:, mine] = OX[me_e]

        FF[c] = (MO[...].reshape(rows, block).astype(f32) * (g1 * g2)).astype(bf16)
        arrive(MP, P_TWIN[1] + 1)
        both = gn[1:2, cut(partner * block, block)] * gains_of(partner)
        FF[1 - c] = (MP[...].reshape(rows, block).astype(f32) * both).astype(bf16)
        for j in range(EARLY):
            dense_part(j, DX.at[j], DR.at[j])
            through(DX.at[j], VD.at[j], P_DENSE[0], V_DENSE + j)
            dense_send(DX.at[j], DR.at[j], P_DENSE[0], P_DENSE[1] + j, near)

        def send_own():
            for _, e in ep_peers:
                put(
                    MO.at[e],
                    MR.at[lax.rem(me_e, ratio)],
                    (e, me_t),
                    P_OWN[0],
                    P_OWN[1] + lax.rem(me_e, ratio),
                )
            MR[lax.rem(me_e, ratio)] = MO[me_e]

        holds = me_e // ratio == me_t
        pl.when(holds)(send_own)
        update(2)
        update(3)
        for j in range(EARLY):
            relay(j)

        arrive(SR.at[0:others], P_STAT[1])
        total = SR[0]
        for e in range(1, n_ep):
            total = total + SR[e]
        inv_mix = lax.rsqrt(total[1:2] / width + EPS)
        squares = total[0:1] + 2.0 * inv_mix * total[2:3] + inv_mix * inv_mix * total[3:4]
        inv_after = lax.rsqrt(jnp.maximum(squares, 0.0) / width + EPS)
        weight = jax.nn.sigmoid(inv_after * (total[4:5] + inv_mix * total[5:6]))
        back = jnp.where(row == 0, inv_mix, jnp.where(row == 1, inv_after, jnp.where(row == 2, weight, 0.0)))
        back = back.T
        COL[...] = back
        def normed(base, mixed, device):
            at = cut(device * block, block)
            after = base[...].reshape(rows, block).astype(f32)
            after = after + mixed[...].reshape(rows, block).astype(f32) * back[:, 0:1] * gn[1:2, at]
            return (after * back[:, 1:2] * gn[2:3, at]).astype(bf16)

        FF[c] = normed(R, MO, me_e)
        FF[1 - c] = normed(RP, MP, partner)
        for j in range(EARLY, CHUNKS):
            dense_part(j, DX.at[j], DR.at[j])
            through(DX.at[j], VD.at[j], P_DENSE[0], V_DENSE + j)
        for j in range(EARLY, CHUNKS):
            dense_send(DX.at[j], DR.at[j], P_DENSE[0], P_DENSE[1] + j, near)

        arrive(OT.at[0:others], P_ROWS[1])
        arrive(OX.at[0:others], P_EXP[1])
        marks = jnp.dot(
            SEL[me_e, me_t].astype(f32),
            back,
            precision=lax.Precision.HIGHEST,
            preferred_element_type=f32,
        )
        share = pl.ds(pl.multiple_of(me_t * few, few), few)
        after = ET[...].astype(f32) + ER[...].astype(f32) * marks[:, 0:1] * gn[1:2, :]
        EI[share, :] = (after * marks[:, 1:2] * gn[2:3, :]).astype(bf16)
        for dt, t in tp_peers:
            put(EI.at[share], EI.at[share], (me_e, t), P_ALL[0], P_ALL[1])

        for j in range(EARLY, CHUNKS):
            relay(j)
        chip_rows = pl.ds(pl.multiple_of(q * duo, duo), duo)

        def hidden(j):
            landed(DR.at[j], P_DENSE[1] + j)
            total = DR[j, 0].astype(f32)
            for kk in range(1, half):
                total = total + DR[j, kk].astype(f32)
            if j == 0:
                arrive(AR.at[:, 0:far], P_BASE[1])
            if j < EARLY:
                base = AR[j, 0].astype(f32)
                for kk in range(1, half):
                    base = base + AR[j, kk].astype(f32)
                own = COL[chip_rows, :]
                total = (base + own[:, 0:1] * total) * own[:, 1:2]
            here = DH.at[j, c, q]
            here[...] = (silu(total[:, :hc]) * total[:, hc:]).astype(bf16)
            for kk in away:
                put(here, here, (2 * kk + c, me_t), P_GATH[0], P_GATH[1] + j)
            put(here, here, (partner, me_t), P_HAND[0], P_HAND[1] + j)

        def hand_over(j):
            arrive(DH.at[j, 0, 0:far], P_GATH[1] + j)
            for kk in away:
                here = DH.at[j, c, kk]
                put(here, here, (partner, me_t), P_HAND[0], P_HAND[1] + j)

        def gathered(j):
            arrive(DH.at[j, 0], P_HAND[1] + j)
            total = 0.0
            for i in range(2):
                at = j * chunk + i * hc
                total = total + dot32(DH[j, i].reshape(rows, hc), wdd[at : at + hc, :])
            return total

        for copy in l_exp:
            copy.wait()
        hidden(0)
        arrive(EI.at[0 : peers * few], P_ALL[1])

        @pl.loop(0, eff // tile)
        def _(i):
            both = dot32(EI[...], wgu[:, cut(i * 2 * tile, 2 * tile)])
            hid[:, cut(i * tile, tile)] = (silu(both[:, :tile]) * both[:, tile:]).astype(bf16)

        hidden(1)
        for dt, t in (tp_peers + [(0, me_t)])[:2]:
            piece = dot32(hid[...], wed[:, cut(t * part, part)]).astype(bf16)
            if dt:
                RX[dt] = piece
                put(RX.at[dt], RR.at[me_t], (me_e, t), P_RTP[0], P_RTP[1])
            else:
                RR[me_t] = piece
        hidden(2)
        for dt, t in (tp_peers + [(0, me_t)])[2:]:
            piece = dot32(hid[...], wed[:, cut(t * part, part)]).astype(bf16)
            if dt:
                RX[dt] = piece
                put(RX.at[dt], RR.at[me_t], (me_e, t), P_RTP[0], P_RTP[1])
            else:
                RR[me_t] = piece

        def give_back():
            arrive(RR.at[0:peers], P_RTP[1])
            total = RR[0].astype(f32)
            for t in range(1, n_tp):
                total = total + RR[t].astype(f32)
            total = total.astype(bf16)
            for e in range(n_ep):
                RB[e] = total[e * cap : (e + 1) * cap]
            RG[me_e] = RB[me_e]
            for de, e in ep_peers:
                put(RB.at[e], RG.at[me_e], (e, me_t), P_RET[0], P_RET[1])

        for j in range(CHUNKS):
            hand_over(j)
        give_back()
        l_wdd.wait()
        total = gathered(0)
        for j in range(1, CHUNKS):
            total = total + gathered(j)
        total = total.astype(bf16)
        for e in range(n_ep):
            dd[e] = total[e * seqs : (e + 1) * seqs]
        to = me_e // ratio
        landing = ddr.at[lax.rem(me_e, ratio), me_t]
        for _, e in ep_peers:
            put(dd.at[e], landing, (e, to), P_COLS[0], P_COLS[1])

        def keep():
            landing[...] = dd[me_e]

        pl.when(holds)(keep)
        pl.when(jnp.logical_not(holds))(
            lambda: put(dd.at[me_e], landing, (me_e, to), P_COLS[0], P_COLS[1])
        )

        arrive(RG.at[0:others], P_RET[1])
        expert_sum = jnp.dot(
            table,
            RG[...].astype(f32).reshape(cells, part),
            precision=lax.Precision.HIGHEST,
            preferred_element_type=f32,
        )
        own_cols = COL[own_rows, :]
        part_at = cut(me_t * part, part)
        for j in range(ratio):
            source = me_t * ratio + j

            def wait_own(j=j):
                arrive(MR.at[j], P_OWN[1] + j)

            pl.when(source != me_e)(wait_own)
        mix_own = jnp.concatenate([MR[j].astype(f32) for j in range(ratio)], axis=1)
        after_own = tok[:, part_at].astype(f32) + mix_own * own_cols[:, 0:1] * gn[1:2, part_at]
        pl.when(holds)(lambda: arrive(dd.at[0:others], P_COLS[1]))
        pl.when(jnp.logical_not(holds))(lambda: arrive(dd, P_COLS[1]))
        pieces = []
        for j in range(ratio):
            total = ddr[j, 0].astype(f32)
            for t in range(1, n_tp):
                total = total + ddr[j, t].astype(f32)
            pieces.append(total)
        ffn_out = expert_sum + own_cols[:, 2:3] * jnp.concatenate(pieces, axis=1)
        mass = jnp.sum(ffn_out * ffn_out, axis=1, keepdims=True)
        sq[...] = jnp.broadcast_to(mass, (seqs, lanes))
        sqr[me_t] = sq[...]
        for dt, t in tp_peers:
            put(sq, sqr.at[me_t], (me_e, t), P_SQ[0], P_SQ[1])
        arrive(sqr.at[0:peers], P_SQ[1])
        total = sqr[0]
        for t in range(1, n_tp):
            total = total + sqr[t]
        scale = lax.rsqrt(total[:, 0:1] / width + EPS)
        out[...] = (after_own + ffn_out * scale * gn[3:4, part_at]).astype(bf16)
        pl.when(holds)(lambda: left(MO.at[0:others], P_OWN[0]))
        pl.when(holds)(lambda: left(dd.at[0:others], P_COLS[0]))
        pl.when(jnp.logical_not(holds))(lambda: left(dd, P_COLS[0]))
        for whole, ends in (
            (R.at[0:others], P_TOK),
            (RT.at[0:others], P_ROUTE),
            (Y, P_PAIR),
            (Z.at[:, 0:far], P_HEAD),
            (MA.at[:, 0:others], P_MIX),
            (TR.at[0:peers], P_TP),
            (SR.at[0:others], P_STAT),
            (wd.at[:, 0], P_SWAP),
            (FF, P_TWIN),
            (AX.at[:, 0:far], P_BASE),
            (EI.at[0 : peers * few], P_ALL),
            (OT.at[0:others], P_ROWS),
            (OX.at[0:others], P_EXP),
            (DX.at[:, 0:far], P_DENSE),
            (DH.at[:, 0, 0:far], P_GATH),
            (DH.at[:, 0], P_HAND),
            (RR.at[0:peers], P_RTP),
            (RB.at[0:others], P_RET),
            (sqr.at[0:peers], P_SQ),
        ):
            left(whole, ends[0])

    vmem = pl.BlockSpec(memory_space=pltpu.VMEM)
    hbm = pl.BlockSpec(memory_space=pltpu.HBM)
    b = lambda *s: pltpu.VMEM(s, bf16)
    f = lambda *s: pltpu.VMEM(s, f32)
    n = lambda *s: pltpu.VMEM(s, i32)
    return pl.pallas_call(
        kernel,
        out_shape=(
            jax.ShapeDtypeStruct((seqs, part), bf16),
            pltpu.VMEM(old_state.shape, f32),
        ),
        in_specs=[hbm] * 19,
        out_specs=(vmem, vmem),
        scratch_shapes=[
            b(seqs, width),
            f(*old_state.shape),
            f(1, chans),
            f(1, chans),
            f(*norm_gains.shape),
            b(heads, block, 4 * hs),
            b(chans, block),
            n(topk, seqs),
            f(topk, seqs),
            b(width, 2 * eff),
            b(eff, width),
            b(CHUNKS, 2, block, chunk),
            b(dff, block),
            b(width // lanes, lanes),
            f(width // lanes, lanes),
            b(n_ep, seqs, block),
            b(n_ep, seqs, block),
            n(n_ep, topk, seqs),
            b(heads, 2, half, seqs, 4 * hs),
            b(heads, half, seqs, 4 * hs),
            b(heads, half, seqs, 4 * hs),
            b(CHUNKS, duo, chunk),
            b(heads, half, seqs, 4 * hs),
            f(seqs, hs),
            f(heads, hs, hs),
            f(heads, seqs, hs),
            b(heads, n_ep, seqs, hs),
            b(half, duo, block),
            b(n_tp, half, duo, block),
            f(half, duo, lanes),
            f(8, lanes),
            f(n_ep, 8, lanes),
            f(rows, lanes),
            n(rows, lanes),
            b(n_ep, n_tp, few, rows),
            b(n_ep, seqs, block),
            b(n_ep, seqs, block),
            b(ratio, seqs, block),
            b(2, rows, block),
            b(EARLY, half, duo, chunk),
            b(EARLY, half, duo, chunk),
            b(CHUNKS, half, duo, chunk),
            b(CHUNKS, half, duo, chunk),
            b(CHUNKS, 2, half, duo, hc),
            b(n_ep, few, block),
            b(n_ep, few, block),
            b(few, width),
            b(few, width),
            b(cells, width),
            b(cells, eff),
            b(n_tp, cells, part),
            b(n_tp, cells, part),
            b(n_ep, cap, part),
            b(n_ep, cap, part),
            b(n_ep, seqs, block),
            b(ratio, n_tp, seqs, block),
            f(seqs, lanes),
            f(n_tp, seqs, lanes),
            pltpu.SemaphoreType.DMA((send_at.used,)),
            pltpu.SemaphoreType.DMA((recv_at.used,)),
            pltpu.SemaphoreType.DMA((n_load,)),
        ],
        compiler_params=pltpu.CompilerParams(
            collective_id=1, has_side_effects=True, vmem_limit_bytes=40 * 1024 * 1024
        ),
        name="fused_layer",
    )(
        *(
            pltpu.with_memory_space_constraint(x, pltpu.HBM)
            for x in (
                tokens,
                old_state,
                bounds,
                head_gain,
                norm_gains,
                *in_weights,
                w_mix,
                routes,
                scores,
                *experts,
                *dense,
                mix_row,
            )
        )
    )


PIECES = 16


def write_out(layer_out, new_state):
    per = new_state.shape[0] // PIECES

    def kernel(small, big, small_to, big_to, sems):
        copies = [pltpu.make_async_copy(small, small_to, sems.at[PIECES])]
        for i in range(PIECES):
            at = pl.ds(i * per, per)
            copies.append(pltpu.make_async_copy(big.at[at], big_to.at[at], sems.at[i]))
        for copy in copies:
            copy.start()
        for copy in copies:
            copy.wait()

    vmem = pl.BlockSpec(memory_space=pltpu.VMEM)
    hbm = pl.BlockSpec(memory_space=pltpu.HBM)
    return pl.pallas_call(
        kernel,
        out_shape=(
            pltpu.HBM(layer_out.shape, layer_out.dtype),
            pltpu.HBM(new_state.shape, new_state.dtype),
        ),
        in_specs=[vmem] * 2,
        out_specs=(hbm, hbm),
        scratch_shapes=[pltpu.SemaphoreType.DMA((PIECES + 1,))],
        compiler_params=pltpu.CompilerParams(vmem_limit_bytes=1024 * 1024),
        name="write_out",
    )(
        pltpu.with_memory_space_constraint(layer_out, pltpu.VMEM),
        pltpu.with_memory_space_constraint(new_state, pltpu.VMEM),
    )


def fast_body(
    tokens,
    old_state,
    lower_bound,
    head_gain,
    norm_gains,
    w_query,
    w_forget,
    w_value,
    w_outgate,
    w_mix_out,
    routes,
    route_scores,
    w_exp_gate,
    w_exp_up,
    w_exp_down,
    w_dense_gate,
    w_dense_up,
    w_dense_down,
    dense_mix,
):
    layer_out, new_state = fused_layer(
        tokens,
        old_state,
        lower_bound[None, :],
        head_gain[None, :],
        norm_gains,
        (w_query, w_forget, w_value, w_outgate),
        w_mix_out,
        routes.T,
        route_scores.T,
        (w_exp_gate, w_exp_up, w_exp_down),
        (w_dense_gate, w_dense_up, w_dense_down),
        dense_mix.reshape(-1, 128),
        lax.axis_size("ep"),
        lax.axis_size("tp"),
    )
    return write_out(layer_out, new_state)


def solution(mesh):
    n_ep, n_tp = mesh.shape['ep'], mesh.shape['tp']
    fits = n_ep % n_tp == 0 and n_ep % 2 == 0 and n_ep * n_tp <= 64
    return jax.shard_map(
        fast_body if fits else body,
        mesh=mesh,
        in_specs=(
            P("ep", None),
            P("ep", "tp", None, None),
            P("tp"),
            P("tp"),
            P(),
            P("ep", "tp"),
            P("ep", "tp"),
            P("ep", "tp"),
            P("ep", "tp"),
            P("tp", "ep"),
            P("ep", None),
            P("ep", None),
            P("ep", None, "tp"),
            P("ep", None, "tp"),
            P("ep", "tp", None),
            P("ep", "tp"),
            P("ep", "tp"),
            P("tp", "ep"),
            P(),
        ),
        out_specs=(P("ep", "tp"), P("ep", "tp", None, None)),
        check_vma=False,
    )
```

```python
import jax
import jax.numpy as jnp
from jax import lax
from jax.experimental import pallas as pl
from jax.experimental.pallas import tpu as pltpu
from jax.sharding import PartitionSpec as P

EPS = 1e-06


def rms_scale(values):
    return lax.rsqrt(jnp.mean(values * values, axis=-1, keepdims=True) + EPS)


def body(
    tokens,
    old_state,
    lower_bound,
    head_gain,
    norm_gains,
    w_query,
    w_forget,
    w_value,
    w_outgate,
    w_mix_out,
    routes,
    route_scores,
    w_exp_gate,
    w_exp_up,
    w_exp_down,
    w_dense_gate,
    w_dense_up,
    w_dense_down,
    dense_mix,
):
    highest = lax.Precision.HIGHEST
    seqs, width = tokens.shape
    column_index = lax.axis_index("tp")
    part_width = width // lax.axis_size("tp")
    resid = tokens.astype(jnp.float32)
    normed = (resid * rms_scale(resid) * norm_gains[0]).astype(jnp.bfloat16)
    in_weights = jnp.concatenate([w_query, w_forget, w_value, w_outgate], axis=1)
    mix_rows = lax.all_to_all(normed, "ep", split_axis=1, concat_axis=0, tiled=True)
    projected = lax.psum_scatter(
        jnp.dot(mix_rows, in_weights, preferred_element_type=jnp.float32).astype(jnp.bfloat16),
        "ep",
        scatter_dimension=0,
        tiled=True,
    ).astype(jnp.float32)
    query_raw, forget_raw, value, out_gate = jnp.split(projected, 4, axis=1)
    heads = old_state.shape[1]
    head_size = old_state.shape[2]
    shape_heads = (seqs, heads, head_size)
    forget = lower_bound + (1.0 - lower_bound) * jax.nn.sigmoid(forget_raw)
    key_in = (1.0 - lower_bound) * jax.nn.sigmoid(-forget_raw)
    new_state = forget.reshape(shape_heads)[..., None] * old_state + key_in.reshape(shape_heads)[
        ..., None
    ] * value.reshape(seqs, heads, 1, head_size)
    query = jax.nn.silu(query_raw).reshape(shape_heads)
    read = jnp.einsum("thk,thkv->thv", query, new_state, precision=highest)
    gated = (
        read
        * rms_scale(read)
        * head_gain.reshape(heads, head_size)
        * jax.nn.silu(out_gate).reshape(shape_heads)
    )
    mixed_heads = gated.reshape(seqs, heads * head_size).astype(jnp.bfloat16)
    mix_part = jnp.dot(
        mixed_heads,
        lax.all_gather(w_mix_out, "ep", axis=1, tiled=True),
        preferred_element_type=jnp.float32,
    ).astype(jnp.bfloat16)
    mix_part = lax.optimization_barrier(mix_part).astype(jnp.float32)
    mix_out = lax.psum(mix_part.astype(jnp.bfloat16), "tp")
    mix_wide = lax.optimization_barrier(mix_out).astype(jnp.float32)
    after_mix = resid + mix_wide * rms_scale(mix_wide) * norm_gains[1]
    ffn_in = (after_mix * rms_scale(after_mix) * norm_gains[2]).astype(jnp.bfloat16)
    experts = lax.axis_size("ep")
    topk = routes.shape[1]
    capacity = max(2, 2 * seqs * topk // experts)
    flat_routes = routes.reshape(-1)
    onehot = (flat_routes[:, None] == jnp.arange(experts, dtype=jnp.int32)[None, :]).astype(
        jnp.int32
    )
    before = jnp.cumsum(onehot, axis=0) - onehot
    slots = jnp.sum(onehot * before, axis=1)
    cells = flat_routes * capacity + slots
    placed = cells[None, :] == jnp.arange(experts * capacity, dtype=jnp.int32)[:, None]
    repeated = jnp.repeat(ffn_in, topk, axis=0)
    outgoing = jnp.dot(placed.astype(jnp.bfloat16), repeated, preferred_element_type=jnp.float32)
    outgoing = outgoing.astype(jnp.bfloat16).reshape(experts, capacity, width)
    arrived = lax.all_to_all(outgoing, "ep", split_axis=0, concat_axis=0, tiled=True)
    sources, items, _ = arrived.shape
    expert_rows = arrived.reshape(sources * items, width)
    gate_pre = jnp.dot(expert_rows, w_exp_gate[0], preferred_element_type=jnp.float32)
    up_pre = jnp.dot(expert_rows, w_exp_up[0], preferred_element_type=jnp.float32)
    hidden = (jax.nn.silu(gate_pre) * up_pre).astype(jnp.bfloat16)
    partial_rows = jnp.dot(hidden, w_exp_down[0], preferred_element_type=jnp.float32).astype(
        jnp.bfloat16
    )
    partial_rows = lax.optimization_barrier(partial_rows).astype(jnp.float32)
    partial_rows = partial_rows.reshape(sources, items, width)
    summed = lax.psum_scatter(
        partial_rows.astype(jnp.bfloat16), "tp", scatter_dimension=2, tiled=True
    )
    returned = lax.all_to_all(summed, "ep", split_axis=0, concat_axis=0, tiled=True)
    first = jax.nn.sigmoid(route_scores[:, 0] - route_scores[:, 1])
    second = jax.nn.sigmoid(route_scores[:, 1] - route_scores[:, 0])
    route_weight = jnp.stack([first, second], axis=1).reshape(-1)
    weight_table = jnp.sum(
        (placed.astype(jnp.float32) * route_weight[None, :]).reshape(
            experts * capacity, seqs, topk
        ),
        axis=2,
    )
    expert_sum = jnp.dot(
        weight_table.T,
        returned.reshape(experts * capacity, part_width).astype(jnp.float32),
        precision=highest,
    )
    dense_weights = jnp.concatenate([w_dense_gate, w_dense_up], axis=1)
    dense_rows = lax.all_to_all(ffn_in, "ep", split_axis=1, concat_axis=0, tiled=True)
    dense_pre = lax.psum_scatter(
        jnp.dot(dense_rows, dense_weights, preferred_element_type=jnp.float32).astype(jnp.bfloat16),
        "ep",
        scatter_dimension=0,
        tiled=True,
    ).astype(jnp.float32)
    dense_gate_pre, dense_up_pre = jnp.split(dense_pre, 2, axis=1)
    dense_hidden = (jax.nn.silu(dense_gate_pre) * dense_up_pre).astype(jnp.bfloat16)
    dense_partial = jnp.dot(
        dense_hidden,
        lax.all_gather(w_dense_down, "ep", axis=1, tiled=True),
        preferred_element_type=jnp.float32,
    )
    dense_out = lax.psum_scatter(
        dense_partial.astype(jnp.bfloat16), "tp", scatter_dimension=1, tiled=True
    ).astype(jnp.float32)
    mix_weight = jax.nn.sigmoid(jnp.dot(ffn_in, dense_mix, preferred_element_type=jnp.float32))
    ffn_out = expert_sum + mix_weight[:, None] * dense_out
    squares = lax.psum(jnp.sum(ffn_out * ffn_out, axis=1), "tp")
    out_scale = lax.rsqrt(squares / width + EPS)
    gain_part = lax.dynamic_slice_in_dim(norm_gains[3], column_index * part_width, part_width, 0)
    resid_part = lax.dynamic_slice_in_dim(after_mix, column_index * part_width, part_width, 1)
    layer_out = (resid_part + ffn_out * out_scale[:, None] * gain_part).astype(jnp.bfloat16)
    return (layer_out, new_state)


def dot32(a, b):
    return jnp.dot(a, b, preferred_element_type=jnp.float32)


def silu(x):
    return x * jax.nn.sigmoid(x)


MESH = pl.DeviceIdType.MESH


class Sems:
    def __init__(self):
        self.used = 0

    def take(self, count):
        first = self.used
        self.used += count
        return first


def chips_by_distance(q, half):
    if half == 4:
        return [q, q + 1 - 2 * lax.rem(q, 2), 2 - q // 2, 3 - 3 * (q // 2)]
    return [q] + [lax.rem(q + k, half) for k in range(1, half)]


CHUNKS = 3
EARLY = 1


def fused_layer(
    tokens,
    old_state,
    bounds,
    head_gain,
    norm_gains,
    in_weights,
    w_mix,
    routes,
    scores,
    experts,
    dense,
    mix_row,
    n_ep,
    n_tp,
):
    bf16, f32, i32 = jnp.bfloat16, jnp.float32, jnp.int32
    seqs, width = tokens.shape
    heads, hs = old_state.shape[1:3]
    block, part = width // n_ep, width // n_tp
    chans = heads * hs
    topk = routes.shape[0]
    cap = max(2, 2 * seqs * topk // n_ep)
    cells, rows = n_ep * cap, n_ep * seqs
    eff, dff = experts[0].shape[2], dense[0].shape[1]
    half, ratio = n_ep // 2, n_ep // n_tp
    duo = 2 * seqs
    lanes = 128
    tile = 128
    chunk = dff // CHUNKS
    hc = chunk // 2
    few = ratio * cap

    send_at, recv_at = Sems(), Sems()

    def pair(count):
        return send_at.take(1), recv_at.take(count)

    P_TOK, P_ROUTE, P_PAIR, P_HEAD = pair(1), pair(1), pair(heads), pair(heads)
    V_DENSE = recv_at.take(CHUNKS)
    P_MIX, P_TP, P_STAT, P_OWN = pair(half), pair(half), pair(1), pair(ratio)
    P_SWAP, P_TWIN, P_BASE, P_DENSE = pair(1), pair(2), pair(1), pair(CHUNKS)
    P_ROWS, P_EXP, P_ALL = pair(1), pair(1), pair(2)
    P_RTP, P_RET = pair(1), pair(1)
    P_GATH, P_HAND, P_COLS, P_SQ = pair(CHUNKS), pair(CHUNKS), pair(1), pair(1)
    n_load = 14

    def kernel(
        tok_h, st_h, lb_h, hg_h, gn_h, wq_h, wf_h, wv_h, wo_h, wm_h, rt_h, sc_h,
        eg_h, eu_h, ed_h, dg_h, du_h, dd_h, mr_h,
        out, ns,
        tok, st, lb, hg, gn, win, wm, rt0, sc, wgu, wed, wd, wdd, mrow, wide_row,
        R, RP, RT, X, Y, Z, VD, PR, rd, KC, VL, MA, TX, TR, STAT, SX, SR, COL, OWN, SEL, MO, MP, MR,
        FF, AX, AR, DX, DR, DH, OT, OX, ET, ER, EI, acc, hid, RX, RR, RB, RG, dd, ddr, sq, sqr,
        send, recv, lsem,
    ):
        me_e, me_t = lax.axis_index("ep"), lax.axis_index("tp")
        q, c = me_e // 2, lax.rem(me_e, 2)
        partner = 2 * q + 1 - c
        chips = chips_by_distance(q, half)
        away = chips[:0:-1]
        line = half == 4
        at_end = lax.rem(q, 3) == 0
        beside = 1 + q // 3
        near = away[1:] if line else away

        def landed(ref, r):
            if line:
                pl.when(at_end)(lambda: arrive(ref.at[0 : far - 1], r))
                pl.when(jnp.logical_not(at_end))(lambda: arrive(ref.at[0:far], r))
            else:
                arrive(ref.at[0:far], r)

        def through(ox, via, s, r):
            if line:
                pl.when(at_end)(
                    lambda: put(ox.at[away[0]], via, (2 * beside + c, me_t), s, r)
                )

        def relay(j):
            def run():
                arrive(VD.at[j], V_DENSE + j)
                total = DX[j, away[0]].astype(f32) + VD[j].astype(f32)
                DX[j, away[0]] = total.astype(bf16)
                put(
                    DX.at[j, away[0]],
                    DR.at[j, q],
                    (2 * away[0] + c, me_t),
                    P_DENSE[0],
                    P_DENSE[1] + j,
                )

            def clear():
                DR[j, away[0]] = jnp.zeros((duo, chunk), bf16)

            if line:
                pl.when(jnp.logical_not(at_end))(run)
                pl.when(at_end)(clear)
        far_first = [2 * kk + d for kk in away for d in (c, 1 - c)] + [partner]
        ep_peers = list(enumerate(far_first, 1))
        if n_tp == 4:
            turn_tp = [n_tp - 1 - me_t, lax.rem(me_t + 2, n_tp), me_t + 1 - 2 * lax.rem(me_t, 2)]
        else:
            turn_tp = [lax.rem(me_t + dt, n_tp) for dt in range(1, n_tp)]
        tp_peers = list(enumerate(turn_tp, 1))

        barrier = pltpu.get_barrier_semaphore()
        for _, e in ep_peers:
            pl.semaphore_signal(barrier, inc=1, device_id=(e, me_t), device_id_type=MESH)
        for _, t in tp_peers:
            pl.semaphore_signal(barrier, inc=1, device_id=(me_e, t), device_id_type=MESH)

        def cut(first, size):
            return pl.ds(pl.multiple_of(first, 128), size)

        count = [0]

        def load(whole, *copies):
            at = count[0]
            count[0] += 1
            for src, dst in copies:
                pltpu.make_async_copy(src, dst, lsem.at[at]).start()
            return pltpu.make_async_copy(whole, whole, lsem.at[at])

        l_tok = load(tok, (tok_h, tok))
        l_gn = load(gn, (gn_h, gn))
        l_rt = load(rt0, (rt_h, rt0))
        l_in = load(
            win,
            *(
                (w.at[:, h * hs : (h + 1) * hs], win.at[h, :, i * hs : (i + 1) * hs])
                for h in range(heads)
                for i, w in enumerate((wq_h, wf_h, wv_h, wo_h))
            ),
        )
        l_small = [
            load(v, (h, v)) for h, v in ((lb_h, lb), (hg_h, hg), (sc_h, sc), (mr_h, mrow))
        ]
        l_st = load(st, (st_h, st))
        l_wm = load(wm, (wm_h, wm))
        l_wd = load(
            wd.at[:, 0],
            *(
                (
                    w.at[:, cut(j * chunk + c * hc, hc)],
                    wd.at[j, c, :, i * hc : (i + 1) * hc],
                )
                for j in range(CHUNKS)
                for i, w in enumerate((dg_h, du_h))
            ),
        )
        l_exp = [
            load(
                wgu,
                *(
                    (
                        w.at[0, :, i * tile : (i + 1) * tile],
                        wgu.at[:, (2 * i + k) * tile : (2 * i + k + 1) * tile],
                    )
                    for i in range(eff // tile)
                    for k, w in enumerate((eg_h, eu_h))
                ),
            ),
            load(wed, (ed_h.at[0], wed)),
        ]
        l_wdd = load(wdd, (dd_h, wdd))

        def put(src, dst, device, s, r):
            pltpu.make_async_remote_copy(
                src_ref=src,
                dst_ref=dst,
                send_sem=send.at[s],
                recv_sem=recv.at[r],
                device_id=device,
                device_id_type=MESH,
            ).start()

        def arrive(whole, r):
            pltpu.make_async_copy(whole, whole, recv.at[r]).wait()

        def left(whole, s):
            pltpu.make_async_copy(whole, whole, send.at[s]).wait()

        others, peers, far = n_ep - 1, n_tp - 1, half - 1

        mine = cut(me_e * block, block)
        own_rows = pl.ds(pl.multiple_of(me_e * seqs, seqs), seqs)

        l_tok.wait()
        l_gn.wait()
        l_rt.wait()
        pl.semaphore_wait(barrier, n_ep + n_tp - 2)
        for de, e in ep_peers:
            put(tok.at[:, cut(e * block, block)], R.at[me_e], (e, me_t), P_TOK[0], P_TOK[1])
        for de, e in ep_peers:
            put(rt0, RT.at[me_e], (e, me_t), P_ROUTE[0], P_ROUTE[1])
        for j in range(CHUNKS):
            for i, w in enumerate((dg_h, du_h)):
                put(
                    w.at[:, cut(j * chunk + (1 - c) * hc, hc)],
                    wd.at[j, c, :, i * hc : (i + 1) * hc],
                    (partner, me_t),
                    P_SWAP[0],
                    P_SWAP[1],
                )
        R[me_e] = tok[:, mine]
        RT[me_e] = rt0[...]
        resid = tok[...].astype(f32)
        scale0 = rms_scale(resid)
        g0 = gn[0:1, mine]
        g1 = gn[1:2, mine]
        g2 = gn[2:3, mine]
        l_in.wait()
        arrive(R.at[0:others], P_TOK[1])

        put(R, RP, (partner, me_t), P_TWIN[0], P_TWIN[1])
        scaled = (R[...].reshape(rows, block).astype(f32) * g0).astype(bf16)

        def project(h):
            piece = dot32(scaled, win[h]).astype(bf16)
            for e in range(n_ep):
                X[h, e % 2, e // 2] = piece[e * seqs : (e + 1) * seqs]
            put(X.at[h, 1 - c], Y.at[h], (partner, me_t), P_PAIR[0], P_PAIR[1] + h)

        def spread_head(h):
            arrive(Y.at[h], P_PAIR[1] + h)
            for kk in away:
                Z[h, kk] = (X[h, c, kk].astype(f32) + Y[h, kk].astype(f32)).astype(bf16)
                put(
                    Z.at[h, kk],
                    PR.at[h, q],
                    (2 * kk + c, me_t),
                    P_HEAD[0],
                    P_HEAD[1] + h,
                )
            PR[h, q] = (X[h, c, q].astype(f32) + Y[h, q].astype(f32)).astype(bf16)

        project(0)
        project(1)
        for h in range(heads):
            spread_head(h)
            if h + 2 < heads:
                project(h + 2)

        arrive(RT.at[0:others], P_ROUTE[1])
        short = lax.broadcasted_iota(i32, (rows, seqs), 1)
        turn = lax.broadcasted_iota(i32, (rows, seqs), 0)
        diagonal = short == turn - (turn // seqs) * seqs
        named = []
        for k in range(topk):
            across = jnp.concatenate(
                [jnp.broadcast_to(RT[e, k : k + 1, :], (seqs, seqs)) for e in range(n_ep)], axis=0
            )
            named.append(jnp.sum(jnp.where(diagonal, across, 0), axis=1, keepdims=True))
        lane = lax.broadcasted_iota(i32, (rows, lanes), 1)
        row = lax.broadcasted_iota(i32, (rows, lanes), 0)
        ones = [(lane == named[k]).astype(f32) for k in range(topk)]
        earlier = ((lane < row) & (lane >= (row // seqs) * seqs)).astype(bf16)
        before = dot32(earlier, sum(ones).astype(bf16))
        slots = [
            jnp.sum(o * before, axis=1, keepdims=True).astype(i32) for o in ones
        ]
        spot = lax.broadcasted_iota(i32, (rows, 1), 0) // seqs
        wide = lax.broadcasted_iota(i32, (rows, n_ep * cells), 1)
        chosen = jnp.zeros((rows, n_ep * cells), f32)
        for k in range(topk):
            place = named[k] * cells + spot * cap + slots[k]
            chosen = chosen + (wide == place).astype(f32)
        per = lanes // cells
        for i in range(n_ep // per):
            flipped = chosen[:, i * lanes : (i + 1) * lanes].T.astype(bf16)
            SEL[i * per : (i + 1) * per] = flipped.reshape(per, n_tp, few, rows)

        def pick(base, ox):
            lhs = SEL[:, pl.ds(me_t, 1)].reshape(n_ep * few, rows)
            picked = dot32(lhs, base[...].reshape(rows, block)).astype(bf16)
            for e in range(n_ep):
                ox[e] = picked[e * few : (e + 1) * few]

        pick(R, OT)
        ET[:, mine] = OT[me_e]
        ours = jnp.zeros((rows, lanes), i32)
        for k in range(topk):
            ours = ours + jnp.where(lane == k, named[k] * cap + slots[k], 0)
        OWN[...] = ours
        for copy in l_small:
            copy.wait()
        wide_row[...] = mrow[...].astype(f32)
        at_own = OWN[own_rows, :]
        spread = lax.broadcasted_iota(i32, (seqs, cells), 1)
        gap = jnp.sum(
            jnp.where(diagonal[0:seqs], jnp.broadcast_to(sc[0:1, :] - sc[1:2, :], (seqs, seqs)), 0.0),
            axis=1,
            keepdims=True,
        )
        table = jnp.where(spread == at_own[:, 0:1], jax.nn.sigmoid(gap), 0.0)
        table = table + jnp.where(spread == at_own[:, 1:2], jax.nn.sigmoid(-gap), 0.0)

        arrive(RP, P_TWIN[1])

        def gains_of(device):
            return gn[2:3, cut(device * block, block)]

        FF[c] = (R[...].reshape(rows, block).astype(f32) * g2).astype(bf16)
        FF[1 - c] = (RP[...].reshape(rows, block).astype(f32) * gains_of(partner)).astype(bf16)

        def dense_part(j, ox, to):
            piece = (dot32(FF[0], wd[j, 0]) + dot32(FF[1], wd[j, 1])).astype(bf16)
            for kk in range(half):
                ox[kk] = piece[kk * duo : (kk + 1) * duo]
            to[q] = ox[q]

        def dense_send(ox, to, s, r, direct=away):
            for kk in direct:
                put(ox.at[kk], to.at[q], (2 * kk + c, me_t), s, r)

        l_wd.wait()
        arrive(wd.at[:, 0], P_SWAP[1])
        for j in range(EARLY):
            dense_part(j, AX.at[j], AR.at[j])

        l_st.wait()
        for h in range(heads):
            arrive(PR.at[h, 0:far], P_HEAD[1] + h)
            total = PR[h, 0].astype(f32)
            for kk in range(1, half):
                total = total + PR[h, kk].astype(f32)
            total = total * scale0
            at = slice(h * hs, (h + 1) * hs)
            bound = lb[0:1, at]
            raw = total[:, hs : 2 * hs]
            forget = bound + (1.0 - bound) * jax.nn.sigmoid(raw)
            key_in = (1.0 - bound) * jax.nn.sigmoid(-raw)
            query = silu(total[:, 0:hs])
            value = total[:, 2 * hs : 3 * hs]
            columns = jnp.concatenate(
                [forget, key_in, query * forget, jnp.zeros((hs - 3 * seqs, hs), f32)], axis=0
            ).T
            KC[h] = columns
            VL[h] = value
            for s in range(seqs):
                rd[s : s + 1, :] = jnp.sum(
                    columns[:, 2 * seqs + s : 2 * seqs + s + 1] * st[s, h], axis=0, keepdims=True
                )
            read = rd[...] + jnp.sum(query * key_in, axis=1, keepdims=True) * value
            gated = read * rms_scale(read) * hg[0:1, at] * silu(total[:, 3 * hs :])
            MA[h, me_e] = gated.astype(bf16)
            for de, e in ep_peers:
                put(
                    MA.at[h, me_e],
                    MA.at[h, me_e],
                    (e, me_t),
                    P_MIX[0],
                    P_MIX[1] + q,
                )

        def update(h):
            for s in range(seqs):
                ns[s, h] = (
                    KC[h, :, s : s + 1] * st[s, h]
                    + KC[h, :, seqs + s : seqs + s + 1] * VL[h, s : s + 1, :]
                )

        update(0)
        update(1)
        for de, e in ep_peers:
            put(OT.at[e], ET.at[:, mine], (e, me_t), P_ROWS[0], P_ROWS[1])

        l_wm.wait()
        for g, kk in enumerate(chips):
            arrive(MA.at[:, 0 : 2 if g else 1], P_MIX[1] + kk)
            lhs = jnp.concatenate(
                [MA[h, pl.ds(2 * kk, 2)].reshape(duo, hs) for h in range(heads)], axis=1
            )
            piece = dot32(lhs, wm[...]).astype(bf16)
            TX[kk] = piece
            TR[me_t, kk] = piece
            for dt, t in tp_peers:
                put(
                    TX.at[kk],
                    TR.at[me_t, kk],
                    (me_e, t),
                    P_TP[0],
                    P_TP[1] + kk,
                )
        for j in range(EARLY):
            dense_send(AX.at[j], AR.at[j], *P_BASE)
        lane_duo = lax.broadcasted_iota(i32, (duo, lanes), 1)
        mixer = jnp.concatenate(
            [
                wide_row[pl.ds(me_e * (block // lanes) + i, 1), :]
                for i in range(block // lanes)
            ],
            axis=1,
        )
        for kk in chips:
            arrive(TR.at[0:peers, 0], P_TP[1] + kk)
            total = TR[0, kk].astype(f32)
            for t in range(1, n_tp):
                total = total + TR[t, kk].astype(f32)
            narrow = total.astype(bf16)
            MO[pl.ds(2 * kk, 2)] = narrow.reshape(2, seqs, block)
            mixed = narrow.astype(f32)
            base = R[pl.ds(2 * kk, 2)].reshape(duo, block).astype(f32)
            lifted = mixed * g1
            figures = (
                base * base,
                mixed * mixed,
                base * lifted,
                lifted * lifted,
                base * g2 * mixer,
                lifted * g2 * mixer,
            )
            stat = jnp.zeros((duo, lanes), f32)
            for i, figure in enumerate(figures):
                stat = stat + jnp.where(
                    lane_duo == i, jnp.sum(figure, axis=1, keepdims=True), 0.0
                )
            STAT[kk] = stat
        put(MO, MP, (partner, me_t), P_TWIN[0], P_TWIN[1] + 1)
        SX[...] = STAT[...].reshape(rows, lanes).T[0:8, :]
        SR[me_e] = SX[...]
        for de, e in ep_peers:
            put(SX, SR.at[me_e], (e, me_t), P_STAT[0], P_STAT[1])
        pick(MO, OX)
        for de, e in ep_peers:
            put(OX.at[e], ER.at[:, mine], (e, me_t), P_EXP[0], P_EXP[1])
        ER[:, mine] = OX[me_e]

        FF[c] = (MO[...].reshape(rows, block).astype(f32) * (g1 * g2)).astype(bf16)
        arrive(MP, P_TWIN[1] + 1)
        both = gn[1:2, cut(partner * block, block)] * gains_of(partner)
        FF[1 - c] = (MP[...].reshape(rows, block).astype(f32) * both).astype(bf16)
        for j in range(EARLY):
            dense_part(j, DX.at[j], DR.at[j])
            through(DX.at[j], VD.at[j], P_DENSE[0], V_DENSE + j)
            dense_send(DX.at[j], DR.at[j], P_DENSE[0], P_DENSE[1] + j, near)

        def send_own():
            for _, e in ep_peers:
                put(
                    MO.at[e],
                    MR.at[lax.rem(me_e, ratio)],
                    (e, me_t),
                    P_OWN[0],
                    P_OWN[1] + lax.rem(me_e, ratio),
                )
            MR[lax.rem(me_e, ratio)] = MO[me_e]

        holds = me_e // ratio == me_t
        pl.when(holds)(send_own)
        update(2)
        update(3)
        for j in range(EARLY):
            relay(j)

        arrive(SR.at[0:others], P_STAT[1])
        total = SR[0]
        for e in range(1, n_ep):
            total = total + SR[e]
        inv_mix = lax.rsqrt(total[1:2] / width + EPS)
        squares = total[0:1] + 2.0 * inv_mix * total[2:3] + inv_mix * inv_mix * total[3:4]
        inv_after = lax.rsqrt(jnp.maximum(squares, 0.0) / width + EPS)
        weight = jax.nn.sigmoid(inv_after * (total[4:5] + inv_mix * total[5:6]))
        back = jnp.where(row == 0, inv_mix, jnp.where(row == 1, inv_after, jnp.where(row == 2, weight, 0.0)))
        back = back.T
        COL[...] = back
        def normed(base, mixed, device):
            at = cut(device * block, block)
            after = base[...].reshape(rows, block).astype(f32)
            after = after + mixed[...].reshape(rows, block).astype(f32) * back[:, 0:1] * gn[1:2, at]
            return (after * back[:, 1:2] * gn[2:3, at]).astype(bf16)

        FF[c] = normed(R, MO, me_e)
        FF[1 - c] = normed(RP, MP, partner)
        for j in range(EARLY, CHUNKS):
            dense_part(j, DX.at[j], DR.at[j])
            through(DX.at[j], VD.at[j], P_DENSE[0], V_DENSE + j)
        for j in range(EARLY, CHUNKS):
            dense_send(DX.at[j], DR.at[j], P_DENSE[0], P_DENSE[1] + j, near)

        arrive(OT.at[0:others], P_ROWS[1])
        arrive(OX.at[0:others], P_EXP[1])
        marks = jnp.dot(
            SEL[me_e, me_t].astype(f32),
            back,
            precision=lax.Precision.HIGHEST,
            preferred_element_type=f32,
        )
        share = pl.ds(pl.multiple_of(me_t * few, few), few)
        sides = (slice(0, width // 2), slice(width // 2, width))
        for i, side in enumerate(sides):
            after = ET[:, side].astype(f32) + ER[:, side].astype(f32) * marks[:, 0:1] * gn[1:2, side]
            EI[share, side] = (after * marks[:, 1:2] * gn[2:3, side]).astype(bf16)
            for dt, t in tp_peers:
                here = EI.at[share, side]
                put(here, here, (me_e, t), P_ALL[0], P_ALL[1] + i)

        for j in range(EARLY, CHUNKS):
            relay(j)
        chip_rows = pl.ds(pl.multiple_of(q * duo, duo), duo)

        def hidden(j):
            landed(DR.at[j], P_DENSE[1] + j)
            total = DR[j, 0].astype(f32)
            for kk in range(1, half):
                total = total + DR[j, kk].astype(f32)
            if j == 0:
                arrive(AR.at[:, 0:far], P_BASE[1])
            if j < EARLY:
                base = AR[j, 0].astype(f32)
                for kk in range(1, half):
                    base = base + AR[j, kk].astype(f32)
                own = COL[chip_rows, :]
                total = (base + own[:, 0:1] * total) * own[:, 1:2]
            here = DH.at[j, c, q]
            here[...] = (silu(total[:, :hc]) * total[:, hc:]).astype(bf16)
            for kk in away:
                put(here, here, (2 * kk + c, me_t), P_GATH[0], P_GATH[1] + j)
            put(here, here, (partner, me_t), P_HAND[0], P_HAND[1] + j)

        def hand_over(j):
            arrive(DH.at[j, 0, 0:far], P_GATH[1] + j)
            for kk in away:
                here = DH.at[j, c, kk]
                put(here, here, (partner, me_t), P_HAND[0], P_HAND[1] + j)

        def gathered(j):
            arrive(DH.at[j, 0], P_HAND[1] + j)
            total = 0.0
            for i in range(2):
                at = j * chunk + i * hc
                total = total + dot32(DH[j, i].reshape(rows, hc), wdd[at : at + hc, :])
            return total

        for copy in l_exp:
            copy.wait()
        hidden(0)
        arrive(EI.at[0 : peers * few, sides[0]], P_ALL[1])

        @pl.loop(0, eff // tile)
        def _(i):
            at = cut(i * 2 * tile, 2 * tile)
            acc[:, at] = dot32(EI[:, sides[0]], wgu[sides[0], at])

        arrive(EI.at[0 : peers * few, sides[1]], P_ALL[1] + 1)

        @pl.loop(0, eff // tile)
        def _(i):
            at = cut(i * 2 * tile, 2 * tile)
            both = acc[:, at] + dot32(EI[:, sides[1]], wgu[sides[1], at])
            hid[:, cut(i * tile, tile)] = (silu(both[:, :tile]) * both[:, tile:]).astype(bf16)

        hidden(1)
        for dt, t in (tp_peers + [(0, me_t)])[:2]:
            piece = dot32(hid[...], wed[:, cut(t * part, part)]).astype(bf16)
            if dt:
                RX[dt] = piece
                put(RX.at[dt], RR.at[me_t], (me_e, t), P_RTP[0], P_RTP[1])
            else:
                RR[me_t] = piece
        hidden(2)
        for dt, t in (tp_peers + [(0, me_t)])[2:]:
            piece = dot32(hid[...], wed[:, cut(t * part, part)]).astype(bf16)
            if dt:
                RX[dt] = piece
                put(RX.at[dt], RR.at[me_t], (me_e, t), P_RTP[0], P_RTP[1])
            else:
                RR[me_t] = piece

        def give_back():
            arrive(RR.at[0:peers], P_RTP[1])
            total = RR[0].astype(f32)
            for t in range(1, n_tp):
                total = total + RR[t].astype(f32)
            total = total.astype(bf16)
            for e in range(n_ep):
                RB[e] = total[e * cap : (e + 1) * cap]
            RG[me_e] = RB[me_e]
            for de, e in ep_peers:
                put(RB.at[e], RG.at[me_e], (e, me_t), P_RET[0], P_RET[1])

        for j in range(CHUNKS):
            hand_over(j)
        give_back()
        l_wdd.wait()
        total = gathered(0)
        for j in range(1, CHUNKS):
            total = total + gathered(j)
        total = total.astype(bf16)
        for e in range(n_ep):
            dd[e] = total[e * seqs : (e + 1) * seqs]
        to = me_e // ratio
        landing = ddr.at[lax.rem(me_e, ratio), me_t]
        for _, e in ep_peers:
            put(dd.at[e], landing, (e, to), P_COLS[0], P_COLS[1])

        def keep():
            landing[...] = dd[me_e]

        pl.when(holds)(keep)
        pl.when(jnp.logical_not(holds))(
            lambda: put(dd.at[me_e], landing, (me_e, to), P_COLS[0], P_COLS[1])
        )

        arrive(RG.at[0:others], P_RET[1])
        expert_sum = jnp.dot(
            table,
            RG[...].astype(f32).reshape(cells, part),
            precision=lax.Precision.HIGHEST,
            preferred_element_type=f32,
        )
        own_cols = COL[own_rows, :]
        part_at = cut(me_t * part, part)
        for j in range(ratio):
            source = me_t * ratio + j

            def wait_own(j=j):
                arrive(MR.at[j], P_OWN[1] + j)

            pl.when(source != me_e)(wait_own)
        mix_own = jnp.concatenate([MR[j].astype(f32) for j in range(ratio)], axis=1)
        after_own = tok[:, part_at].astype(f32) + mix_own * own_cols[:, 0:1] * gn[1:2, part_at]
        pl.when(holds)(lambda: arrive(dd.at[0:others], P_COLS[1]))
        pl.when(jnp.logical_not(holds))(lambda: arrive(dd, P_COLS[1]))
        pieces = []
        for j in range(ratio):
            total = ddr[j, 0].astype(f32)
            for t in range(1, n_tp):
                total = total + ddr[j, t].astype(f32)
            pieces.append(total)
        ffn_out = expert_sum + own_cols[:, 2:3] * jnp.concatenate(pieces, axis=1)
        mass = jnp.sum(ffn_out * ffn_out, axis=1, keepdims=True)
        sq[...] = jnp.broadcast_to(mass, (seqs, lanes))
        sqr[me_t] = sq[...]
        for dt, t in tp_peers:
            put(sq, sqr.at[me_t], (me_e, t), P_SQ[0], P_SQ[1])
        arrive(sqr.at[0:peers], P_SQ[1])
        total = sqr[0]
        for t in range(1, n_tp):
            total = total + sqr[t]
        scale = lax.rsqrt(total[:, 0:1] / width + EPS)
        out[...] = (after_own + ffn_out * scale * gn[3:4, part_at]).astype(bf16)
        pl.when(holds)(lambda: left(MO.at[0:others], P_OWN[0]))
        pl.when(holds)(lambda: left(dd.at[0:others], P_COLS[0]))
        pl.when(jnp.logical_not(holds))(lambda: left(dd, P_COLS[0]))
        for whole, ends in (
            (R.at[0:others], P_TOK),
            (RT.at[0:others], P_ROUTE),
            (Y, P_PAIR),
            (Z.at[:, 0:far], P_HEAD),
            (MA.at[:, 0:others], P_MIX),
            (TR.at[0:peers], P_TP),
            (SR.at[0:others], P_STAT),
            (wd.at[:, 0], P_SWAP),
            (FF, P_TWIN),
            (AX.at[:, 0:far], P_BASE),
            (EI.at[0 : peers * few], P_ALL),
            (OT.at[0:others], P_ROWS),
            (OX.at[0:others], P_EXP),
            (DX.at[:, 0:far], P_DENSE),
            (DH.at[:, 0, 0:far], P_GATH),
            (DH.at[:, 0], P_HAND),
            (RR.at[0:peers], P_RTP),
            (RB.at[0:others], P_RET),
            (sqr.at[0:peers], P_SQ),
        ):
            left(whole, ends[0])

    vmem = pl.BlockSpec(memory_space=pltpu.VMEM)
    hbm = pl.BlockSpec(memory_space=pltpu.HBM)
    b = lambda *s: pltpu.VMEM(s, bf16)
    f = lambda *s: pltpu.VMEM(s, f32)
    n = lambda *s: pltpu.VMEM(s, i32)
    return pl.pallas_call(
        kernel,
        out_shape=(
            jax.ShapeDtypeStruct((seqs, part), bf16),
            pltpu.VMEM(old_state.shape, f32),
        ),
        in_specs=[hbm] * 19,
        out_specs=(vmem, vmem),
        scratch_shapes=[
            b(seqs, width),
            f(*old_state.shape),
            f(1, chans),
            f(1, chans),
            f(*norm_gains.shape),
            b(heads, block, 4 * hs),
            b(chans, block),
            n(topk, seqs),
            f(topk, seqs),
            b(width, 2 * eff),
            b(eff, width),
            b(CHUNKS, 2, block, chunk),
            b(dff, block),
            b(width // lanes, lanes),
            f(width // lanes, lanes),
            b(n_ep, seqs, block),
            b(n_ep, seqs, block),
            n(n_ep, topk, seqs),
            b(heads, 2, half, seqs, 4 * hs),
            b(heads, half, seqs, 4 * hs),
            b(heads, half, seqs, 4 * hs),
            b(CHUNKS, duo, chunk),
            b(heads, half, seqs, 4 * hs),
            f(seqs, hs),
            f(heads, hs, hs),
            f(heads, seqs, hs),
            b(heads, n_ep, seqs, hs),
            b(half, duo, block),
            b(n_tp, half, duo, block),
            f(half, duo, lanes),
            f(8, lanes),
            f(n_ep, 8, lanes),
            f(rows, lanes),
            n(rows, lanes),
            b(n_ep, n_tp, few, rows),
            b(n_ep, seqs, block),
            b(n_ep, seqs, block),
            b(ratio, seqs, block),
            b(2, rows, block),
            b(EARLY, half, duo, chunk),
            b(EARLY, half, duo, chunk),
            b(CHUNKS, half, duo, chunk),
            b(CHUNKS, half, duo, chunk),
            b(CHUNKS, 2, half, duo, hc),
            b(n_ep, few, block),
            b(n_ep, few, block),
            b(few, width),
            b(few, width),
            b(cells, width),
            f(cells, 2 * eff),
            b(cells, eff),
            b(n_tp, cells, part),
            b(n_tp, cells, part),
            b(n_ep, cap, part),
            b(n_ep, cap, part),
            b(n_ep, seqs, block),
            b(ratio, n_tp, seqs, block),
            f(seqs, lanes),
            f(n_tp, seqs, lanes),
            pltpu.SemaphoreType.DMA((send_at.used,)),
            pltpu.SemaphoreType.DMA((recv_at.used,)),
            pltpu.SemaphoreType.DMA((n_load,)),
        ],
        compiler_params=pltpu.CompilerParams(
            collective_id=1, has_side_effects=True, vmem_limit_bytes=40 * 1024 * 1024
        ),
        name="fused_layer",
    )(
        *(
            pltpu.with_memory_space_constraint(x, pltpu.HBM)
            for x in (
                tokens,
                old_state,
                bounds,
                head_gain,
                norm_gains,
                *in_weights,
                w_mix,
                routes,
                scores,
                *experts,
                *dense,
                mix_row,
            )
        )
    )


PIECES = 16


def write_out(layer_out, new_state):
    per = new_state.shape[0] // PIECES

    def kernel(small, big, small_to, big_to, sems):
        copies = [pltpu.make_async_copy(small, small_to, sems.at[PIECES])]
        for i in range(PIECES):
            at = pl.ds(i * per, per)
            copies.append(pltpu.make_async_copy(big.at[at], big_to.at[at], sems.at[i]))
        for copy in copies:
            copy.start()
        for copy in copies:
            copy.wait()

    vmem = pl.BlockSpec(memory_space=pltpu.VMEM)
    hbm = pl.BlockSpec(memory_space=pltpu.HBM)
    return pl.pallas_call(
        kernel,
        out_shape=(
            pltpu.HBM(layer_out.shape, layer_out.dtype),
            pltpu.HBM(new_state.shape, new_state.dtype),
        ),
        in_specs=[vmem] * 2,
        out_specs=(hbm, hbm),
        scratch_shapes=[pltpu.SemaphoreType.DMA((PIECES + 1,))],
        compiler_params=pltpu.CompilerParams(vmem_limit_bytes=1024 * 1024),
        name="write_out",
    )(
        pltpu.with_memory_space_constraint(layer_out, pltpu.VMEM),
        pltpu.with_memory_space_constraint(new_state, pltpu.VMEM),
    )


def fast_body(
    tokens,
    old_state,
    lower_bound,
    head_gain,
    norm_gains,
    w_query,
    w_forget,
    w_value,
    w_outgate,
    w_mix_out,
    routes,
    route_scores,
    w_exp_gate,
    w_exp_up,
    w_exp_down,
    w_dense_gate,
    w_dense_up,
    w_dense_down,
    dense_mix,
):
    layer_out, new_state = fused_layer(
        tokens,
        old_state,
        lower_bound[None, :],
        head_gain[None, :],
        norm_gains,
        (w_query, w_forget, w_value, w_outgate),
        w_mix_out,
        routes.T,
        route_scores.T,
        (w_exp_gate, w_exp_up, w_exp_down),
        (w_dense_gate, w_dense_up, w_dense_down),
        dense_mix.reshape(-1, 128),
        lax.axis_size("ep"),
        lax.axis_size("tp"),
    )
    return write_out(layer_out, new_state)


def solution(mesh):
    n_ep, n_tp = mesh.shape['ep'], mesh.shape['tp']
    fits = n_ep % n_tp == 0 and n_ep % 2 == 0 and n_ep * n_tp <= 64
    return jax.shard_map(
        fast_body if fits else body,
        mesh=mesh,
        in_specs=(
            P("ep", None),
            P("ep", "tp", None, None),
            P("tp"),
            P("tp"),
            P(),
            P("ep", "tp"),
            P("ep", "tp"),
            P("ep", "tp"),
            P("ep", "tp"),
            P("tp", "ep"),
            P("ep", None),
            P("ep", None),
            P("ep", None, "tp"),
            P("ep", None, "tp"),
            P("ep", "tp", None),
            P("ep", "tp"),
            P("ep", "tp"),
            P("tp", "ep"),
            P(),
        ),
        out_specs=(P("ep", "tp"), P("ep", "tp", None, None)),
        check_vma=False,
    )
```
